32 devices in a mesh: sp: 4 (over z), fs: 4 (over y, x), tp: 2 (over core).
Axes of the slice: x: 2, y: 2, z: 4, core: 2. Of those that a mesh axis runs over, the one named last changes fastest.
Arguments:
- stream: bfloat16 [4, 1024, 2048], P('fs', 'sp'), may hold values from -6 to 6
- norm_gain: bfloat16 [2048], replicated, may hold values from 0.099609375 to 1.8984375
- query_weight: bfloat16 [2048, 1024], P(None, 'tp'), may hold values from -0.125 to 0.125
- key_weight: bfloat16 [2048, 1024], P(None, 'tp'), may hold values from -0.125 to 0.125
- value_weight: bfloat16 [2048, 1024], P(None, 'tp'), may hold values from -0.125 to 0.125
- filter_input: bfloat16 [2048, 1024], P(None, 'tp'), may hold values from -0.125 to 0.125
- filter_gate: bfloat16 [2048, 1024], P(None, 'tp'), may hold values from -0.125 to 0.125
- score_offset: bfloat16 [4, 1024, 16], P('fs', 'sp', 'tp'), may hold values from -16 to 0
- head_gain: bfloat16 [1024], P('tp'), may hold values from 0.099609375 to 1.8984375
- filter_taps: bfloat16 [31, 1024], P(None, 'tp'), may hold values from -5 to 5
- channel_gain: bfloat16 [1024], P('tp'), may hold values from 0.099609375 to 1.8984375
- channel_shift: bfloat16 [1024], P('tp'), may hold values from -3 to 3
- attend_out: bfloat16 [1024, 2048], P('tp'), may hold values from -0.125 to 0.125
- filter_out: bfloat16 [1024, 2048], P('tp'), may hold values from -0.125 to 0.125
Outputs:
- mixed_out: bfloat16 [4, 1024, 2048], P('fs', ('sp', 'tp'))
- mass_log: float32 [4, 1024, 16], P('fs', 'sp', 'tp')
The draws below stay inside these ranges and needn't reach their ends.
All inputs are finite; a program needn't handle non-finite values.
Results may differ from the reference program's by a relative error of at most 0.015.
Values may be sent and summed in bfloat16 or wider, within the bound.
A program may use at most 64 MiB of HBM per device.

```python
import math
import jax
import jax.numpy as jnp
from jax import lax

D = 2048
HEAD_COUNT = 16
HEAD_DIM = 64
CONV = 1024
KERNEL = 31
TOK_DEV = 256
ATTN = 1024
SEQUENCE_LENGTH = 1024
SEQUENCE_COUNT = 4


def draw_score_offset(key, part):
    key_collection = jax.random.split(jax.random.fold_in(key, 3), 4)
    slow_share = 0.5
    slowly = jax.random.bernoulli(key_collection[0], slow_share, (SEQUENCE_COUNT, 1, HEAD_COUNT))
    levels = jnp.where(slowly, math.log(0.15 / SEQUENCE_LENGTH), math.log(1.0 / 40.0))
    blocks = SEQUENCE_LENGTH // TOK_DEV
    shifts = jax.random.uniform(key_collection[1], (SEQUENCE_COUNT, blocks, 1, HEAD_COUNT), jnp.float32, -0.7, 0.7)
    shifts = jnp.broadcast_to(shifts, (SEQUENCE_COUNT, blocks, TOK_DEV, HEAD_COUNT)).reshape(SEQUENCE_COUNT, SEQUENCE_LENGTH, HEAD_COUNT)
    jitter = jax.random.uniform(key_collection[2], (SEQUENCE_COUNT, SEQUENCE_LENGTH, HEAD_COUNT), jnp.float32, -1.0, 1.0)
    break_fractions = jax.random.randint(key_collection[3], (SEQUENCE_COUNT, 4, 1, HEAD_COUNT), 0, SEQUENCE_LENGTH)
    slot_positions = jnp.arange(SEQUENCE_LENGTH, dtype=jnp.int32)[None, None, :, None]
    broken_weights = jnp.any(slot_positions == break_fractions, axis=1)
    values = jnp.where(broken_weights, -0.6 + 0.3 * jitter, levels + shifts + jitter)
    return values.astype(jnp.bfloat16)


def draw_filter_taps(key, part):
    entry_key, scale_key = jax.random.split(jax.random.fold_in(key, 7))
    channel = jnp.arange(CONV, dtype=jnp.float32) / CONV
    roughness = jax.random.uniform(scale_key, (1, CONV), jnp.float32, 0.7, 1.4)
    entries = jnp.clip(jax.random.normal(entry_key, (KERNEL, CONV), jnp.float32), -4.0, 4.0)
    scaling = 4.0 ** channel
    return (entries * scaling[None, :] * roughness / math.sqrt(KERNEL)).astype(jnp.bfloat16)


def block_scale(rng, shape, cuts, smallest, top_value):
    factor_of = 1.0
    for dim, shards_of in cuts:
        draws = jax.random.uniform(jax.random.fold_in(jax.random.fold_in(rng, 6), dim), (shards_of,), jnp.float32, smallest / len(cuts), top_value / len(cuts))
        factor_of = factor_of * jnp.repeat(jnp.exp(draws), shape[dim] // shards_of).reshape((-1,) + (1,) * (len(shape) - 1 - dim))
    return factor_of


def normal_values(own_key, dims, width, reach, shards=(), kind=jnp.bfloat16):
    array = width * jax.random.normal(own_key, dims, jnp.float32)
    if shards:
        array = array * block_scale(own_key, dims, shards, -0.22, 0.18)
    return jnp.clip(array, -reach, reach).astype(kind)


def setup_inputs(seed: int = 0) -> dict:
    key_of = jax.random.split(jax.random.key(seed), 15)
    return {
        "stream": normal_values(key_of[0], (SEQUENCE_COUNT, SEQUENCE_LENGTH, D), 1.0, 6.0, ((0, 4), (1, 4))),
        "norm_gain": jnp.clip(1.0 + 0.18 * jax.random.normal(key_of[1], (D,), jnp.float32), 0.099609375, 1.8984375).astype(jnp.bfloat16),
        "query_weight": normal_values(key_of[2], (D, ATTN), D ** -0.5, 0.125, ((1, 2),)),
        "key_weight": normal_values(key_of[3], (D, ATTN), D ** -0.5, 0.125, ((1, 2),)),
        "value_weight": normal_values(key_of[4], (D, ATTN), D ** -0.5, 0.125, ((1, 2),)),
        "filter_input": normal_values(key_of[5], (D, CONV), D ** -0.5, 0.125, ((1, 2),)),
        "filter_gate": normal_values(key_of[6], (D, CONV), D ** -0.5, 0.125, ((1, 2),)),
        "score_offset": draw_score_offset(jax.random.fold_in(key_of[14], 71), 0),
        "head_gain": jnp.clip(1.0 + 0.18 * jax.random.normal(key_of[8], (ATTN,), jnp.float32), 0.099609375, 1.8984375).astype(jnp.bfloat16),
        "filter_taps": draw_filter_taps(jax.random.fold_in(key_of[14], 71), 0),
        "channel_gain": jnp.clip(1.0 + 0.18 * jax.random.normal(key_of[10], (CONV,), jnp.float32), 0.099609375, 1.8984375).astype(jnp.bfloat16),
        "channel_shift": normal_values(key_of[11], (CONV,), 0.5, 3.0, ((0, 2),)),
        "attend_out": normal_values(key_of[12], (ATTN, D), (ATTN + CONV) ** -0.5, 0.125, ((0, 2),)),
        "filter_out": normal_values(key_of[13], (CONV, D), (ATTN + CONV) ** -0.5, 0.125, ((0, 2),)),
    }


rms_eps = 1e-06
norm_eps = 1e-05
mass_floor = 0.01

def attend_sequence(queries, keys_seq, values_seq, offsets):
    query_block = min(512, SEQUENCE_LENGTH)
    qfloat = queries.astype(jnp.float32).reshape(SEQUENCE_LENGTH, HEAD_COUNT, HEAD_DIM)
    kfloat = keys_seq.astype(jnp.float32).reshape(SEQUENCE_LENGTH, HEAD_COUNT, HEAD_DIM)
    vfloat = values_seq.astype(jnp.float32).reshape(SEQUENCE_LENGTH, HEAD_COUNT, HEAD_DIM)
    offsets_t = offsets.astype(jnp.float32).T
    key_pos = jnp.arange(SEQUENCE_LENGTH, dtype=jnp.int32)

    def one_block(block_index):
        first_row = (block_index * query_block).astype(jnp.int32)
        qpart = lax.dynamic_slice_in_dim(qfloat, first_row, query_block, 0)
        scores = jnp.einsum('thd,shd->hts', qpart, kfloat, precision=lax.Precision.HIGHEST) * HEAD_DIM ** (-0.5)
        scores = scores + offsets_t[:, None, :]
        query_pos = first_row + jnp.arange(query_block, dtype=jnp.int32)
        strict = key_pos[None, :] < query_pos[:, None]
        losing = jnp.where(strict[None], jax.nn.log_sigmoid(-scores), 0.0)
        beyond = lax.cumsum(losing, axis=2, reverse=True) - losing
        weights = jnp.where(strict[None], jnp.exp(jax.nn.log_sigmoid(scores) + beyond), 0.0)
        weight_mass = lax.optimization_barrier(jnp.sum(weights, axis=2))
        rounded = lax.optimization_barrier(weights.astype(jnp.bfloat16)).astype(jnp.float32)
        attended = jnp.einsum('hts,shd->thd', rounded, vfloat, precision=lax.Precision.HIGHEST)
        return (attended, weight_mass.T)
    attended, weight_mass = lax.map(one_block, jnp.arange(SEQUENCE_LENGTH // query_block, dtype=jnp.int32))
    return (attended.reshape(SEQUENCE_LENGTH, HEAD_COUNT, HEAD_DIM), weight_mass.reshape(SEQUENCE_LENGTH, HEAD_COUNT))

def reference(stream, norm_gain, query_weight, key_weight, value_weight, filter_input, filter_gate, score_offset, head_gain, filter_taps, channel_gain, channel_shift, attend_out, filter_out):
    xfloat = stream.astype(jnp.float32)
    normed = xfloat * lax.rsqrt(lax.optimization_barrier(jnp.mean(xfloat * xfloat, axis=-1, keepdims=True)) + rms_eps)
    normed = (normed * norm_gain.astype(jnp.float32)).astype(jnp.bfloat16)
    flat = normed.reshape(SEQUENCE_COUNT * SEQUENCE_LENGTH, D)

    def project(weight):
        return jnp.dot(flat, weight, preferred_element_type=jnp.float32).astype(jnp.bfloat16)
    queries = project(query_weight).reshape(SEQUENCE_COUNT, SEQUENCE_LENGTH, ATTN)
    keys_all = project(key_weight).reshape(SEQUENCE_COUNT, SEQUENCE_LENGTH, ATTN)
    values_all = project(value_weight).reshape(SEQUENCE_COUNT, SEQUENCE_LENGTH, ATTN)
    conv_values = project(filter_input)
    conv_gates = project(filter_gate)

    def per_sequence(seq_index):
        return attend_sequence(queries[seq_index], keys_all[seq_index], values_all[seq_index], score_offset[seq_index])
    attended, weight_mass = lax.map(per_sequence, jnp.arange(SEQUENCE_COUNT, dtype=jnp.int32))
    head_scale = lax.rsqrt(lax.optimization_barrier(jnp.mean(attended * attended, axis=-1, keepdims=True)) + rms_eps)
    heads_out = attended * head_scale * head_gain.astype(jnp.float32).reshape(HEAD_COUNT, HEAD_DIM)
    heads_out = heads_out.astype(jnp.bfloat16).reshape(SEQUENCE_COUNT * SEQUENCE_LENGTH, ATTN)
    mass_log = jnp.log(jnp.maximum(weight_mass, mass_floor))
    gated_rows = (conv_values.astype(jnp.float32) * jax.nn.sigmoid(conv_gates.astype(jnp.float32))).astype(jnp.bfloat16)
    gated_rows = gated_rows.reshape(SEQUENCE_COUNT, SEQUENCE_LENGTH, CONV)
    padded = jnp.pad(gated_rows.astype(jnp.float32), ((0, 0), (KERNEL - 1, 0), (0, 0)))
    tap_values = filter_taps.astype(jnp.float32)
    filtered = jnp.zeros((SEQUENCE_COUNT, SEQUENCE_LENGTH, CONV), jnp.float32)
    for tap_index in range(KERNEL):
        filtered = filtered + padded[:, tap_index:tap_index + SEQUENCE_LENGTH] * tap_values[tap_index]
    center = lax.optimization_barrier(jnp.mean(filtered, axis=-1, keepdims=True))
    deviation = filtered - center
    spread = lax.optimization_barrier(jnp.mean(deviation * deviation, axis=-1, keepdims=True))
    conv_out = jax.nn.silu(deviation * lax.rsqrt(spread + norm_eps) * channel_gain.astype(jnp.float32) + channel_shift.astype(jnp.float32)).astype(jnp.bfloat16)
    conv_out = conv_out.reshape(SEQUENCE_COUNT * SEQUENCE_LENGTH, CONV)
    mixed_out = jnp.dot(heads_out, attend_out, preferred_element_type=jnp.float32)
    mixed_out = mixed_out + jnp.dot(conv_out, filter_out, preferred_element_type=jnp.float32)
    return (mixed_out.astype(jnp.bfloat16).reshape(SEQUENCE_COUNT, SEQUENCE_LENGTH, D), mass_log)
```

```python
import functools

import jax
import jax.numpy as jnp
from jax import lax
from jax.experimental import pallas as pl
from jax.experimental.pallas import tpu as pltpu
from jax.sharding import PartitionSpec as P

HEAD_DIM = 64

rms_eps = 1e-06
norm_eps = 1e-05
mass_floor = 0.01
HALO = 32
LANES = 128
LOG2E = 1.4426950408889634
MESH = pl.DeviceIdType.MESH


def kernel(
    n, tp, taps, total_channels,
    stream_hbm, ngain, offs, raw_taps, gain_ref, cgain_ref, cshift_ref,
    q_hbm, k_hbm, v_hbm, in_hbm, gate_hbm, attend_hbm, filter_hbm,
    out_ref, log_ref,
    stream, normed, weights, out_weights, packet, q_in, kv_in, offs_in, o_out, o_in, stat_out, stat_in,
    own_r, own_t, far_r, far_t, masses, off_rows, tap_ref, heads_ref, conv_ref, conv_share, leaving, arrived_ref,
    gated, halo, ext, filt, stats, stats_got,
    stream_sem, weight_sem, out_weight_sem, q_send, q_recv, kv_send, kv_recv, offs_send, offs_recv,
    o_send, o_recv, stat_send, stat_recv, out_send, out_recv, halo_send, halo_recv, chan_send, chan_recv,
):
    f32, bf16 = jnp.float32, jnp.bfloat16
    me = lax.axis_index("sp")
    core = lax.axis_index("tp")
    partner = 1 - core
    rows, model = normed.shape
    chans = in_hbm.shape[1]
    groups = packet.shape[1]
    slabs = chans // LANES
    lane = lax.broadcasted_iota(jnp.int32, (rows, LANES), 1)
    low = lane < HEAD_DIM

    def local_copy(src, dst, sem):
        return pltpu.make_async_copy(src, dst, sem)

    def send(src, dst, send_sem, recv_sem, to):
        return pltpu.make_async_remote_copy(
            src_ref=src, dst_ref=dst, send_sem=send_sem, recv_sem=recv_sem,
            device_id=to, device_id_type=MESH)

    projections = (q_hbm, k_hbm, v_hbm)
    first_order, other_order = (1, 2, 0), (0, 1, 2)

    def slot_of(t):
        return jnp.where(me == 0, first_order[t], other_order[t])

    def fetch(t):
        @pl.when(me == 0)
        def _():
            s = first_order[t]
            local_copy(projections[s], weights.at[s], weight_sem.at[s]).start()

        @pl.when(me != 0)
        def _():
            s = other_order[t]
            local_copy(projections[s], weights.at[s], weight_sem.at[s]).start()

    stream_copy = local_copy(stream_hbm, stream, stream_sem)
    gate_copies = [local_copy(w, weights.at[3 + t], weight_sem.at[3 + t]) for t, w in enumerate((in_hbm, gate_hbm))]
    out_copies = [local_copy(w, out_weights.at[t], out_weight_sem.at[t]) for t, w in enumerate((filter_hbm, attend_hbm))]
    stream_copy.start()
    fetch(0)
    fetch(1)

    barrier = pltpu.get_barrier_semaphore()
    peers = {0: (1,), 1: (0, 2, 3), 2: (1, 3), 3: (1, 2)}
    pl.semaphore_signal(barrier, inc=1, device_id={"tp": partner}, device_id_type=MESH)
    for d in range(n):
        @pl.when(me == d)
        def _(d=d):
            for p in peers[d]:
                pl.semaphore_signal(barrier, inc=1, device_id={"sp": p}, device_id_type=MESH)

    tap_ref[...] = jnp.zeros_like(tap_ref)
    for c in range(slabs):
        tap_ref[c, :taps] = raw_taps[:, c * LANES:(c + 1) * LANES].astype(f32)
    off_rows[0] = offs[...].astype(f32) * LOG2E
    masses[...] = jnp.zeros_like(masses)
    norm_gain = ngain[...].astype(f32).reshape(1, -1)
    band = min(64, rows)
    stream_copy.wait()

    @pl.loop(0, rows // band)
    def _(c):
        some = pl.ds(pl.multiple_of(c * band, band), band)
        x = stream[some, :].astype(f32)
        x = x * lax.rsqrt(jnp.mean(x * x, axis=-1, keepdims=True) + rms_eps)
        normed[some, :] = (x * norm_gain).astype(bf16)

    for d in range(n):
        @pl.when(me == d)
        def _(d=d):
            pl.semaphore_wait(barrier, len(peers[d]) + tp - 1)

    def q_copy(src_dev, dst_dev, g):
        return send(packet.at[0, g], q_in.at[src_dev - 2, g], q_send.at[dst_dev - 1, g],
                    q_recv.at[src_dev - 2, g], {"sp": dst_dev})

    def kv_copy(t, g):
        return send(packet.at[1 + t, g], kv_in.at[t, g], kv_send.at[t, g], kv_recv.at[t, g], {"sp": 1})

    offs_copy = send(offs, offs_in, offs_send, offs_recv, {"sp": 1})

    def o_copy(src_dev, dst_dev, g):
        return send(o_out.at[dst_dev - 2, g], o_in.at[src_dev - 1, g], o_send.at[dst_dev - 2, g],
                    o_recv.at[src_dev - 1, g], {"sp": dst_dev})

    def stat_copy(src_dev, dst_dev):
        return send(stat_out.at[dst_dev - 2], stat_in.at[src_dev - 1], stat_send.at[dst_dev - 2],
                    stat_recv.at[src_dev - 1], {"sp": dst_dev})

    @pl.when(me == 0)
    def _():
        offs_copy.start()

    wide = 2 * LANES
    halves = chans // wide

    def project(t, after):
        slot = slot_of(t)
        local_copy(q_hbm, weights.at[slot], weight_sem.at[slot]).wait()
        factor = jnp.where(slot == 0, LOG2E * HEAD_DIM ** (-0.5), 1.0).astype(f32)
        for half in range(halves):
            y = jnp.dot(normed[...], weights[slot, :, half * wide:(half + 1) * wide], preferred_element_type=f32)
            y = (y * factor).astype(bf16)
            for u in range(2):
                packet[slot, 2 * half + u] = y[:, u * LANES:(u + 1) * LANES]
            after(half)

    def after_first(half):
        @pl.when(me == 2)
        def _():
            for u in range(2):
                q_copy(2, 1, 2 * half + u).start()

        @pl.when(me == 3)
        def _():
            for u in range(2):
                q_copy(3, 1, 2 * half + u).start()
                q_copy(3, 2, 2 * half + u).start()

        if half == 0:
            @pl.when(me == 0)
            def _():
                kv_copy(0, 0).start()

    def after_second(half):
        if half == 0:
            @pl.when(me == 0)
            def _():
                kv_copy(1, 0).start()

    for copy in gate_copies:
        copy.start()
    project(0, after_first)
    fetch(2)
    project(1, after_second)
    for copy in out_copies:
        copy.start()
    for copy in gate_copies:
        copy.wait()

    @pl.loop(0, halves)
    def _(c):
        cols = pl.ds(pl.multiple_of(c * wide, wide), wide)
        x = normed[...]
        value = jnp.dot(x, weights[3, :, cols], preferred_element_type=f32).astype(bf16).astype(f32)
        gate = jnp.dot(x, weights[4, :, cols], preferred_element_type=f32).astype(bf16).astype(f32)
        g = (value * jax.nn.sigmoid(gate)).astype(bf16)
        gated[:, cols] = g[rows - HALO:]
        g = g.astype(f32)
        for u in range(2):
            ext[2 * c + u, HALO:, :] = g[:, u * LANES:(u + 1) * LANES]

    halo_copy = send(gated, halo, halo_send, halo_recv, {"sp": lax.rem(me + 1, n)})

    @pl.when(me < n - 1)
    def _():
        halo_copy.start()

    @pl.when(me == 0)
    def _():
        for g in range(1, groups):
            for t in range(2):
                if g == 1:
                    kv_copy(t, g).start()

    def after_third(half):
        pass

    project(2, after_third)

    @pl.when(me == 0)
    def _():
        for g in range(2, groups):
            for t in range(2):
                kv_copy(t, g).start()

    step = min(128, rows)

    def convolve(starts):
        @pl.loop(0, slabs)
        def _(c):
            for r0 in starts:
                acc = jnp.zeros((step, LANES), f32)
                for k in range(taps):
                    start = HALO - (taps - 1) + k + r0
                    acc = acc + ext[c, start:start + step, :] * tap_ref[c, k:k + 1, :]
                filt[c, r0:r0 + step, :] = acc

    chan_copy = send(stats, stats_got, chan_send, chan_recv, {"tp": partner})

    def convolve_first():
        @pl.when(me > 0)
        def _():
            halo_copy.wait_recv()
            for c in range(slabs):
                ext[c, :HALO, :] = halo[:, c * LANES:(c + 1) * LANES].astype(f32)

        @pl.when(me == 0)
        def _():
            for c in range(slabs):
                ext[c, :HALO, :] = jnp.zeros((HALO, LANES), f32)

        convolve([0])
        total = filt[0]
        for c in range(1, slabs):
            total = total + filt[c]
        lsum = jnp.sum(total, axis=1, keepdims=True)
        mean = lsum * (1.0 / chans)
        square = jnp.zeros((rows, LANES), f32)
        for c in range(slabs):
            dev = filt[c] - mean
            square = square + dev * dev
        lsq = jnp.sum(square, axis=1, keepdims=True)
        stats[...] = jnp.where(low, lsum, lsq)
        chan_copy.start()

    def channel_norm():
        chan_copy.wait()
        mine, other = stats[...], stats_got[...]
        mean = (mine[:, 0:1] + other[:, 0:1]) * (1.0 / total_channels)
        spread = jnp.zeros((rows, 1), f32)
        for s in (mine, other):
            apart = s[:, 0:1] * (1.0 / chans) - mean
            spread = spread + s[:, HEAD_DIM:HEAD_DIM + 1] + chans * apart * apart
        scale = lax.rsqrt(spread * (1.0 / total_channels) + norm_eps)
        for c in range(slabs):
            cols = slice(c * LANES, (c + 1) * LANES)
            y = (filt[c] - mean) * scale * cgain_ref[cols].astype(f32).reshape(1, -1) + cshift_ref[cols].astype(f32).reshape(1, -1)
            conv_ref[:, cols] = (y * jax.nn.sigmoid(y)).astype(bf16)

    tile = min(512, model)

    def conv_product():
        out_copies[0].wait()
        for c in range(0, model, tile):
            conv_share[:, c:c + tile] = jnp.dot(
                conv_ref[...], out_weights[0, :, c:c + tile], preferred_element_type=f32)

    ri = lax.broadcasted_iota(jnp.int32, (rows, rows), 0)
    ci = lax.broadcasted_iota(jnp.int32, (rows, rows), 1)
    tri = (ri >= ci).astype(bf16)

    def split_keys(k):
        zero = jnp.zeros_like(k)
        return jnp.where(low, k, zero), jnp.where(low, zero, k)

    def split_values(v):
        one = jnp.ones_like(v)
        return jnp.where(low, v, one), jnp.where(low, one, v)

    def attend(q, k, v, off, strict=None):
        z = lax.dot_general(q, k, (((1,), (1,)), ((), ())), preferred_element_type=f32) + off
        lose = jnp.maximum(z, jnp.log(1.0 + jnp.exp2(jnp.minimum(z, 100.0))) * LOG2E)
        if strict is not None:
            lose = jnp.where(strict, lose, 0.0)
        cum = jnp.dot(lose.astype(bf16), tri, preferred_element_type=f32)
        w = jnp.exp2(z - cum)
        if strict is not None:
            w = jnp.where(strict, w, 0.0)
        res = jnp.dot(w.astype(bf16), v, preferred_element_type=f32)
        return res, jnp.broadcast_to(cum[:, 0:1], (rows, LANES))

    def note(which, g, h, res, total):
        base = 0 if h else HEAD_DIM
        masses[which] = jnp.where(lane == base + g, res, jnp.where(lane == base + 4 + g, total, masses[which]))

    def pair(a, b):
        return jnp.where(low, a, b)

    @pl.loop(0, groups)
    def _(g):
        keys = split_keys(packet[1, g])
        values = split_values(packet[2, g])
        strict = ci < ri
        for h in range(2):
            res, total = attend(packet[0, g], keys[h], values[h], off_rows[0, pl.ds(2 * g + h, 1), :], strict)
            own_r[g, h] = res
            own_t[g, h] = jnp.exp2(-total)
            note(0, g, h, res, total)

        @pl.when(me == 1)
        def _():
            keys = split_keys(packet[1, g])
            values = split_values(packet[2, g])
            for i in (1, 0):
                send(packet.at[0, g], q_in.at[i, g], q_send.at[0, g], q_recv.at[i, g], {"sp": i + 2}).wait_recv()
                for h in range(2):
                    res, total = attend(q_in[i, g], keys[h], values[h], off_rows[0, pl.ds(2 * g + h, 1), :])
                    far_r[i, h] = res
                    far_t[i, h] = jnp.exp2(-total)

        @pl.when(me == 2)
        def _():
            keys = split_keys(packet[1, g])
            values = split_values(packet[2, g])
            send(packet.at[0, g], q_in.at[1, g], q_send.at[0, g], q_recv.at[1, g], {"sp": 3}).wait_recv()
            parts = []
            for h in range(2):
                res, total = attend(q_in[1, g], keys[h], values[h], off_rows[0, pl.ds(2 * g + h, 1), :])
                note(2, g, h, res, total)
                parts.append(res)
            o_out[1, g] = pair(*parts).astype(bf16)
            send(o_out.at[1, g], o_in.at[1, g], o_send.at[1, g], o_recv.at[1, g], {"sp": 3}).start()

        @pl.when(g == 0)
        def _():
            convolve(range(step, rows, step))

        @pl.when(g == 1)
        def _():
            convolve_first()

        @pl.when(g == 2)
        def _():
            channel_norm()

        @pl.when(g == 3)
        def _():
            conv_product()

        @pl.when(me == 1)
        def _():
            @pl.when(g == 0)
            def _():
                send(offs, offs_in, offs_send, offs_recv, {"sp": 0}).wait_recv()
                off_rows[1] = offs_in[...].astype(f32) * LOG2E

            for t in range(2):
                send(packet.at[1 + t, g], kv_in.at[t, g], kv_send.at[t, g], kv_recv.at[t, g], {"sp": 0}).wait_recv()
            keys = split_keys(kv_in[0, g])
            values = split_values(kv_in[1, g])
            for i in (1, 0):
                parts = []
                for h in range(2):
                    res, _ = attend(q_in[i, g], keys[h], values[h], off_rows[1, pl.ds(2 * g + h, 1), :])
                    res = far_r[i, h] + far_t[i, h] * res
                    note(1 + i, g, h, res, res)
                    parts.append(res)
                o_out[i, g] = pair(*parts).astype(bf16)
                send(o_out.at[i, g], o_in.at[0, g], o_send.at[i, g], o_recv.at[0, g], {"sp": i + 2}).start()
            for h in range(2):
                res, _ = attend(packet[0, g], keys[h], values[h], off_rows[1, pl.ds(2 * g + h, 1), :])
                res = own_r[g, h] + own_t[g, h] * res
                own_r[g, h] = res
                note(0, g, h, res, res)

    def stat_rows(which):
        t = jnp.transpose(masses[which])
        return jnp.concatenate([t[0:8], t[HEAD_DIM:HEAD_DIM + 8]], axis=0)

    @pl.when(me == 1)
    def _():
        for i in (1, 0):
            stat_out[i] = stat_rows(1 + i)
            stat_copy(1, i + 2).start()

    @pl.when(me == 2)
    def _():
        stat_out[1] = stat_rows(2)
        stat_copy(2, 3).start()

    blocks = (lax.broadcasted_iota(jnp.int32, (LANES, LANES), 0) // HEAD_DIM
              == lax.broadcasted_iota(jnp.int32, (LANES, LANES), 1) // HEAD_DIM).astype(bf16)

    @pl.when(me == 3)
    def _():
        stat_copy(2, 3).wait_recv()
        rest = jnp.zeros((LANES - 16, rows), f32)
        far_t[0, 0] = jnp.transpose(jnp.concatenate([stat_in[1], rest], axis=0))

    def finish(g):
        cols = slice(g * LANES, (g + 1) * LANES)

        def close(o):
            sq = jnp.dot((o * o).astype(bf16), blocks, preferred_element_type=f32)
            gain = gain_ref[cols].astype(f32).reshape(1, LANES)
            heads_ref[:, cols] = (o * lax.rsqrt(sq * (1.0 / HEAD_DIM) + rms_eps) * gain).astype(bf16)

        own = pair(own_r[g, 0], own_r[g, 1])

        @pl.when(me < 2)
        def _():
            close(own)

        @pl.when(me == 2)
        def _():
            through = pair(own_t[g, 0], own_t[g, 1])
            o_copy(1, 2, g).wait_recv()
            close(own + through * o_in[0, g].astype(f32))

        @pl.when(me == 3)
        def _():
            through = pair(own_t[g, 0], own_t[g, 1])
            tot = far_t[0, 0]
            middle = jnp.exp2(-pair(tot[:, 12 + g:13 + g], tot[:, 4 + g:5 + g]))
            send(o_out.at[1, g], o_in.at[1, g], o_send.at[1, g], o_recv.at[1, g], {"sp": 2}).wait_recv()
            send(o_out.at[1, g], o_in.at[0, g], o_send.at[1, g], o_recv.at[0, g], {"sp": 1}).wait_recv()
            close(own + through * (o_in[1, g].astype(f32) + middle * o_in[0, g].astype(f32)))

    out_copies[1].wait()
    early = groups // 2
    for g in range(early):
        finish(g)
    cut = early * LANES
    for c in range(0, model, tile):
        conv_share[:, c:c + tile] += jnp.dot(
            heads_ref[:, :cut], out_weights[1, :cut, c:c + tile], preferred_element_type=f32)
    for g in range(early, groups):
        finish(g)
    share = rows // tp
    theirs = pl.ds(pl.multiple_of(partner * share, share), share)
    ours = pl.ds(pl.multiple_of(core * share, share), share)
    leaves = []
    for c in range(0, model, tile):
        cols = slice(c, c + tile)
        leaving[:, cols] = (conv_share[theirs, cols] + jnp.dot(
            heads_ref[theirs, cut:], out_weights[1, cut:, cols], preferred_element_type=f32)).astype(bf16)
        copy = send(leaving.at[:, pl.ds(c, tile)], arrived_ref.at[:, pl.ds(c, tile)],
                    out_send.at[c // tile], out_recv.at[c // tile], {"tp": partner})
        copy.start()
        leaves.append(copy)

    mine = stat_rows(0)

    def write_log(m_odd, m_even):
        for g in range(groups):
            log_ref[2 * g:2 * g + 1] = jnp.log(jnp.maximum(m_even[g:g + 1], mass_floor))
            log_ref[2 * g + 1:2 * g + 2] = jnp.log(jnp.maximum(m_odd[g:g + 1], mass_floor))

    @pl.when(me < 2)
    def _():
        write_log(mine[0:4], mine[8:12])

    @pl.when(me == 2)
    def _():
        stat_copy(1, 2).wait_recv()
        far = stat_in[0]
        write_log(mine[0:4] + jnp.exp2(-mine[4:8]) * far[0:4], mine[8:12] + jnp.exp2(-mine[12:16]) * far[8:12])

    @pl.when(me == 3)
    def _():
        send(stat_out.at[1], stat_in.at[0], stat_send.at[1], stat_recv.at[0], {"sp": 1}).wait_recv()
        far, mid = stat_in[0], stat_in[1]
        odd = mid[0:4] + jnp.exp2(-mid[4:8]) * far[0:4]
        even = mid[8:12] + jnp.exp2(-mid[12:16]) * far[8:12]
        write_log(mine[0:4] + jnp.exp2(-mine[4:8]) * odd, mine[8:12] + jnp.exp2(-mine[12:16]) * even)

    for c in range(0, model, tile):
        cols = slice(c, c + tile)
        acc = conv_share[ours, cols] + jnp.dot(
            heads_ref[ours, cut:], out_weights[1, cut:, cols], preferred_element_type=f32)
        leaves[c // tile].wait()
        out_ref[:, cols] = (acc + arrived_ref[:, cols].astype(f32)).astype(bf16)

    @pl.when(me < n - 1)
    def _():
        halo_copy.wait_send()

    @pl.when(me == 0)
    def _():
        offs_copy.wait_send()
        for g in range(groups):
            for t in range(2):
                kv_copy(t, g).wait_send()

    @pl.when(me == 1)
    def _():
        for i in (1, 0):
            for g in range(groups):
                o_copy(1, i + 2, g).wait_send()
            stat_copy(1, i + 2).wait_send()

    @pl.when(me == 2)
    def _():
        for g in range(groups):
            q_copy(2, 1, g).wait_send()
            o_copy(2, 3, g).wait_send()
        stat_copy(2, 3).wait_send()

    @pl.when(me == 3)
    def _():
        for g in range(groups):
            q_copy(3, 1, g).wait_send()
            q_copy(3, 2, g).wait_send()


def place(mixed, mass_log, out_ref, log_ref, sem):
    copies = [
        pltpu.make_async_copy(mixed, out_ref, sem.at[0]),
        pltpu.make_async_copy(mass_log, log_ref, sem.at[1]),
    ]
    for copy in copies:
        copy.start()
    for copy in copies:
        copy.wait()


def local(n, tp,
    stream, norm_gain, query_weight, key_weight, value_weight, filter_input, filter_gate,
    score_offset, head_gain, filter_taps, channel_gain, channel_shift, attend_out, filter_out,
):
    f32, bf16 = jnp.float32, jnp.bfloat16
    rows = stream.shape[1]
    heads = score_offset.shape[2]
    groups = heads * HEAD_DIM // LANES
    chans = filter_input.shape[1]
    slabs = chans // LANES
    taps = filter_taps.shape[0]
    model = stream.shape[2]
    share = rows // tp
    tiles = model // min(512, model)

    vmem = pl.BlockSpec(memory_space=pltpu.VMEM)
    hbm = pl.BlockSpec(memory_space=pl.ANY)
    dma = pltpu.SemaphoreType.DMA
    mixed, mass_log = pl.pallas_call(
        functools.partial(kernel, n, tp, taps, chans * tp),
        out_shape=(
            jax.ShapeDtypeStruct((share, model), bf16),
            jax.ShapeDtypeStruct((heads, rows), f32),
        ),
        in_specs=[hbm] + [vmem] * 6 + [hbm] * 7,
        out_specs=(vmem,) * 2,
        scratch_shapes=[
            pltpu.VMEM((rows, model), bf16),
            pltpu.VMEM((rows, model), bf16),
            pltpu.VMEM((5, model, chans), bf16),
            pltpu.VMEM((2, chans, model), bf16),
            pltpu.VMEM((3, groups, rows, LANES), bf16),
            pltpu.VMEM((2, groups, rows, LANES), bf16),
            pltpu.VMEM((2, groups, rows, LANES), bf16),
            pltpu.VMEM((heads, rows), bf16),
            pltpu.VMEM((2, groups, rows, LANES), bf16),
            pltpu.VMEM((2, groups, rows, LANES), bf16),
            pltpu.VMEM((2, 16, rows), f32),
            pltpu.VMEM((2, 16, rows), f32),
            pltpu.VMEM((groups, 2, rows, LANES), f32),
            pltpu.VMEM((groups, 2, rows, LANES), f32),
            pltpu.VMEM((2, 2, rows, LANES), f32),
            pltpu.VMEM((2, 2, rows, LANES), f32),
            pltpu.VMEM((3, rows, LANES), f32),
            pltpu.VMEM((2, heads, rows), f32),
            pltpu.VMEM((slabs, taps + -taps % 8, LANES), f32),
            pltpu.VMEM((rows, heads * HEAD_DIM), bf16),
            pltpu.VMEM((rows, chans), bf16),
            pltpu.VMEM((rows, model), f32),
            pltpu.VMEM((share, model), bf16),
            pltpu.VMEM((share, model), bf16),
            pltpu.VMEM((HALO, chans), bf16),
            pltpu.VMEM((HALO, chans), bf16),
            pltpu.VMEM((slabs, HALO + rows, LANES), f32),
            pltpu.VMEM((slabs, rows, LANES), f32),
            pltpu.VMEM((rows, LANES), f32),
            pltpu.VMEM((rows, LANES), f32),
            dma, dma((5,)), dma((2,)), dma((2, groups)), dma((2, groups)), dma((2, groups)), dma((2, groups)), dma, dma,
            dma((2, groups)), dma((2, groups)), dma((2,)), dma((2,)), dma((tiles,)), dma((tiles,)), dma, dma, dma, dma,
        ],
        compiler_params=pltpu.CompilerParams(
            collective_id=0, has_side_effects=True, vmem_limit_bytes=56 * 1024 * 1024),
    )(stream[0], norm_gain, score_offset[0].T, filter_taps, head_gain, channel_gain, channel_shift,
      query_weight, key_weight, value_weight, filter_input, filter_gate, attend_out, filter_out)
    mixed, mass_log = pl.pallas_call(
        place,
        out_shape=(
            jax.ShapeDtypeStruct((share, model), bf16),
            jax.ShapeDtypeStruct((heads, rows), f32),
        ),
        in_specs=[vmem] * 2,
        out_specs=(hbm,) * 2,
        scratch_shapes=[dma((2,))],
    )(mixed, mass_log)
    return (mixed[None], mass_log.T[None])


def shifted(value, axis, steps):
    count = lax.axis_size(axis)
    first, last = (max(0, -steps), min(count, count - steps))
    return lax.ppermute(value, axis, [(source, source + steps) for source in range(first, last)])


def local_ring(
    stream,
    norm_gain,
    query_weight,
    key_weight,
    value_weight,
    filter_input,
    filter_gate,
    score_offset,
    head_gain,
    filter_taps,
    channel_gain,
    channel_shift,
    attend_out,
    filter_out,
):
    rows_here = stream.shape[1]
    total_channels = filter_input.shape[1] * lax.axis_size("tp")
    xfloat = stream[0].astype(jnp.float32)
    normed = xfloat * lax.rsqrt(jnp.mean(xfloat * xfloat, axis=-1, keepdims=True) + rms_eps)
    normed = (normed * norm_gain.astype(jnp.float32)).astype(jnp.bfloat16)

    def project(weight):
        return jnp.dot(normed, weight, preferred_element_type=jnp.float32).astype(jnp.bfloat16)

    queries = project(query_weight)
    keys_here = project(key_weight)
    values_here = project(value_weight)
    conv_in = project(filter_input)
    conv_gate = project(filter_gate)
    offsets_here = score_offset[0]
    heads_here = offsets_here.shape[1]
    first_pos = lax.axis_index("sp") * rows_here
    position = first_pos + jnp.arange(rows_here, dtype=jnp.int32)
    qheads = queries.reshape(rows_here, heads_here, HEAD_DIM)

    def absorb(state_now, kblock, vblock, oblock, first_key):
        attended, weight_mass, survive = state_now
        span = kblock.shape[0]
        kblock = kblock.reshape(span, heads_here, HEAD_DIM)
        vblock = vblock.reshape(span, heads_here, HEAD_DIM)
        scores = jnp.einsum(
            "thd,shd->hts", qheads, kblock, preferred_element_type=jnp.float32
        ) * HEAD_DIM ** (-0.5)
        scores = scores + oblock.astype(jnp.float32).T[:, None, :]
        key_pos = first_key + jnp.arange(span, dtype=jnp.int32)
        strict = ((key_pos[None, :] < position[:, None]) & (key_pos[None, :] >= 0))[None]
        losing = jnp.where(strict, jax.nn.log_sigmoid(-scores), 0.0)
        beyond = lax.cumsum(losing, axis=2, reverse=True) - losing + survive[:, :, None]
        weights = jnp.where(strict, jnp.exp(jax.nn.log_sigmoid(scores) + beyond), 0.0)
        weight_mass = weight_mass + jnp.sum(weights, axis=2)
        attended = attended + jnp.einsum(
            "hts,shd->thd", weights.astype(jnp.bfloat16), vblock, preferred_element_type=jnp.float32
        )
        survive = survive + jnp.sum(losing, axis=2)
        return (attended, weight_mass, survive)

    initial = (
        jnp.zeros((rows_here, heads_here, HEAD_DIM), jnp.float32),
        jnp.zeros((heads_here, rows_here), jnp.float32),
        jnp.zeros((heads_here, rows_here), jnp.float32),
    )
    state_now = absorb(initial, keys_here, values_here, offsets_here, first_pos)

    def pass_turn(turn_index, carried):
        state_now, travelling = carried
        travelling = shifted((travelling[0], travelling[1], travelling[2]), "sp", 1)
        first_key = first_pos - (turn_index + 1) * rows_here
        state_now = absorb(state_now, travelling[0], travelling[1], travelling[2], first_key)
        return (state_now, travelling)

    state_now, travelling = lax.fori_loop(
        0, lax.axis_size("sp") - 1, pass_turn, (state_now, (keys_here, values_here, offsets_here))
    )
    attended, weight_mass, survive = state_now
    head_scale = lax.rsqrt(jnp.mean(attended * attended, axis=-1, keepdims=True) + rms_eps)
    heads_flat = attended * head_scale * head_gain.astype(jnp.float32).reshape(heads_here, HEAD_DIM)
    heads_flat = heads_flat.astype(jnp.bfloat16).reshape(rows_here, heads_here * HEAD_DIM)
    mass_log = jnp.log(jnp.maximum(weight_mass.T, mass_floor))
    gated_rows = (
        conv_in.astype(jnp.float32) * jax.nn.sigmoid(conv_gate.astype(jnp.float32))
    ).astype(jnp.bfloat16)
    reach_back = filter_taps.shape[0] - 1
    earlier = shifted(gated_rows[rows_here - reach_back :], "sp", 1)
    extended = jnp.concatenate([earlier, gated_rows], axis=0).astype(jnp.float32)
    tap_values = filter_taps.astype(jnp.float32)
    filtered = jnp.zeros((rows_here, gated_rows.shape[1]), jnp.float32)
    for tap_index in range(reach_back + 1):
        filtered = filtered + extended[tap_index : tap_index + rows_here] * tap_values[tap_index]
    center = lax.psum(jnp.sum(filtered, axis=-1), "tp") / total_channels
    deviation = filtered - center[:, None]
    spread = lax.psum(jnp.sum(deviation * deviation, axis=-1), "tp") / total_channels
    conv_out = jax.nn.silu(
        deviation * lax.rsqrt(spread[:, None] + norm_eps) * channel_gain.astype(jnp.float32)
        + channel_shift.astype(jnp.float32)
    ).astype(jnp.bfloat16)
    mixed_out = lax.psum_scatter(
        (
            jnp.dot(heads_flat, attend_out, preferred_element_type=jnp.float32)
            + jnp.dot(conv_out, filter_out, preferred_element_type=jnp.float32)
        ).astype(jnp.bfloat16),
        "tp",
        scatter_dimension=0,
        tiled=True,
    )
    return (mixed_out[None], mass_log[None])


def solution(mesh):
    n, tp = mesh.shape["sp"], mesh.shape["tp"]

    def choose(*args):
        rows, heads, chans = args[0].shape[1], args[7].shape[2], args[5].shape[1]
        same = args[2].shape[1] == chans and heads * HEAD_DIM == 4 * LANES == chans
        if n == 4 and tp == 2 and same and rows % 128 == 0:
            return local(n, tp, *args)
        return local_ring(*args)

    return jax.shard_map(
        choose,
        mesh=mesh,
        in_specs=(
            P("fs", "sp", None), P(), P(None, "tp"), P(None, "tp"), P(None, "tp"),
            P(None, "tp"), P(None, "tp"), P("fs", "sp", "tp"), P("tp"), P(None, "tp"),
            P("tp"), P("tp"), P("tp", None), P("tp", None),
        ),
        out_specs=(P("fs", ("sp", "tp"), None), P("fs", "sp", "tp")),
        check_vma=False,
    )
```

```python
import functools

import jax
import jax.numpy as jnp
from jax import lax
from jax.experimental import pallas as pl
from jax.experimental.pallas import tpu as pltpu
from jax.sharding import PartitionSpec as P

HEAD_DIM = 64

rms_eps = 1e-06
norm_eps = 1e-05
mass_floor = 0.01
HALO = 32
LANES = 128
LOG2E = 1.4426950408889634
MESH = pl.DeviceIdType.MESH


def kernel(
    n, tp, taps, total_channels,
    stream_hbm, ngain, offs, raw_taps, gain_ref, cgain_ref, cshift_ref,
    q_hbm, k_hbm, v_hbm, in_hbm, gate_hbm, attend_hbm, filter_hbm,
    out_ref, log_ref,
    stream, normed, weights, out_weights, packet, q_in, kv_in, offs_in, o_out, o_in, stat_out, stat_in,
    own_r, own_t, far_r, far_t, masses, off_rows, tap_ref, heads_ref, conv_ref, conv_share, leaving, arrived_ref,
    gated, halo, ext, filt, stats, stats_got,
    stream_sem, weight_sem, out_weight_sem, q_send, q_recv, kv_send, kv_recv, offs_send, offs_recv,
    o_send, o_recv, stat_send, stat_recv, out_send, out_recv, halo_send, halo_recv, chan_send, chan_recv,
):
    f32, bf16 = jnp.float32, jnp.bfloat16
    me = lax.axis_index("sp")
    core = lax.axis_index("tp")
    partner = 1 - core
    rows, model = normed.shape
    chans = in_hbm.shape[1]
    groups = packet.shape[1]
    slabs = chans // LANES
    lane = lax.broadcasted_iota(jnp.int32, (rows, LANES), 1)
    low = lane < HEAD_DIM

    def local_copy(src, dst, sem):
        return pltpu.make_async_copy(src, dst, sem)

    def send(src, dst, send_sem, recv_sem, to):
        return pltpu.make_async_remote_copy(
            src_ref=src, dst_ref=dst, send_sem=send_sem, recv_sem=recv_sem,
            device_id=to, device_id_type=MESH)

    projections = (q_hbm, k_hbm, v_hbm)
    first_order, other_order = (1, 2, 0), (0, 1, 2)

    def slot_of(t):
        return jnp.where(me == 0, first_order[t], other_order[t])

    def fetch(t):
        @pl.when(me == 0)
        def _():
            s = first_order[t]
            local_copy(projections[s], weights.at[s], weight_sem.at[s]).start()

        @pl.when(me != 0)
        def _():
            s = other_order[t]
            local_copy(projections[s], weights.at[s], weight_sem.at[s]).start()

    stream_copy = local_copy(stream_hbm, stream, stream_sem)
    gate_copies = [local_copy(w, weights.at[3 + t], weight_sem.at[3 + t]) for t, w in enumerate((in_hbm, gate_hbm))]
    out_copies = [local_copy(w, out_weights.at[t], out_weight_sem.at[t]) for t, w in enumerate((filter_hbm, attend_hbm))]
    stream_copy.start()
    fetch(0)
    fetch(1)

    barrier = pltpu.get_barrier_semaphore()
    peers = {0: (1,), 1: (0, 2, 3), 2: (1, 3), 3: (1, 2)}
    pl.semaphore_signal(barrier, inc=1, device_id={"tp": partner}, device_id_type=MESH)
    for d in range(n):
        @pl.when(me == d)
        def _(d=d):
            for p in peers[d]:
                pl.semaphore_signal(barrier, inc=1, device_id={"sp": p}, device_id_type=MESH)

    tap_ref[...] = jnp.zeros_like(tap_ref)
    for c in range(slabs):
        tap_ref[c, :taps] = raw_taps[:, c * LANES:(c + 1) * LANES].astype(f32)
    off_rows[0] = offs[...].astype(f32) * LOG2E
    masses[...] = jnp.zeros_like(masses)
    norm_gain = ngain[...].astype(f32).reshape(1, -1)
    band = min(64, rows)
    stream_copy.wait()

    @pl.loop(0, rows // band)
    def _(c):
        some = pl.ds(pl.multiple_of(c * band, band), band)
        x = stream[some, :].astype(f32)
        x = x * lax.rsqrt(jnp.mean(x * x, axis=-1, keepdims=True) + rms_eps)
        normed[some, :] = (x * norm_gain).astype(bf16)

    for d in range(n):
        @pl.when(me == d)
        def _(d=d):
            pl.semaphore_wait(barrier, len(peers[d]) + tp - 1)

    def q_copy(src_dev, dst_dev, g):
        return send(packet.at[0, g], q_in.at[src_dev - 2, g], q_send.at[dst_dev - 1, g],
                    q_recv.at[src_dev - 2, g], {"sp": dst_dev})

    def kv_copy(t, g):
        return send(packet.at[1 + t, g], kv_in.at[t, g], kv_send.at[t, g], kv_recv.at[t, g], {"sp": 1})

    offs_copy = send(offs, offs_in, offs_send, offs_recv, {"sp": 1})

    def o_copy(src_dev, dst_dev, g):
        return send(o_out.at[dst_dev - 2, g], o_in.at[src_dev - 1, g], o_send.at[dst_dev - 2, g],
                    o_recv.at[src_dev - 1, g], {"sp": dst_dev})

    def stat_copy(src_dev, dst_dev):
        return send(stat_out.at[dst_dev - 2], stat_in.at[src_dev - 1], stat_send.at[dst_dev - 2],
                    stat_recv.at[src_dev - 1], {"sp": dst_dev})

    @pl.when(me == 0)
    def _():
        offs_copy.start()

    wide = 2 * LANES
    halves = chans // wide

    def project(t, after):
        slot = slot_of(t)
        local_copy(q_hbm, weights.at[slot], weight_sem.at[slot]).wait()
        factor = jnp.where(slot == 0, LOG2E * HEAD_DIM ** (-0.5), 1.0).astype(f32)
        for half in range(halves):
            y = jnp.dot(normed[...], weights[slot, :, half * wide:(half + 1) * wide], preferred_element_type=f32)
            y = (y * factor).astype(bf16)
            for u in range(2):
                packet[slot, 2 * half + u] = y[:, u * LANES:(u + 1) * LANES]
            after(half)

    def after_first(half):
        @pl.when(me == 2)
        def _():
            for u in range(2):
                q_copy(2, 1, 2 * half + u).start()

        @pl.when(me == 3)
        def _():
            for u in range(2):
                q_copy(3, 1, 2 * half + u).start()
                q_copy(3, 2, 2 * half + u).start()

        if half == 0:
            @pl.when(me == 0)
            def _():
                kv_copy(0, 0).start()

    def after_second(half):
        if half == 0:
            @pl.when(me == 0)
            def _():
                kv_copy(1, 0).start()

    for copy in gate_copies:
        copy.start()
    project(0, after_first)
    fetch(2)
    project(1, after_second)
    for copy in out_copies:
        copy.start()
    for copy in gate_copies:
        copy.wait()

    @pl.loop(0, halves)
    def _(c):
        cols = pl.ds(pl.multiple_of(c * wide, wide), wide)
        x = normed[...]
        value = jnp.dot(x, weights[3, :, cols], preferred_element_type=f32).astype(bf16).astype(f32)
        gate = jnp.dot(x, weights[4, :, cols], preferred_element_type=f32).astype(bf16).astype(f32)
        g = (value * jax.nn.sigmoid(gate)).astype(bf16)
        gated[:, cols] = g[rows - HALO:]
        g = g.astype(f32)
        for u in range(2):
            ext[2 * c + u, HALO:, :] = g[:, u * LANES:(u + 1) * LANES]

    halo_copy = send(gated, halo, halo_send, halo_recv, {"sp": lax.rem(me + 1, n)})

    @pl.when(me < n - 1)
    def _():
        halo_copy.start()

    @pl.when(me == 0)
    def _():
        for g in range(1, groups):
            for t in range(2):
                if g == 1:
                    kv_copy(t, g).start()

    def after_third(half):
        pass

    project(2, after_third)

    @pl.when(me == 0)
    def _():
        for g in range(2, groups):
            for t in range(2):
                kv_copy(t, g).start()

    step = min(128, rows)

    def convolve(starts):
        @pl.loop(0, slabs)
        def _(c):
            for r0 in starts:
                acc = jnp.zeros((step, LANES), f32)
                for k in range(taps):
                    start = HALO - (taps - 1) + k + r0
                    acc = acc + ext[c, start:start + step, :] * tap_ref[c, k:k + 1, :]
                filt[c, r0:r0 + step, :] = acc

    chan_copy = send(stats, stats_got, chan_send, chan_recv, {"tp": partner})

    def convolve_first():
        @pl.when(me > 0)
        def _():
            halo_copy.wait_recv()
            for c in range(slabs):
                ext[c, :HALO, :] = halo[:, c * LANES:(c + 1) * LANES].astype(f32)

        @pl.when(me == 0)
        def _():
            for c in range(slabs):
                ext[c, :HALO, :] = jnp.zeros((HALO, LANES), f32)

        convolve([0])
        total = filt[0]
        for c in range(1, slabs):
            total = total + filt[c]
        lsum = jnp.sum(total, axis=1, keepdims=True)
        mean = lsum * (1.0 / chans)
        square = jnp.zeros((rows, LANES), f32)
        for c in range(slabs):
            dev = filt[c] - mean
            square = square + dev * dev
        lsq = jnp.sum(square, axis=1, keepdims=True)
        stats[...] = jnp.where(low, lsum, lsq)
        chan_copy.start()

    def channel_norm():
        chan_copy.wait()
        mine, other = stats[...], stats_got[...]
        mean = (mine[:, 0:1] + other[:, 0:1]) * (1.0 / total_channels)
        spread = jnp.zeros((rows, 1), f32)
        for s in (mine, other):
            apart = s[:, 0:1] * (1.0 / chans) - mean
            spread = spread + s[:, HEAD_DIM:HEAD_DIM + 1] + chans * apart * apart
        scale = lax.rsqrt(spread * (1.0 / total_channels) + norm_eps)
        for c in range(slabs):
            cols = slice(c * LANES, (c + 1) * LANES)
            y = (filt[c] - mean) * scale * cgain_ref[cols].astype(f32).reshape(1, -1) + cshift_ref[cols].astype(f32).reshape(1, -1)
            conv_ref[:, cols] = (y * jax.nn.sigmoid(y)).astype(bf16)

    tile = min(512, model)

    def conv_product():
        out_copies[0].wait()
        for c in range(0, model, tile):
            conv_share[:, c:c + tile] = jnp.dot(
                conv_ref[...], out_weights[0, :, c:c + tile], preferred_element_type=f32)

    ri = lax.broadcasted_iota(jnp.int32, (rows, rows), 0)
    ci = lax.broadcasted_iota(jnp.int32, (rows, rows), 1)
    tri = (ri >= ci).astype(bf16)

    def split_keys(k):
        zero = jnp.zeros_like(k)
        return jnp.where(low, k, zero), jnp.where(low, zero, k)

    def split_values(v):
        one = jnp.ones_like(v)
        return jnp.where(low, v, one), jnp.where(low, one, v)

    strict = ci < ri

    def attend(blocks_q, k, v, off, own_first):
        q = jnp.concatenate(blocks_q, axis=0)
        z = lax.dot_general(q, k, (((1,), (1,)), ((), ())), preferred_element_type=f32) + off
        lose = jnp.maximum(z, jnp.log(1.0 + jnp.exp2(jnp.minimum(z, 100.0))) * LOG2E)

        def masked(x):
            if not own_first:
                return x
            head = jnp.where(strict, x[:rows], 0.0)
            return jnp.concatenate([head, x[rows:]], axis=0) if len(blocks_q) > 1 else head

        cum = jnp.dot(masked(lose).astype(bf16), tri, preferred_element_type=f32)
        w = masked(jnp.exp2(z - cum))
        res = jnp.dot(w.astype(bf16), v, preferred_element_type=f32)
        pieces = []
        for r in range(len(blocks_q)):
            some = slice(r * rows, (r + 1) * rows)
            pieces.append((res[some], jnp.broadcast_to(cum[some, 0:1], (rows, LANES))))
        return pieces

    def note(which, g, h, res, total):
        base = 0 if h else HEAD_DIM
        masses[which] = jnp.where(lane == base + g, res, jnp.where(lane == base + 4 + g, total, masses[which]))

    def pair(a, b):
        return jnp.where(low, a, b)

    def near_blocks(g, others):
        keys = split_keys(packet[1, g])
        values = split_values(packet[2, g])
        rest = []
        for h in range(2):
            first, *more = attend([packet[0, g]] + others, keys[h], values[h], off_rows[0, pl.ds(2 * g + h, 1), :], True)
            res, total = first
            own_r[g, h] = res
            own_t[g, h] = jnp.exp2(-total)
            note(0, g, h, res, total)
            rest.append(more)
        return rest

    @pl.loop(0, groups)
    def _(g):
        @pl.when(((me == 0) | (me == 3)) & (g % 2 == 0))
        def _():
            for u in range(2):
                near_blocks(g + u, [])

        @pl.when(me == 1)
        def _():
            for i in (1, 0):
                send(packet.at[0, g], q_in.at[i, g], q_send.at[0, g], q_recv.at[i, g], {"sp": i + 2}).wait_recv()
            rest = near_blocks(g, [q_in[1, g], q_in[0, g]])
            for h in range(2):
                for i in (1, 0):
                    res, total = rest[h][1 - i]
                    far_r[i, h] = res
                    far_t[i, h] = jnp.exp2(-total)

        @pl.when(me == 2)
        def _():
            send(packet.at[0, g], q_in.at[1, g], q_send.at[0, g], q_recv.at[1, g], {"sp": 3}).wait_recv()
            rest = near_blocks(g, [q_in[1, g]])
            for h in range(2):
                note(2, g, h, *rest[h][0])
            o_out[1, g] = pair(rest[0][0][0], rest[1][0][0]).astype(bf16)
            send(o_out.at[1, g], o_in.at[1, g], o_send.at[1, g], o_recv.at[1, g], {"sp": 3}).start()

        @pl.when(g == 0)
        def _():
            convolve(range(step, rows, step))

        @pl.when(g == 1)
        def _():
            convolve_first()

        @pl.when(g == 2)
        def _():
            channel_norm()

        @pl.when(g == 3)
        def _():
            conv_product()

        @pl.when(me == 1)
        def _():
            @pl.when(g == 0)
            def _():
                send(offs, offs_in, offs_send, offs_recv, {"sp": 0}).wait_recv()
                off_rows[1] = offs_in[...].astype(f32) * LOG2E

            for t in range(2):
                send(packet.at[1 + t, g], kv_in.at[t, g], kv_send.at[t, g], kv_recv.at[t, g], {"sp": 0}).wait_recv()
            keys = split_keys(kv_in[0, g])
            values = split_values(kv_in[1, g])
            parts = [[], []]
            for h in range(2):
                pieces = attend([q_in[1, g], q_in[0, g], packet[0, g]], keys[h], values[h],
                                off_rows[1, pl.ds(2 * g + h, 1), :], False)
                for i in (1, 0):
                    res = far_r[i, h] + far_t[i, h] * pieces[1 - i][0]
                    note(1 + i, g, h, res, res)
                    parts[i].append(res)
                res = own_r[g, h] + own_t[g, h] * pieces[2][0]
                own_r[g, h] = res
                note(0, g, h, res, res)
            for i in (1, 0):
                o_out[i, g] = pair(*parts[i]).astype(bf16)
            for i in (1, 0):
                send(o_out.at[i, g], o_in.at[0, g], o_send.at[i, g], o_recv.at[0, g], {"sp": i + 2}).start()

    def stat_rows(which):
        t = jnp.transpose(masses[which])
        return jnp.concatenate([t[0:8], t[HEAD_DIM:HEAD_DIM + 8]], axis=0)

    @pl.when(me == 1)
    def _():
        for i in (1, 0):
            stat_out[i] = stat_rows(1 + i)
            stat_copy(1, i + 2).start()

    @pl.when(me == 2)
    def _():
        stat_out[1] = stat_rows(2)
        stat_copy(2, 3).start()

    blocks = (lax.broadcasted_iota(jnp.int32, (LANES, LANES), 0) // HEAD_DIM
              == lax.broadcasted_iota(jnp.int32, (LANES, LANES), 1) // HEAD_DIM).astype(bf16)

    @pl.when(me == 3)
    def _():
        stat_copy(2, 3).wait_recv()
        rest = jnp.zeros((LANES - 16, rows), f32)
        far_t[0, 0] = jnp.transpose(jnp.concatenate([stat_in[1], rest], axis=0))

    def finish(g):
        cols = slice(g * LANES, (g + 1) * LANES)

        def close(o):
            sq = jnp.dot((o * o).astype(bf16), blocks, preferred_element_type=f32)
            gain = gain_ref[cols].astype(f32).reshape(1, LANES)
            heads_ref[:, cols] = (o * lax.rsqrt(sq * (1.0 / HEAD_DIM) + rms_eps) * gain).astype(bf16)

        own = pair(own_r[g, 0], own_r[g, 1])

        @pl.when(me < 2)
        def _():
            close(own)

        @pl.when(me == 2)
        def _():
            through = pair(own_t[g, 0], own_t[g, 1])
            o_copy(1, 2, g).wait_recv()
            close(own + through * o_in[0, g].astype(f32))

        @pl.when(me == 3)
        def _():
            through = pair(own_t[g, 0], own_t[g, 1])
            tot = far_t[0, 0]
            middle = jnp.exp2(-pair(tot[:, 12 + g:13 + g], tot[:, 4 + g:5 + g]))
            send(o_out.at[1, g], o_in.at[1, g], o_send.at[1, g], o_recv.at[1, g], {"sp": 2}).wait_recv()
            send(o_out.at[1, g], o_in.at[0, g], o_send.at[1, g], o_recv.at[0, g], {"sp": 1}).wait_recv()
            close(own + through * (o_in[1, g].astype(f32) + middle * o_in[0, g].astype(f32)))

    out_copies[1].wait()
    early = groups // 2
    for g in range(early):
        finish(g)
    cut = early * LANES
    for c in range(0, model, tile):
        conv_share[:, c:c + tile] += jnp.dot(
            heads_ref[:, :cut], out_weights[1, :cut, c:c + tile], preferred_element_type=f32)
    for g in range(early, groups):
        finish(g)
    share = rows // tp
    theirs = pl.ds(pl.multiple_of(partner * share, share), share)
    ours = pl.ds(pl.multiple_of(core * share, share), share)
    leaves = []
    for c in range(0, model, tile):
        cols = slice(c, c + tile)
        leaving[:, cols] = (conv_share[theirs, cols] + jnp.dot(
            heads_ref[theirs, cut:], out_weights[1, cut:, cols], preferred_element_type=f32)).astype(bf16)
        copy = send(leaving.at[:, pl.ds(c, tile)], arrived_ref.at[:, pl.ds(c, tile)],
                    out_send.at[c // tile], out_recv.at[c // tile], {"tp": partner})
        copy.start()
        leaves.append(copy)

    mine = stat_rows(0)

    def write_log(m_odd, m_even):
        for g in range(groups):
            log_ref[2 * g:2 * g + 1] = jnp.log(jnp.maximum(m_even[g:g + 1], mass_floor))
            log_ref[2 * g + 1:2 * g + 2] = jnp.log(jnp.maximum(m_odd[g:g + 1], mass_floor))

    @pl.when(me < 2)
    def _():
        write_log(mine[0:4], mine[8:12])

    @pl.when(me == 2)
    def _():
        stat_copy(1, 2).wait_recv()
        far = stat_in[0]
        write_log(mine[0:4] + jnp.exp2(-mine[4:8]) * far[0:4], mine[8:12] + jnp.exp2(-mine[12:16]) * far[8:12])

    @pl.when(me == 3)
    def _():
        send(stat_out.at[1], stat_in.at[0], stat_send.at[1], stat_recv.at[0], {"sp": 1}).wait_recv()
        far, mid = stat_in[0], stat_in[1]
        odd = mid[0:4] + jnp.exp2(-mid[4:8]) * far[0:4]
        even = mid[8:12] + jnp.exp2(-mid[12:16]) * far[8:12]
        write_log(mine[0:4] + jnp.exp2(-mine[4:8]) * odd, mine[8:12] + jnp.exp2(-mine[12:16]) * even)

    for c in range(0, model, tile):
        cols = slice(c, c + tile)
        acc = conv_share[ours, cols] + jnp.dot(
            heads_ref[ours, cut:], out_weights[1, cut:, cols], preferred_element_type=f32)
        leaves[c // tile].wait()
        out_ref[:, cols] = (acc + arrived_ref[:, cols].astype(f32)).astype(bf16)

    @pl.when(me < n - 1)
    def _():
        halo_copy.wait_send()

    @pl.when(me == 0)
    def _():
        offs_copy.wait_send()
        for g in range(groups):
            for t in range(2):
                kv_copy(t, g).wait_send()

    @pl.when(me == 1)
    def _():
        for i in (1, 0):
            for g in range(groups):
                o_copy(1, i + 2, g).wait_send()
            stat_copy(1, i + 2).wait_send()

    @pl.when(me == 2)
    def _():
        for g in range(groups):
            q_copy(2, 1, g).wait_send()
            o_copy(2, 3, g).wait_send()
        stat_copy(2, 3).wait_send()

    @pl.when(me == 3)
    def _():
        for g in range(groups):
            q_copy(3, 1, g).wait_send()
            q_copy(3, 2, g).wait_send()


def place(mixed, mass_log, out_ref, log_ref, sem):
    copies = [
        pltpu.make_async_copy(mixed, out_ref, sem.at[0]),
        pltpu.make_async_copy(mass_log, log_ref, sem.at[1]),
    ]
    for copy in copies:
        copy.start()
    for copy in copies:
        copy.wait()


def local(n, tp,
    stream, norm_gain, query_weight, key_weight, value_weight, filter_input, filter_gate,
    score_offset, head_gain, filter_taps, channel_gain, channel_shift, attend_out, filter_out,
):
    f32, bf16 = jnp.float32, jnp.bfloat16
    rows = stream.shape[1]
    heads = score_offset.shape[2]
    groups = heads * HEAD_DIM // LANES
    chans = filter_input.shape[1]
    slabs = chans // LANES
    taps = filter_taps.shape[0]
    model = stream.shape[2]
    share = rows // tp
    tiles = model // min(512, model)

    vmem = pl.BlockSpec(memory_space=pltpu.VMEM)
    hbm = pl.BlockSpec(memory_space=pl.ANY)
    dma = pltpu.SemaphoreType.DMA
    mixed, mass_log = pl.pallas_call(
        functools.partial(kernel, n, tp, taps, chans * tp),
        out_shape=(
            jax.ShapeDtypeStruct((share, model), bf16),
            jax.ShapeDtypeStruct((heads, rows), f32),
        ),
        in_specs=[hbm] + [vmem] * 6 + [hbm] * 7,
        out_specs=(vmem,) * 2,
        scratch_shapes=[
            pltpu.VMEM((rows, model), bf16),
            pltpu.VMEM((rows, model), bf16),
            pltpu.VMEM((5, model, chans), bf16),
            pltpu.VMEM((2, chans, model), bf16),
            pltpu.VMEM((3, groups, rows, LANES), bf16),
            pltpu.VMEM((2, groups, rows, LANES), bf16),
            pltpu.VMEM((2, groups, rows, LANES), bf16),
            pltpu.VMEM((heads, rows), bf16),
            pltpu.VMEM((2, groups, rows, LANES), bf16),
            pltpu.VMEM((2, groups, rows, LANES), bf16),
            pltpu.VMEM((2, 16, rows), f32),
            pltpu.VMEM((2, 16, rows), f32),
            pltpu.VMEM((groups, 2, rows, LANES), f32),
            pltpu.VMEM((groups, 2, rows, LANES), f32),
            pltpu.VMEM((2, 2, rows, LANES), f32),
            pltpu.VMEM((2, 2, rows, LANES), f32),
            pltpu.VMEM((3, rows, LANES), f32),
            pltpu.VMEM((2, heads, rows), f32),
            pltpu.VMEM((slabs, taps + -taps % 8, LANES), f32),
            pltpu.VMEM((rows, heads * HEAD_DIM), bf16),
            pltpu.VMEM((rows, chans), bf16),
            pltpu.VMEM((rows, model), f32),
            pltpu.VMEM((share, model), bf16),
            pltpu.VMEM((share, model), bf16),
            pltpu.VMEM((HALO, chans), bf16),
            pltpu.VMEM((HALO, chans), bf16),
            pltpu.VMEM((slabs, HALO + rows, LANES), f32),
            pltpu.VMEM((slabs, rows, LANES), f32),
            pltpu.VMEM((rows, LANES), f32),
            pltpu.VMEM((rows, LANES), f32),
            dma, dma((5,)), dma((2,)), dma((2, groups)), dma((2, groups)), dma((2, groups)), dma((2, groups)), dma, dma,
            dma((2, groups)), dma((2, groups)), dma((2,)), dma((2,)), dma((tiles,)), dma((tiles,)), dma, dma, dma, dma,
        ],
        compiler_params=pltpu.CompilerParams(
            collective_id=0, has_side_effects=True, vmem_limit_bytes=56 * 1024 * 1024),
    )(stream[0], norm_gain, score_offset[0].T, filter_taps, head_gain, channel_gain, channel_shift,
      query_weight, key_weight, value_weight, filter_input, filter_gate, attend_out, filter_out)
    mixed, mass_log = pl.pallas_call(
        place,
        out_shape=(
            jax.ShapeDtypeStruct((share, model), bf16),
            jax.ShapeDtypeStruct((heads, rows), f32),
        ),
        in_specs=[vmem] * 2,
        out_specs=(hbm,) * 2,
        scratch_shapes=[dma((2,))],
    )(mixed, mass_log)
    return (mixed[None], mass_log.T[None])


def shifted(value, axis, steps):
    count = lax.axis_size(axis)
    first, last = (max(0, -steps), min(count, count - steps))
    return lax.ppermute(value, axis, [(source, source + steps) for source in range(first, last)])


def local_ring(
    stream,
    norm_gain,
    query_weight,
    key_weight,
    value_weight,
    filter_input,
    filter_gate,
    score_offset,
    head_gain,
    filter_taps,
    channel_gain,
    channel_shift,
    attend_out,
    filter_out,
):
    rows_here = stream.shape[1]
    total_channels = filter_input.shape[1] * lax.axis_size("tp")
    xfloat = stream[0].astype(jnp.float32)
    normed = xfloat * lax.rsqrt(jnp.mean(xfloat * xfloat, axis=-1, keepdims=True) + rms_eps)
    normed = (normed * norm_gain.astype(jnp.float32)).astype(jnp.bfloat16)

    def project(weight):
        return jnp.dot(normed, weight, preferred_element_type=jnp.float32).astype(jnp.bfloat16)

    queries = project(query_weight)
    keys_here = project(key_weight)
    values_here = project(value_weight)
    conv_in = project(filter_input)
    conv_gate = project(filter_gate)
    offsets_here = score_offset[0]
    heads_here = offsets_here.shape[1]
    first_pos = lax.axis_index("sp") * rows_here
    position = first_pos + jnp.arange(rows_here, dtype=jnp.int32)
    qheads = queries.reshape(rows_here, heads_here, HEAD_DIM)

    def absorb(state_now, kblock, vblock, oblock, first_key):
        attended, weight_mass, survive = state_now
        span = kblock.shape[0]
        kblock = kblock.reshape(span, heads_here, HEAD_DIM)
        vblock = vblock.reshape(span, heads_here, HEAD_DIM)
        scores = jnp.einsum(
            "thd,shd->hts", qheads, kblock, preferred_element_type=jnp.float32
        ) * HEAD_DIM ** (-0.5)
        scores = scores + oblock.astype(jnp.float32).T[:, None, :]
        key_pos = first_key + jnp.arange(span, dtype=jnp.int32)
        strict = ((key_pos[None, :] < position[:, None]) & (key_pos[None, :] >= 0))[None]
        losing = jnp.where(strict, jax.nn.log_sigmoid(-scores), 0.0)
        beyond = lax.cumsum(losing, axis=2, reverse=True) - losing + survive[:, :, None]
        weights = jnp.where(strict, jnp.exp(jax.nn.log_sigmoid(scores) + beyond), 0.0)
        weight_mass = weight_mass + jnp.sum(weights, axis=2)
        attended = attended + jnp.einsum(
            "hts,shd->thd", weights.astype(jnp.bfloat16), vblock, preferred_element_type=jnp.float32
        )
        survive = survive + jnp.sum(losing, axis=2)
        return (attended, weight_mass, survive)

    initial = (
        jnp.zeros((rows_here, heads_here, HEAD_DIM), jnp.float32),
        jnp.zeros((heads_here, rows_here), jnp.float32),
        jnp.zeros((heads_here, rows_here), jnp.float32),
    )
    state_now = absorb(initial, keys_here, values_here, offsets_here, first_pos)

    def pass_turn(turn_index, carried):
        state_now, travelling = carried
        travelling = shifted((travelling[0], travelling[1], travelling[2]), "sp", 1)
        first_key = first_pos - (turn_index + 1) * rows_here
        state_now = absorb(state_now, travelling[0], travelling[1], travelling[2], first_key)
        return (state_now, travelling)

    state_now, travelling = lax.fori_loop(
        0, lax.axis_size("sp") - 1, pass_turn, (state_now, (keys_here, values_here, offsets_here))
    )
    attended, weight_mass, survive = state_now
    head_scale = lax.rsqrt(jnp.mean(attended * attended, axis=-1, keepdims=True) + rms_eps)
    heads_flat = attended * head_scale * head_gain.astype(jnp.float32).reshape(heads_here, HEAD_DIM)
    heads_flat = heads_flat.astype(jnp.bfloat16).reshape(rows_here, heads_here * HEAD_DIM)
    mass_log = jnp.log(jnp.maximum(weight_mass.T, mass_floor))
    gated_rows = (
        conv_in.astype(jnp.float32) * jax.nn.sigmoid(conv_gate.astype(jnp.float32))
    ).astype(jnp.bfloat16)
    reach_back = filter_taps.shape[0] - 1
    earlier = shifted(gated_rows[rows_here - reach_back :], "sp", 1)
    extended = jnp.concatenate([earlier, gated_rows], axis=0).astype(jnp.float32)
    tap_values = filter_taps.astype(jnp.float32)
    filtered = jnp.zeros((rows_here, gated_rows.shape[1]), jnp.float32)
    for tap_index in range(reach_back + 1):
        filtered = filtered + extended[tap_index : tap_index + rows_here] * tap_values[tap_index]
    center = lax.psum(jnp.sum(filtered, axis=-1), "tp") / total_channels
    deviation = filtered - center[:, None]
    spread = lax.psum(jnp.sum(deviation * deviation, axis=-1), "tp") / total_channels
    conv_out = jax.nn.silu(
        deviation * lax.rsqrt(spread[:, None] + norm_eps) * channel_gain.astype(jnp.float32)
        + channel_shift.astype(jnp.float32)
    ).astype(jnp.bfloat16)
    mixed_out = lax.psum_scatter(
        (
            jnp.dot(heads_flat, attend_out, preferred_element_type=jnp.float32)
            + jnp.dot(conv_out, filter_out, preferred_element_type=jnp.float32)
        ).astype(jnp.bfloat16),
        "tp",
        scatter_dimension=0,
        tiled=True,
    )
    return (mixed_out[None], mass_log[None])


def solution(mesh):
    n, tp = mesh.shape["sp"], mesh.shape["tp"]

    def choose(*args):
        rows, heads, chans = args[0].shape[1], args[7].shape[2], args[5].shape[1]
        same = args[2].shape[1] == chans and heads * HEAD_DIM == 4 * LANES == chans
        if n == 4 and tp == 2 and same and rows % 128 == 0:
            return local(n, tp, *args)
        return local_ring(*args)

    return jax.shard_map(
        choose,
        mesh=mesh,
        in_specs=(
            P("fs", "sp", None), P(), P(None, "tp"), P(None, "tp"), P(None, "tp"),
            P(None, "tp"), P(None, "tp"), P("fs", "sp", "tp"), P("tp"), P(None, "tp"),
            P("tp"), P("tp"), P("tp", None), P("tp", None),
        ),
        out_specs=(P("fs", ("sp", "tp"), None), P("fs", "sp", "tp")),
        check_vma=False,
    )
```

```python
import functools

import jax
import jax.numpy as jnp
from jax import lax
from jax.experimental import pallas as pl
from jax.experimental.pallas import tpu as pltpu
from jax.sharding import PartitionSpec as P

HEAD_DIM = 64

rms_eps = 1e-06
norm_eps = 1e-05
mass_floor = 0.01
HALO = 32
LANES = 128
LOG2E = 1.4426950408889634
MESH = pl.DeviceIdType.MESH


def kernel(
    n, tp, taps, total_channels,
    stream_hbm, ngain_hbm, offs_hbm, taps_hbm, gain_hbm, cgain_hbm, cshift_hbm,
    q_hbm, k_hbm, v_hbm, in_hbm, gate_hbm, attend_hbm, filter_hbm,
    out_hbm, log_hbm,
    ngain, offs, raw_taps, gain_ref, cgain_ref, cshift_ref, out_ref, log_ref,
    stream, normed, weights, out_weights, packet, q_in, kv_in, offs_in, o_out, o_in, stat_out, stat_in,
    own_r, own_t, far_r, far_t, masses, off_rows, tap_ref, heads_ref, conv_ref, conv_share, leaving, arrived_ref,
    gated, halo, ext, filt, stats, stats_got,
    small_sem, place_sem, stream_sem, weight_sem, out_weight_sem, q_send, q_recv, kv_send, kv_recv, kv_last_send, kv_last_recv, offs_send, offs_recv,
    o_send, o_recv, stat_send, stat_recv, out_send, out_recv, halo_send, halo_recv, chan_send, chan_recv,
):
    f32, bf16 = jnp.float32, jnp.bfloat16
    me = lax.axis_index("sp")
    core = lax.axis_index("tp")
    partner = 1 - core
    rows, model = normed.shape
    chans = in_hbm.shape[1]
    groups = packet.shape[1]
    slabs = chans // LANES
    lane = lax.broadcasted_iota(jnp.int32, (rows, LANES), 1)
    low = lane < HEAD_DIM

    def local_copy(src, dst, sem):
        return pltpu.make_async_copy(src, dst, sem)

    def send(src, dst, send_sem, recv_sem, to):
        return pltpu.make_async_remote_copy(
            src_ref=src, dst_ref=dst, send_sem=send_sem, recv_sem=recv_sem,
            device_id=to, device_id_type=MESH)

    projections = (q_hbm, k_hbm, v_hbm)
    first_order, other_order = (1, 2, 0), (0, 1, 2)

    def slot_of(t):
        return jnp.where(me == 0, first_order[t], other_order[t])

    wide = 2 * LANES
    halves = chans // wide

    def weight_copy(w, slot, half):
        cols = pl.ds(half * wide, wide)
        return local_copy(w.at[:, cols], weights.at[slot, :, cols], weight_sem.at[slot, half])

    def fetch(t, half):
        for order, here in ((first_order, me == 0), (other_order, me != 0)):
            @pl.when(here)
            def _(s=order[t]):
                weight_copy(projections[s], s, half).start()

    band = min(64, rows)

    def stream_copy(c):
        some = pl.ds(pl.multiple_of(c * band, band), band)
        return local_copy(stream_hbm.at[some], stream.at[some], stream_sem.at[c])

    small = [local_copy(a, b, small_sem.at[t]) for t, (a, b) in enumerate((
        (ngain_hbm, ngain), (offs_hbm, offs), (taps_hbm, raw_taps), (gain_hbm, gain_ref),
        (cgain_hbm, cgain_ref), (cshift_hbm, cshift_ref)))]
    gate_copies = [weight_copy(w, 3 + t, half) for half in range(halves) for t, w in enumerate((in_hbm, gate_hbm))]
    out_copies = [local_copy(w, out_weights.at[t], out_weight_sem.at[t]) for t, w in enumerate((filter_hbm, attend_hbm))]
    for c in range(rows // band):
        stream_copy(c).start()
    small[0].start()
    for t in range(2):
        fetch(t, 0)
    for copy in small[1:]:
        copy.start()

    barrier = pltpu.get_barrier_semaphore()
    peers = {0: (1, 2), 1: (0, 2, 3), 2: (0, 1, 3), 3: (1, 2)}
    pl.semaphore_signal(barrier, inc=1, device_id={"tp": partner}, device_id_type=MESH)
    for d in range(n):
        @pl.when(me == d)
        def _(d=d):
            for p in peers[d]:
                pl.semaphore_signal(barrier, inc=1, device_id={"sp": p}, device_id_type=MESH)

    small[0].wait()
    norm_gain = ngain[...].astype(f32).reshape(1, -1)

    @pl.loop(0, rows // band)
    def _(c):
        stream_copy(c).wait()

        @pl.when(c == 0)
        def _():
            for half in range(1, halves):
                for t in range(2):
                    fetch(t, half)
            for copy in gate_copies:
                copy.start()

        some = pl.ds(pl.multiple_of(c * band, band), band)
        x = stream[some, :].astype(f32)
        x = x * lax.rsqrt(jnp.mean(x * x, axis=-1, keepdims=True) + rms_eps)
        normed[some, :] = (x * norm_gain).astype(bf16)

    for half in range(halves):
        fetch(2, half)
    for copy in small[1:]:
        copy.wait()

    for d in range(n):
        @pl.when(me == d)
        def _(d=d):
            pl.semaphore_wait(barrier, len(peers[d]) + tp - 1)

    def q_copy(src_dev, dst_dev, g):
        return send(packet.at[0, g], q_in.at[src_dev - 2, g], q_send.at[dst_dev - 1, g],
                    q_recv.at[src_dev - 2, g], {"sp": dst_dev})

    last = groups - 1

    def kv_copy(t, g):
        return send(packet.at[1 + t, g], kv_in.at[t, g], kv_send.at[t, g], kv_recv.at[t, g], {"sp": 1})

    def kv_last(t, src_dev):
        return send(packet.at[1 + t, last], kv_in.at[t, 0 if src_dev else last],
                    kv_last_send.at[t], kv_last_recv.at[t, src_dev], {"sp": 2})

    def offs_copy(src_dev, dst_dev):
        return send(offs, offs_in.at[src_dev], offs_send.at[dst_dev - 1], offs_recv.at[src_dev], {"sp": dst_dev})

    def o_copy(src_dev, dst_dev, g):
        return send(o_out.at[dst_dev - 2, g], o_in.at[src_dev - 1, g], o_send.at[dst_dev - 2, g],
                    o_recv.at[src_dev - 1, g], {"sp": dst_dev})

    def stat_copy(src_dev, dst_dev):
        return send(stat_out.at[dst_dev - 2], stat_in.at[src_dev - 1], stat_send.at[dst_dev - 2],
                    stat_recv.at[src_dev - 1], {"sp": dst_dev})

    @pl.when(me == 0)
    def _():
        offs_copy(0, 1).start()
        offs_copy(0, 2).start()

    @pl.when(me == 1)
    def _():
        offs_copy(1, 2).start()

    def keep(slot, half, y):
        factor = jnp.where(slot == 0, LOG2E * HEAD_DIM ** (-0.5), 1.0).astype(f32)
        y = (y * factor).astype(bf16)
        for u in range(2):
            packet[slot, 2 * half + u] = y[:, u * LANES:(u + 1) * LANES]

    def project(jobs):
        for t, half in jobs:
            slot = slot_of(t)
            weight_copy(q_hbm, slot, half).wait()
        for t, half in jobs:
            slot = slot_of(t)
            keep(slot, half, jnp.dot(
                normed[...], weights[slot, :, half * wide:(half + 1) * wide], preferred_element_type=f32))

    for half in range(halves):
        project([(0, half), (1, half)])

        @pl.when(me == 0)
        def _():
            if half == 0:
                kv_copy(0, 0).start()
                kv_copy(1, 0).start()

        @pl.when(me == 2)
        def _():
            for g in (2 * half, 2 * half + 1):
                if g < last:
                    q_copy(2, 1, g).start()

        @pl.when(me == 3)
        def _():
            if half > 0:
                q_copy(3, 2, 2 * half - 1).start()
            q_copy(3, 1, 2 * half).start()
            q_copy(3, 2, 2 * half).start()
            if 2 * half + 1 < last:
                q_copy(3, 1, 2 * half + 1).start()
            else:
                q_copy(3, 2, 2 * half + 1).start()

    for copy in out_copies:
        copy.start()
    tap_ref[...] = jnp.zeros_like(tap_ref)
    for c in range(slabs):
        tap_ref[c, :taps] = raw_taps[:, c * LANES:(c + 1) * LANES].astype(f32)
    off_rows[0] = offs[...].astype(f32) * LOG2E
    masses[...] = jnp.zeros_like(masses)
    for copy in gate_copies:
        copy.wait()

    @pl.loop(0, halves)
    def _(c):
        cols = pl.ds(pl.multiple_of(c * wide, wide), wide)
        x = normed[...]
        value = jnp.dot(x, weights[3, :, cols], preferred_element_type=f32).astype(bf16).astype(f32)
        gate = jnp.dot(x, weights[4, :, cols], preferred_element_type=f32).astype(bf16).astype(f32)
        g = (value * jax.nn.sigmoid(gate)).astype(bf16)
        gated[:, cols] = g[rows - HALO:]
        g = g.astype(f32)
        for u in range(2):
            ext[2 * c + u, HALO:, :] = g[:, u * LANES:(u + 1) * LANES]

    halo_copy = send(gated, halo, halo_send, halo_recv, {"sp": lax.rem(me + 1, n)})

    @pl.when(me < n - 1)
    def _():
        halo_copy.start()

    @pl.when(me == 0)
    def _():
        for g in range(1, last):
            for t in range(2):
                kv_copy(t, g).start()
        for t in range(2):
            kv_last(t, 0).start()
        for t in range(2):
            kv_copy(t, last).start()

    project([(2, half) for half in range(halves)])

    @pl.when(me == 1)
    def _():
        for t in range(2):
            kv_last(t, 1).start()

    step = min(128, rows)

    def convolve(starts):
        @pl.loop(0, slabs)
        def _(c):
            for r0 in starts:
                acc = jnp.zeros((step, LANES), f32)
                for k in range(taps):
                    start = HALO - (taps - 1) + k + r0
                    acc = acc + ext[c, start:start + step, :] * tap_ref[c, k:k + 1, :]
                filt[c, r0:r0 + step, :] = acc

    chan_copy = send(stats, stats_got, chan_send, chan_recv, {"tp": partner})

    def convolve_first():
        @pl.when(me > 0)
        def _():
            halo_copy.wait_recv()
            for c in range(slabs):
                ext[c, :HALO, :] = halo[:, c * LANES:(c + 1) * LANES].astype(f32)

        @pl.when(me == 0)
        def _():
            for c in range(slabs):
                ext[c, :HALO, :] = jnp.zeros((HALO, LANES), f32)

        convolve([0])
        total = filt[0]
        for c in range(1, slabs):
            total = total + filt[c]
        lsum = jnp.sum(total, axis=1, keepdims=True)
        mean = lsum * (1.0 / chans)
        square = jnp.zeros((rows, LANES), f32)
        for c in range(slabs):
            dev = filt[c] - mean
            square = square + dev * dev
        lsq = jnp.sum(square, axis=1, keepdims=True)
        stats[...] = jnp.where(low, lsum, lsq)
        chan_copy.start()

    def channel_norm():
        chan_copy.wait()
        mine, other = stats[...], stats_got[...]
        mean = (mine[:, 0:1] + other[:, 0:1]) * (1.0 / total_channels)
        spread = jnp.zeros((rows, 1), f32)
        for s in (mine, other):
            apart = s[:, 0:1] * (1.0 / chans) - mean
            spread = spread + s[:, HEAD_DIM:HEAD_DIM + 1] + chans * apart * apart
        scale = lax.rsqrt(spread * (1.0 / total_channels) + norm_eps)
        for c in range(slabs):
            cols = slice(c * LANES, (c + 1) * LANES)
            y = (filt[c] - mean) * scale * cgain_ref[cols].astype(f32).reshape(1, -1) + cshift_ref[cols].astype(f32).reshape(1, -1)
            conv_ref[:, cols] = (y * jax.nn.sigmoid(y)).astype(bf16)

    tile = min(1024, model)

    def conv_product():
        out_copies[0].wait()
        for c in range(0, model, tile):
            conv_share[:, c:c + tile] = jnp.dot(
                conv_ref[...], out_weights[0, :, c:c + tile], preferred_element_type=f32)

    ri = lax.broadcasted_iota(jnp.int32, (rows, rows), 0)
    ci = lax.broadcasted_iota(jnp.int32, (rows, rows), 1)
    tri = (ri >= ci).astype(bf16)

    def split_keys(k):
        zero = jnp.zeros_like(k)
        return jnp.where(low, k, zero), jnp.where(low, zero, k)

    def split_values(v):
        one = jnp.ones_like(v)
        return jnp.where(low, v, one), jnp.where(low, one, v)

    strict = ci < ri

    def attend(blocks_q, k, v, off, own_first):
        q = jnp.concatenate(blocks_q, axis=0)
        z = lax.dot_general(q, k, (((1,), (1,)), ((), ())), preferred_element_type=f32) + off
        lose = jnp.maximum(z, jnp.log(1.0 + jnp.exp2(jnp.minimum(z, 100.0))) * LOG2E)

        def masked(x):
            if not own_first:
                return x
            head = jnp.where(strict, x[:rows], 0.0)
            return jnp.concatenate([head, x[rows:]], axis=0) if len(blocks_q) > 1 else head

        cum = jnp.dot(masked(lose).astype(bf16), tri, preferred_element_type=f32)
        w = masked(jnp.exp2(z - cum))
        res = jnp.dot(w.astype(bf16), v, preferred_element_type=f32)
        pieces = []
        for r in range(len(blocks_q)):
            some = slice(r * rows, (r + 1) * rows)
            pieces.append((res[some], jnp.broadcast_to(cum[some, 0:1], (rows, LANES))))
        return pieces

    def note(which, g, h, res, total):
        base = 0 if h else HEAD_DIM
        masses[which] = jnp.where(lane == base + g, res, jnp.where(lane == base + 4 + g, total, masses[which]))

    def pair(a, b):
        return jnp.where(low, a, b)

    def near_blocks(g, others):
        keys = split_keys(packet[1, g])
        values = split_values(packet[2, g])
        rest = []
        for h in range(2):
            first, *more = attend([packet[0, g]] + others, keys[h], values[h], off_rows[0, pl.ds(2 * g + h, 1), :], True)
            res, total = first
            own_r[g, h] = res
            own_t[g, h] = jnp.exp2(-total)
            note(0, g, h, res, total)
            rest.append(more)
        return rest

    convolve(range(step, rows, step))

    @pl.when(me != 2)
    def _():
        @pl.loop(0, groups // 2)
        def _(half):
            for u in range(2):
                near_blocks(2 * half + u, [])

    convolve_first()

    def q_from(src_dev, dst_dev, g):
        return send(packet.at[0, g], q_in.at[src_dev - 2, g], q_send.at[dst_dev - 1, g],
                    q_recv.at[src_dev - 2, g], {"sp": src_dev})

    def kv_from(t, g):
        return send(packet.at[1 + t, g], kv_in.at[t, g], kv_send.at[t, g], kv_recv.at[t, g], {"sp": 0})

    @pl.when(me == 1)
    def _():
        offs_copy_back = send(offs, offs_in.at[0], offs_send.at[0], offs_recv.at[0], {"sp": 0})
        offs_copy_back.wait_recv()
        off_rows[1] = offs_in[0].astype(f32) * LOG2E

    @pl.when(me == 2)
    def _():
        for src in range(2):
            send(offs, offs_in.at[src], offs_send.at[1], offs_recv.at[src], {"sp": src}).wait_recv()
            off_rows[1 + src] = offs_in[src].astype(f32) * LOG2E

    def middle_block(g):
        q_from(3, 2, g).wait_recv()
        return near_blocks(g, [q_in[1, g]])

    @pl.loop(0, last)
    def _(g):
        @pl.when(me == 1)
        def _():
            keys = split_keys(packet[1, g])
            values = split_values(packet[2, g])
            for i in (1, 0):
                q_from(i + 2, 1, g).wait_recv()
            for h in range(2):
                pieces = attend([q_in[1, g], q_in[0, g]], keys[h], values[h], off_rows[0, pl.ds(2 * g + h, 1), :], False)
                for i in (1, 0):
                    res, total = pieces[1 - i]
                    far_r[i, h] = res
                    far_t[i, h] = jnp.exp2(-total)

        @pl.when(me == 2)
        def _():
            rest = middle_block(g)
            for h in range(2):
                note(2, g, h, *rest[h][0])
            o_out[1, g] = pair(rest[0][0][0], rest[1][0][0]).astype(bf16)
            send(o_out.at[1, g], o_in.at[1, g], o_send.at[1, g], o_recv.at[1, g], {"sp": 3}).start()

        @pl.when(g == 0)
        def _():
            channel_norm()

        @pl.when(g == 1)
        def _():
            conv_product()

        @pl.when(me == 1)
        def _():
            for t in range(2):
                kv_from(t, g).wait_recv()
            keys = split_keys(kv_in[0, g])
            values = split_values(kv_in[1, g])
            parts = [[], []]
            for h in range(2):
                pieces = attend([q_in[1, g], q_in[0, g], packet[0, g]], keys[h], values[h],
                                off_rows[1, pl.ds(2 * g + h, 1), :], False)
                for i in (1, 0):
                    res = far_r[i, h] + far_t[i, h] * pieces[1 - i][0]
                    note(1 + i, g, h, res, res)
                    parts[i].append(res)
                res = own_r[g, h] + own_t[g, h] * pieces[2][0]
                own_r[g, h] = res
                note(0, g, h, res, res)
            for i in (1, 0):
                o_out[i, g] = pair(*parts[i]).astype(bf16)
            for i in (1, 0):
                send(o_out.at[i, g], o_in.at[0, g], o_send.at[i, g], o_recv.at[0, g], {"sp": i + 2}).start()

    @pl.when(me == 2)
    def _():
        rest = middle_block(last)
        for h in range(2):
            res, total = rest[h][0]
            far_r[1, h] = res
            far_t[1, h] = jnp.exp2(-total)
        for src, where in ((1, 0), (0, last)):
            for t in range(2):
                send(packet.at[1 + t, last], kv_in.at[t, where], kv_last_send.at[t],
                     kv_last_recv.at[t, src], {"sp": src}).wait_recv()
            keys = split_keys(kv_in[0, where])
            values = split_values(kv_in[1, where])
            parts = []
            for h in range(2):
                (own, own_total), (far, far_total) = attend(
                    [packet[0, last], q_in[1, last]], keys[h], values[h], off_rows[1 + src, 2 * last + h:2 * last + h + 1, :], False)
                own = own_r[last, h] + own_t[last, h] * own
                far = far_r[1, h] + far_t[1, h] * far
                own_r[last, h] = own
                if src:
                    far_r[1, h] = far
                    own_t[last, h] = own_t[last, h] * jnp.exp2(-own_total)
                    far_t[1, h] = far_t[1, h] * jnp.exp2(-far_total)
                else:
                    note(0, last, h, own, own)
                    note(2, last, h, far, far)
                    parts.append(far)
        o_out[1, last] = pair(*parts).astype(bf16)
        o_copy(2, 3, last).start()

    def stat_rows(which):
        t = jnp.transpose(masses[which])
        return jnp.concatenate([t[0:8], t[HEAD_DIM:HEAD_DIM + 8]], axis=0)

    @pl.when(me == 1)
    def _():
        for i in (1, 0):
            stat_out[i] = stat_rows(1 + i)
            stat_copy(1, i + 2).start()

    @pl.when(me == 2)
    def _():
        stat_out[1] = stat_rows(2)
        stat_copy(2, 3).start()

    @pl.when(me == 1)
    def _():
        for t in range(2):
            kv_from(t, last).wait_recv()
        keys = split_keys(kv_in[0, last])
        values = split_values(kv_in[1, last])
        for h in range(2):
            res, _ = attend([packet[0, last]], keys[h], values[h], off_rows[1, 2 * last + h:2 * last + h + 1, :], False)[0]
            res = own_r[last, h] + own_t[last, h] * res
            own_r[last, h] = res
            note(0, last, h, res, res)

    blocks = (lax.broadcasted_iota(jnp.int32, (LANES, LANES), 0) // HEAD_DIM
              == lax.broadcasted_iota(jnp.int32, (LANES, LANES), 1) // HEAD_DIM).astype(bf16)

    @pl.when(me == 3)
    def _():
        stat_copy(2, 3).wait_recv()
        rest = jnp.zeros((LANES - 16, rows), f32)
        far_t[0, 0] = jnp.transpose(jnp.concatenate([stat_in[1], rest], axis=0))

    def finish(g):
        cols = slice(g * LANES, (g + 1) * LANES)

        def close(o):
            sq = jnp.dot((o * o).astype(bf16), blocks, preferred_element_type=f32)
            gain = gain_ref[cols].astype(f32).reshape(1, LANES)
            heads_ref[:, cols] = (o * lax.rsqrt(sq * (1.0 / HEAD_DIM) + rms_eps) * gain).astype(bf16)

        own = pair(own_r[g, 0], own_r[g, 1])

        @pl.when(me < 2)
        def _():
            close(own)

        @pl.when(me == 2)
        def _():
            if g == last:
                close(own)
            else:
                through = pair(own_t[g, 0], own_t[g, 1])
                send(o_out.at[0, g], o_in.at[0, g], o_send.at[0, g], o_recv.at[0, g], {"sp": 1}).wait_recv()
                close(own + through * o_in[0, g].astype(f32))

        @pl.when(me == 3)
        def _():
            through = pair(own_t[g, 0], own_t[g, 1])
            send(o_out.at[1, g], o_in.at[1, g], o_send.at[1, g], o_recv.at[1, g], {"sp": 2}).wait_recv()
            inner = o_in[1, g].astype(f32)
            if g < last:
                tot = far_t[0, 0]
                middle = jnp.exp2(-pair(tot[:, 12 + g:13 + g], tot[:, 4 + g:5 + g]))
                send(o_out.at[1, g], o_in.at[0, g], o_send.at[1, g], o_recv.at[0, g], {"sp": 1}).wait_recv()
                inner = inner + middle * o_in[0, g].astype(f32)
            close(own + through * inner)

    out_copies[1].wait()
    early = groups // 2
    for g in range(early):
        finish(g)
    cut = early * LANES
    for c in range(0, model, tile):
        conv_share[:, c:c + tile] += jnp.dot(
            heads_ref[:, :cut], out_weights[1, :cut, c:c + tile], preferred_element_type=f32)
    for g in range(early, groups):
        finish(g)
    share = rows // tp
    theirs = pl.ds(pl.multiple_of(partner * share, share), share)
    ours = pl.ds(pl.multiple_of(core * share, share), share)
    leaves = []
    for c in range(0, model, tile):
        cols = slice(c, c + tile)
        leaving[:, cols] = (conv_share[theirs, cols] + jnp.dot(
            heads_ref[theirs, cut:], out_weights[1, cut:, cols], preferred_element_type=f32)).astype(bf16)
        copy = send(leaving.at[:, pl.ds(c, tile)], arrived_ref.at[:, pl.ds(c, tile)],
                    out_send.at[c // tile], out_recv.at[c // tile], {"tp": partner})
        copy.start()
        leaves.append(copy)
    for c in range(0, model, tile):
        cols = slice(c, c + tile)
        conv_share[ours, cols] += jnp.dot(
            heads_ref[ours, cut:], out_weights[1, cut:, cols], preferred_element_type=f32)

    mine = stat_rows(0)

    def write_log(m_odd, m_even):
        for g in range(groups):
            log_ref[2 * g:2 * g + 1] = jnp.log(jnp.maximum(m_even[g:g + 1], mass_floor))
            log_ref[2 * g + 1:2 * g + 2] = jnp.log(jnp.maximum(m_odd[g:g + 1], mass_floor))

    @pl.when(me < 2)
    def _():
        write_log(mine[0:4], mine[8:12])

    @pl.when(me == 2)
    def _():
        stat_copy(1, 2).wait_recv()
        far = stat_in[0]
        write_log(mine[0:4] + jnp.exp2(-mine[4:8]) * far[0:4], mine[8:12] + jnp.exp2(-mine[12:16]) * far[8:12])

    @pl.when(me == 3)
    def _():
        send(stat_out.at[1], stat_in.at[0], stat_send.at[1], stat_recv.at[0], {"sp": 1}).wait_recv()
        far, mid = stat_in[0], stat_in[1]
        odd = mid[0:4] + jnp.exp2(-mid[4:8]) * far[0:4]
        even = mid[8:12] + jnp.exp2(-mid[12:16]) * far[8:12]
        write_log(mine[0:4] + jnp.exp2(-mine[4:8]) * odd, mine[8:12] + jnp.exp2(-mine[12:16]) * even)

    places = [local_copy(log_ref, log_hbm, place_sem.at[0])]
    places[0].start()
    for c in range(0, model, tile):
        cols = slice(c, c + tile)
        leaves[c // tile].wait()
        out_ref[:, cols] = (conv_share[ours, cols] + arrived_ref[:, cols].astype(f32)).astype(bf16)
        copy = local_copy(out_ref.at[:, pl.ds(c, tile)], out_hbm.at[:, pl.ds(c, tile)], place_sem.at[1 + c // tile])
        copy.start()
        places.append(copy)

    @pl.when(me < n - 1)
    def _():
        halo_copy.wait_send()

    @pl.when(me == 0)
    def _():
        offs_copy(0, 1).wait_send()
        offs_copy(0, 2).wait_send()
        for t in range(2):
            for g in range(groups):
                kv_copy(t, g).wait_send()
            kv_last(t, 0).wait_send()

    @pl.when(me == 1)
    def _():
        offs_copy(1, 2).wait_send()
        for t in range(2):
            kv_last(t, 1).wait_send()
        for i in (1, 0):
            for g in range(last):
                o_copy(1, i + 2, g).wait_send()
            stat_copy(1, i + 2).wait_send()

    @pl.when(me == 2)
    def _():
        for g in range(last):
            q_copy(2, 1, g).wait_send()
        for g in range(groups):
            o_copy(2, 3, g).wait_send()
        stat_copy(2, 3).wait_send()

    @pl.when(me == 3)
    def _():
        for g in range(groups):
            if g < last:
                q_copy(3, 1, g).wait_send()
            q_copy(3, 2, g).wait_send()

    for copy in places:
        copy.wait()


def place(mixed, mass_log, out_ref, log_ref, sem):
    copies = [
        pltpu.make_async_copy(mixed, out_ref, sem.at[0]),
        pltpu.make_async_copy(mass_log, log_ref, sem.at[1]),
    ]
    for copy in copies:
        copy.start()
    for copy in copies:
        copy.wait()


def local(n, tp,
    stream, norm_gain, query_weight, key_weight, value_weight, filter_input, filter_gate,
    score_offset, head_gain, filter_taps, channel_gain, channel_shift, attend_out, filter_out,
):
    f32, bf16 = jnp.float32, jnp.bfloat16
    rows = stream.shape[1]
    heads = score_offset.shape[2]
    groups = heads * HEAD_DIM // LANES
    chans = filter_input.shape[1]
    slabs = chans // LANES
    taps = filter_taps.shape[0]
    model = stream.shape[2]
    share = rows // tp
    tiles = model // min(1024, model)

    vmem = pl.BlockSpec(memory_space=pltpu.VMEM)
    hbm = pl.BlockSpec(memory_space=pl.ANY)
    dma = pltpu.SemaphoreType.DMA
    mixed, mass_log = pl.pallas_call(
        functools.partial(kernel, n, tp, taps, chans * tp),
        out_shape=(
            jax.ShapeDtypeStruct((share, model), bf16),
            jax.ShapeDtypeStruct((heads, rows), f32),
        ),
        in_specs=[hbm] * 14,
        out_specs=(hbm,) * 2,
        scratch_shapes=[
            pltpu.VMEM((model,), bf16),
            pltpu.VMEM((heads, rows), bf16),
            pltpu.VMEM((taps, chans), bf16),
            pltpu.VMEM((chans,), bf16),
            pltpu.VMEM((chans,), bf16),
            pltpu.VMEM((chans,), bf16),
            pltpu.VMEM((share, model), bf16),
            pltpu.VMEM((heads, rows), f32),
            pltpu.VMEM((rows, model), bf16),
            pltpu.VMEM((rows, model), bf16),
            pltpu.VMEM((5, model, chans), bf16),
            pltpu.VMEM((2, chans, model), bf16),
            pltpu.VMEM((3, groups, rows, LANES), bf16),
            pltpu.VMEM((2, groups, rows, LANES), bf16),
            pltpu.VMEM((2, groups, rows, LANES), bf16),
            pltpu.VMEM((2, heads, rows), bf16),
            pltpu.VMEM((2, groups, rows, LANES), bf16),
            pltpu.VMEM((2, groups, rows, LANES), bf16),
            pltpu.VMEM((2, 16, rows), f32),
            pltpu.VMEM((2, 16, rows), f32),
            pltpu.VMEM((groups, 2, rows, LANES), f32),
            pltpu.VMEM((groups, 2, rows, LANES), f32),
            pltpu.VMEM((2, 2, rows, LANES), f32),
            pltpu.VMEM((2, 2, rows, LANES), f32),
            pltpu.VMEM((3, rows, LANES), f32),
            pltpu.VMEM((3, heads, rows), f32),
            pltpu.VMEM((slabs, taps + -taps % 8, LANES), f32),
            pltpu.VMEM((rows, heads * HEAD_DIM), bf16),
            pltpu.VMEM((rows, chans), bf16),
            pltpu.VMEM((rows, model), f32),
            pltpu.VMEM((share, model), bf16),
            pltpu.VMEM((share, model), bf16),
            pltpu.VMEM((HALO, chans), bf16),
            pltpu.VMEM((HALO, chans), bf16),
            pltpu.VMEM((slabs, HALO + rows, LANES), f32),
            pltpu.VMEM((slabs, rows, LANES), f32),
            pltpu.VMEM((rows, LANES), f32),
            pltpu.VMEM((rows, LANES), f32),
            dma((6,)), dma((1 + tiles,)), dma((rows // min(64, rows),)), dma((5, chans // (2 * LANES))), dma((2,)), dma((2, groups)), dma((2, groups)), dma((2, groups)), dma((2, groups)), dma((2,)), dma((2, 2)), dma((2,)), dma((2,)),
            dma((2, groups)), dma((2, groups)), dma((2,)), dma((2,)), dma((tiles,)), dma((tiles,)), dma, dma, dma, dma,
        ],
        compiler_params=pltpu.CompilerParams(
            collective_id=0, has_side_effects=True, vmem_limit_bytes=56 * 1024 * 1024),
    )(stream[0], norm_gain, score_offset[0].T, filter_taps, head_gain, channel_gain, channel_shift,
      query_weight, key_weight, value_weight, filter_input, filter_gate, attend_out, filter_out)
    mixed, mass_log = pl.pallas_call(
        place,
        out_shape=(
            jax.ShapeDtypeStruct((share, model), bf16),
            jax.ShapeDtypeStruct((heads, rows), f32),
        ),
        in_specs=[vmem] * 2,
        out_specs=(hbm,) * 2,
        scratch_shapes=[dma((2,))],
    )(mixed, mass_log)
    return (mixed[None], mass_log.T[None])


def shifted(value, axis, steps):
    count = lax.axis_size(axis)
    first, last = (max(0, -steps), min(count, count - steps))
    return lax.ppermute(value, axis, [(source, source + steps) for source in range(first, last)])


def local_ring(
    stream,
    norm_gain,
    query_weight,
    key_weight,
    value_weight,
    filter_input,
    filter_gate,
    score_offset,
    head_gain,
    filter_taps,
    channel_gain,
    channel_shift,
    attend_out,
    filter_out,
):
    rows_here = stream.shape[1]
    total_channels = filter_input.shape[1] * lax.axis_size("tp")
    xfloat = stream[0].astype(jnp.float32)
    normed = xfloat * lax.rsqrt(jnp.mean(xfloat * xfloat, axis=-1, keepdims=True) + rms_eps)
    normed = (normed * norm_gain.astype(jnp.float32)).astype(jnp.bfloat16)

    def project(weight):
        return jnp.dot(normed, weight, preferred_element_type=jnp.float32).astype(jnp.bfloat16)

    queries = project(query_weight)
    keys_here = project(key_weight)
    values_here = project(value_weight)
    conv_in = project(filter_input)
    conv_gate = project(filter_gate)
    offsets_here = score_offset[0]
    heads_here = offsets_here.shape[1]
    first_pos = lax.axis_index("sp") * rows_here
    position = first_pos + jnp.arange(rows_here, dtype=jnp.int32)
    qheads = queries.reshape(rows_here, heads_here, HEAD_DIM)

    def absorb(state_now, kblock, vblock, oblock, first_key):
        attended, weight_mass, survive = state_now
        span = kblock.shape[0]
        kblock = kblock.reshape(span, heads_here, HEAD_DIM)
        vblock = vblock.reshape(span, heads_here, HEAD_DIM)
        scores = jnp.einsum(
            "thd,shd->hts", qheads, kblock, preferred_element_type=jnp.float32
        ) * HEAD_DIM ** (-0.5)
        scores = scores + oblock.astype(jnp.float32).T[:, None, :]
        key_pos = first_key + jnp.arange(span, dtype=jnp.int32)
        strict = ((key_pos[None, :] < position[:, None]) & (key_pos[None, :] >= 0))[None]
        losing = jnp.where(strict, jax.nn.log_sigmoid(-scores), 0.0)
        beyond = lax.cumsum(losing, axis=2, reverse=True) - losing + survive[:, :, None]
        weights = jnp.where(strict, jnp.exp(jax.nn.log_sigmoid(scores) + beyond), 0.0)
        weight_mass = weight_mass + jnp.sum(weights, axis=2)
        attended = attended + jnp.einsum(
            "hts,shd->thd", weights.astype(jnp.bfloat16), vblock, preferred_element_type=jnp.float32
        )
        survive = survive + jnp.sum(losing, axis=2)
        return (attended, weight_mass, survive)

    initial = (
        jnp.zeros((rows_here, heads_here, HEAD_DIM), jnp.float32),
        jnp.zeros((heads_here, rows_here), jnp.float32),
        jnp.zeros((heads_here, rows_here), jnp.float32),
    )
    state_now = absorb(initial, keys_here, values_here, offsets_here, first_pos)

    def pass_turn(turn_index, carried):
        state_now, travelling = carried
        travelling = shifted((travelling[0], travelling[1], travelling[2]), "sp", 1)
        first_key = first_pos - (turn_index + 1) * rows_here
        state_now = absorb(state_now, travelling[0], travelling[1], travelling[2], first_key)
        return (state_now, travelling)

    state_now, travelling = lax.fori_loop(
        0, lax.axis_size("sp") - 1, pass_turn, (state_now, (keys_here, values_here, offsets_here))
    )
    attended, weight_mass, survive = state_now
    head_scale = lax.rsqrt(jnp.mean(attended * attended, axis=-1, keepdims=True) + rms_eps)
    heads_flat = attended * head_scale * head_gain.astype(jnp.float32).reshape(heads_here, HEAD_DIM)
    heads_flat = heads_flat.astype(jnp.bfloat16).reshape(rows_here, heads_here * HEAD_DIM)
    mass_log = jnp.log(jnp.maximum(weight_mass.T, mass_floor))
    gated_rows = (
        conv_in.astype(jnp.float32) * jax.nn.sigmoid(conv_gate.astype(jnp.float32))
    ).astype(jnp.bfloat16)
    reach_back = filter_taps.shape[0] - 1
    earlier = shifted(gated_rows[rows_here - reach_back :], "sp", 1)
    extended = jnp.concatenate([earlier, gated_rows], axis=0).astype(jnp.float32)
    tap_values = filter_taps.astype(jnp.float32)
    filtered = jnp.zeros((rows_here, gated_rows.shape[1]), jnp.float32)
    for tap_index in range(reach_back + 1):
        filtered = filtered + extended[tap_index : tap_index + rows_here] * tap_values[tap_index]
    center = lax.psum(jnp.sum(filtered, axis=-1), "tp") / total_channels
    deviation = filtered - center[:, None]
    spread = lax.psum(jnp.sum(deviation * deviation, axis=-1), "tp") / total_channels
    conv_out = jax.nn.silu(
        deviation * lax.rsqrt(spread[:, None] + norm_eps) * channel_gain.astype(jnp.float32)
        + channel_shift.astype(jnp.float32)
    ).astype(jnp.bfloat16)
    mixed_out = lax.psum_scatter(
        (
            jnp.dot(heads_flat, attend_out, preferred_element_type=jnp.float32)
            + jnp.dot(conv_out, filter_out, preferred_element_type=jnp.float32)
        ).astype(jnp.bfloat16),
        "tp",
        scatter_dimension=0,
        tiled=True,
    )
    return (mixed_out[None], mass_log[None])


def solution(mesh):
    n, tp = mesh.shape["sp"], mesh.shape["tp"]

    def choose(*args):
        rows, heads, chans = args[0].shape[1], args[7].shape[2], args[5].shape[1]
        same = args[2].shape[1] == chans and heads * HEAD_DIM == 4 * LANES == chans
        if n == 4 and tp == 2 and same and rows % 128 == 0:
            return local(n, tp, *args)
        return local_ring(*args)

    return jax.shard_map(
        choose,
        mesh=mesh,
        in_specs=(
            P("fs", "sp", None), P(), P(None, "tp"), P(None, "tp"), P(None, "tp"),
            P(None, "tp"), P(None, "tp"), P("fs", "sp", "tp"), P("tp"), P(None, "tp"),
            P("tp"), P("tp"), P("tp", None), P("tp", None),
        ),
        out_specs=(P("fs", ("sp", "tp"), None), P("fs", "sp", "tp")),
        check_vma=False,
    )
```

```python
import functools

import jax
import jax.numpy as jnp
from jax import lax
from jax.experimental import pallas as pl
from jax.experimental.pallas import tpu as pltpu
from jax.sharding import PartitionSpec as P

HEAD_DIM = 64

rms_eps = 1e-06
norm_eps = 1e-05
mass_floor = 0.01
HALO = 32
LANES = 128
LOG2E = 1.4426950408889634
MESH = pl.DeviceIdType.MESH


def kernel(
    n, tp, taps, total_channels,
    stream_hbm, ngain_hbm, offs_hbm, taps_hbm, gain_hbm, cgain_hbm, cshift_hbm,
    q_hbm, k_hbm, v_hbm, in_hbm, gate_hbm, attend_hbm, filter_hbm,
    out_ref, log_ref,
    ngain, offs, raw_taps, gain_ref, cgain_ref, cshift_ref,
    stream, normed, weights, out_weights, packet, q_in, kv_in, offs_in, o_out, o_in, stat_out, stat_in,
    own_r, own_t, far_r, far_t, masses, off_rows, tap_ref, heads_ref, conv_ref, conv_share, leaving, arrived_ref,
    gated, halo, ext, filt, stats, stats_got,
    small_sem, stream_sem, weight_sem, out_weight_sem, q_send, q_recv, kv_send, kv_recv, kv_last_send, kv_last_recv, offs_send, offs_recv,
    o_send, o_recv, stat_send, stat_recv, out_send, out_recv, halo_send, halo_recv, chan_send, chan_recv,
):
    f32, bf16 = jnp.float32, jnp.bfloat16
    me = lax.axis_index("sp")
    core = lax.axis_index("tp")
    partner = 1 - core
    rows, model = normed.shape
    chans = in_hbm.shape[1]
    groups = packet.shape[1]
    slabs = chans // LANES
    lane = lax.broadcasted_iota(jnp.int32, (rows, LANES), 1)
    low = lane < HEAD_DIM

    def local_copy(src, dst, sem):
        return pltpu.make_async_copy(src, dst, sem)

    def send(src, dst, send_sem, recv_sem, to):
        return pltpu.make_async_remote_copy(
            src_ref=src, dst_ref=dst, send_sem=send_sem, recv_sem=recv_sem,
            device_id=to, device_id_type=MESH)

    projections = (q_hbm, k_hbm, v_hbm)
    first_order, other_order = (1, 2, 0), (0, 1, 2)

    def slot_of(t):
        return jnp.where(me == 0, first_order[t], other_order[t])

    wide = 2 * LANES
    halves = chans // wide

    def weight_copy(w, slot, half):
        cols = pl.ds(half * wide, wide)
        return local_copy(w.at[:, cols], weights.at[slot, :, cols], weight_sem.at[slot, half])

    def fetch(t, half):
        for order, here in ((first_order, me == 0), (other_order, me != 0)):
            @pl.when(here)
            def _(s=order[t]):
                weight_copy(projections[s], s, half).start()

    band = min(64, rows)

    def stream_copy(c):
        some = pl.ds(pl.multiple_of(c * band, band), band)
        return local_copy(stream_hbm.at[some], stream.at[some], stream_sem.at[c])

    small = [local_copy(a, b, small_sem.at[t]) for t, (a, b) in enumerate((
        (ngain_hbm, ngain), (offs_hbm, offs), (taps_hbm, raw_taps), (gain_hbm, gain_ref),
        (cgain_hbm, cgain_ref), (cshift_hbm, cshift_ref)))]
    gate_copies = [weight_copy(w, 3 + t, half) for half in range(halves) for t, w in enumerate((in_hbm, gate_hbm))]
    out_copies = [local_copy(w, out_weights.at[t], out_weight_sem.at[t]) for t, w in enumerate((filter_hbm, attend_hbm))]
    for c in range(rows // band):
        stream_copy(c).start()
    small[0].start()
    for t in range(2):
        fetch(t, 0)
    for copy in small[1:]:
        copy.start()

    barrier = pltpu.get_barrier_semaphore()
    peers = {0: (1, 2), 1: (0, 2, 3), 2: (0, 1, 3), 3: (1, 2)}
    pl.semaphore_signal(barrier, inc=1, device_id={"tp": partner}, device_id_type=MESH)
    for d in range(n):
        @pl.when(me == d)
        def _(d=d):
            for p in peers[d]:
                pl.semaphore_signal(barrier, inc=1, device_id={"sp": p}, device_id_type=MESH)

    small[0].wait()
    norm_gain = ngain[...].astype(f32).reshape(1, -1)

    @pl.loop(0, rows // band)
    def _(c):
        stream_copy(c).wait()

        @pl.when(c == 0)
        def _():
            for half in range(1, halves):
                for t in range(2):
                    fetch(t, half)
            for copy in gate_copies:
                copy.start()

        some = pl.ds(pl.multiple_of(c * band, band), band)
        x = stream[some, :].astype(f32)
        x = x * lax.rsqrt(jnp.mean(x * x, axis=-1, keepdims=True) + rms_eps)
        normed[some, :] = (x * norm_gain).astype(bf16)

    for half in range(halves):
        fetch(2, half)
    for copy in small[1:]:
        copy.wait()

    def q_copy(src_dev, dst_dev, g):
        return send(packet.at[0, g], q_in.at[src_dev - 2, g], q_send.at[dst_dev - 1, g],
                    q_recv.at[src_dev - 2, g], {"sp": dst_dev})

    far_g = 0
    dev1_groups = range(1, groups)

    def kv_copy(t, g):
        return send(packet.at[1 + t, g], kv_in.at[t, g], kv_send.at[t, g], kv_recv.at[t, g], {"sp": 1})

    def kv_last(t, src_dev):
        return send(packet.at[1 + t, far_g], kv_in.at[t, src_dev],
                    kv_last_send.at[t], kv_last_recv.at[t, src_dev], {"sp": 2})

    def offs_copy(src_dev, dst_dev):
        return send(offs, offs_in.at[src_dev], offs_send.at[dst_dev - 1], offs_recv.at[src_dev], {"sp": dst_dev})

    def o_copy(src_dev, dst_dev, g):
        return send(o_out.at[dst_dev - 2, g], o_in.at[src_dev - 1, g], o_send.at[dst_dev - 2, g],
                    o_recv.at[src_dev - 1, g], {"sp": dst_dev})

    def stat_copy(src_dev, dst_dev):
        return send(stat_out.at[dst_dev - 2], stat_in.at[src_dev - 1], stat_send.at[dst_dev - 2],
                    stat_recv.at[src_dev - 1], {"sp": dst_dev})

    def keep(slot, half, y):
        factor = jnp.where(slot == 0, LOG2E * HEAD_DIM ** (-0.5), 1.0).astype(f32)
        y = (y * factor).astype(bf16)
        for u in range(2):
            packet[slot, 2 * half + u] = y[:, u * LANES:(u + 1) * LANES]

    def project(jobs):
        for t, half in jobs:
            slot = slot_of(t)
            weight_copy(q_hbm, slot, half).wait()
        for t, half in jobs:
            slot = slot_of(t)
            keep(slot, half, jnp.dot(
                normed[...], weights[slot, :, half * wide:(half + 1) * wide], preferred_element_type=f32))

    for half in range(halves):
        project([(0, half), (1, half)])

        if half == 0:
            for d in range(n):
                @pl.when(me == d)
                def _(d=d):
                    pl.semaphore_wait(barrier, len(peers[d]) + tp - 1)

        @pl.when(me == 0)
        def _():
            if half == 0:
                for t in range(2):
                    kv_last(t, 0).start()
                offs_copy(0, 1).start()
                offs_copy(0, 2).start()

        @pl.when(me == 1)
        def _():
            if half == 0:
                offs_copy(1, 2).start()

        @pl.when(me == 2)
        def _():
            for g in (2 * half, 2 * half + 1):
                if g in dev1_groups:
                    q_copy(2, 1, g).start()

        @pl.when(me == 3)
        def _():
            for g in (2 * half, 2 * half + 1):
                if g in dev1_groups:
                    q_copy(3, 1, g).start()
                q_copy(3, 2, g).start()

    for copy in out_copies:
        copy.start()
    tap_ref[...] = jnp.zeros_like(tap_ref)
    for c in range(slabs):
        tap_ref[c, :taps] = raw_taps[:, c * LANES:(c + 1) * LANES].astype(f32)
    off_rows[0] = offs[...].astype(f32) * LOG2E
    masses[...] = jnp.zeros_like(masses)
    for copy in gate_copies:
        copy.wait()

    @pl.loop(0, halves)
    def _(c):
        cols = pl.ds(pl.multiple_of(c * wide, wide), wide)
        x = normed[...]
        value = jnp.dot(x, weights[3, :, cols], preferred_element_type=f32).astype(bf16).astype(f32)
        gate = jnp.dot(x, weights[4, :, cols], preferred_element_type=f32).astype(bf16).astype(f32)
        g = (value * jax.nn.sigmoid(gate)).astype(bf16)
        gated[:, cols] = g[rows - HALO:]
        g = g.astype(f32)
        for u in range(2):
            ext[2 * c + u, HALO:, :] = g[:, u * LANES:(u + 1) * LANES]

    halo_copy = send(gated, halo, halo_send, halo_recv, {"sp": lax.rem(me + 1, n)})

    @pl.when(me < n - 1)
    def _():
        halo_copy.start()

    @pl.when(me == 0)
    def _():
        for g in (*dev1_groups, far_g):
            for t in range(2):
                kv_copy(t, g).start()

    project([(2, half) for half in range(halves)])

    @pl.when(me == 1)
    def _():
        for t in range(2):
            kv_last(t, 1).start()

    step = min(128, rows)

    def convolve(starts):
        @pl.loop(0, slabs)
        def _(c):
            for r0 in starts:
                acc = jnp.zeros((step, LANES), f32)
                for k in range(taps):
                    start = HALO - (taps - 1) + k + r0
                    acc = acc + ext[c, start:start + step, :] * tap_ref[c, k:k + 1, :]
                filt[c, r0:r0 + step, :] = acc

    chan_copy = send(stats, stats_got, chan_send, chan_recv, {"tp": partner})

    def convolve_first():
        @pl.when(me > 0)
        def _():
            halo_copy.wait_recv()
            for c in range(slabs):
                ext[c, :HALO, :] = halo[:, c * LANES:(c + 1) * LANES].astype(f32)

        @pl.when(me == 0)
        def _():
            for c in range(slabs):
                ext[c, :HALO, :] = jnp.zeros((HALO, LANES), f32)

        convolve([0])
        total = filt[0]
        for c in range(1, slabs):
            total = total + filt[c]
        lsum = jnp.sum(total, axis=1, keepdims=True)
        mean = lsum * (1.0 / chans)
        square = jnp.zeros((rows, LANES), f32)
        for c in range(slabs):
            dev = filt[c] - mean
            square = square + dev * dev
        lsq = jnp.sum(square, axis=1, keepdims=True)
        stats[...] = jnp.where(low, lsum, lsq)
        chan_copy.start()

    def channel_norm():
        chan_copy.wait()
        mine, other = stats[...], stats_got[...]
        mean = (mine[:, 0:1] + other[:, 0:1]) * (1.0 / total_channels)
        spread = jnp.zeros((rows, 1), f32)
        for s in (mine, other):
            apart = s[:, 0:1] * (1.0 / chans) - mean
            spread = spread + s[:, HEAD_DIM:HEAD_DIM + 1] + chans * apart * apart
        scale = lax.rsqrt(spread * (1.0 / total_channels) + norm_eps)
        for c in range(slabs):
            cols = slice(c * LANES, (c + 1) * LANES)
            y = (filt[c] - mean) * scale * cgain_ref[cols].astype(f32).reshape(1, -1) + cshift_ref[cols].astype(f32).reshape(1, -1)
            conv_ref[:, cols] = (y * jax.nn.sigmoid(y)).astype(bf16)

    tile = min(1024, model)

    def conv_product():
        out_copies[0].wait()
        for c in range(0, model, tile):
            conv_share[:, c:c + tile] = jnp.dot(
                conv_ref[...], out_weights[0, :, c:c + tile], preferred_element_type=f32)

    ri = lax.broadcasted_iota(jnp.int32, (rows, rows), 0)
    ci = lax.broadcasted_iota(jnp.int32, (rows, rows), 1)
    tri = (ri >= ci).astype(bf16)

    def split_keys(k):
        zero = jnp.zeros_like(k)
        return jnp.where(low, k, zero), jnp.where(low, zero, k)

    def split_values(v):
        one = jnp.ones_like(v)
        return jnp.where(low, v, one), jnp.where(low, one, v)

    strict = ci < ri

    def attend(blocks_q, k, v, off, own_first):
        q = jnp.concatenate(blocks_q, axis=0)
        z = lax.dot_general(q, k, (((1,), (1,)), ((), ())), preferred_element_type=f32) + off
        lose = jnp.maximum(z, jnp.log(1.0 + jnp.exp2(jnp.minimum(z, 100.0))) * LOG2E)

        def masked(x):
            if not own_first:
                return x
            head = jnp.where(strict, x[:rows], 0.0)
            return jnp.concatenate([head, x[rows:]], axis=0) if len(blocks_q) > 1 else head

        cum = jnp.dot(masked(lose).astype(bf16), tri, preferred_element_type=f32)
        w = masked(jnp.exp2(z - cum))
        res = jnp.dot(w.astype(bf16), v, preferred_element_type=f32)
        pieces = []
        for r in range(len(blocks_q)):
            some = slice(r * rows, (r + 1) * rows)
            pieces.append((res[some], jnp.broadcast_to(cum[some, 0:1], (rows, LANES))))
        return pieces

    def note(which, g, h, res, total):
        base = 0 if h else HEAD_DIM
        masses[which] = jnp.where(lane == base + g, res, jnp.where(lane == base + 4 + g, total, masses[which]))

    def pair(a, b):
        return jnp.where(low, a, b)

    def near_blocks(g, others):
        keys = split_keys(packet[1, g])
        values = split_values(packet[2, g])
        rest = []
        for h in range(2):
            first, *more = attend([packet[0, g]] + others, keys[h], values[h], off_rows[0, pl.ds(2 * g + h, 1), :], True)
            res, total = first
            own_r[g, h] = res
            own_t[g, h] = jnp.exp2(-total)
            note(0, g, h, res, total)
            rest.append(more)
        return rest

    convolve(range(step, rows, step))

    @pl.when(me != 2)
    def _():
        @pl.loop(0, groups // 2)
        def _(half):
            for u in range(2):
                near_blocks(2 * half + u, [])

    def q_from(src_dev, dst_dev, g):
        return send(packet.at[0, g], q_in.at[src_dev - 2, g], q_send.at[dst_dev - 1, g],
                    q_recv.at[src_dev - 2, g], {"sp": src_dev})

    def kv_from(t, g):
        return send(packet.at[1 + t, g], kv_in.at[t, g], kv_send.at[t, g], kv_recv.at[t, g], {"sp": 0})

    def middle_block(g):
        q_from(3, 2, g).wait_recv()
        return near_blocks(g, [q_in[1, g]])

    @pl.when(me == 2)
    def _():
        rest = middle_block(far_g)
        for h in range(2):
            res, total = rest[h][0]
            far_r[1, h] = res
            far_t[1, h] = jnp.exp2(-total)

    convolve_first()

    @pl.when(me == 1)
    def _():
        offs_copy_back = send(offs, offs_in.at[0], offs_send.at[0], offs_recv.at[0], {"sp": 0})
        offs_copy_back.wait_recv()
        off_rows[1] = offs_in[0].astype(f32) * LOG2E

    @pl.when(me == 2)
    def _():
        for src in range(2):
            send(offs, offs_in.at[src], offs_send.at[1], offs_recv.at[src], {"sp": src}).wait_recv()
            off_rows[1 + src] = offs_in[src].astype(f32) * LOG2E

    def far_blocks():
        @pl.when(me == 2)
        def _():
            for src in (1, 0):
                for t in range(2):
                    send(packet.at[1 + t, far_g], kv_in.at[t, src], kv_last_send.at[t],
                         kv_last_recv.at[t, src], {"sp": src}).wait_recv()
                keys = split_keys(kv_in[0, src])
                values = split_values(kv_in[1, src])
                parts = []
                for h in range(2):
                    (own, own_total), (far, far_total) = attend(
                        [packet[0, far_g], q_in[1, far_g]], keys[h], values[h], off_rows[1 + src, 2 * far_g + h:2 * far_g + h + 1, :], False)
                    own = own_r[far_g, h] + own_t[far_g, h] * own
                    far = far_r[1, h] + far_t[1, h] * far
                    own_r[far_g, h] = own
                    if src:
                        far_r[1, h] = far
                        own_t[far_g, h] = own_t[far_g, h] * jnp.exp2(-own_total)
                        far_t[1, h] = far_t[1, h] * jnp.exp2(-far_total)
                    else:
                        note(0, far_g, h, own, own)
                        note(2, far_g, h, far, far)
                        parts.append(far)
            o_out[1, far_g] = pair(*parts).astype(bf16)
            o_copy(2, 3, far_g).start()

    @pl.loop(1, groups)
    def _(g):
        @pl.when(me == 1)
        def _():
            keys = split_keys(packet[1, g])
            values = split_values(packet[2, g])
            for i in (1, 0):
                q_from(i + 2, 1, g).wait_recv()
            for h in range(2):
                pieces = attend([q_in[1, g], q_in[0, g]], keys[h], values[h], off_rows[0, pl.ds(2 * g + h, 1), :], False)
                for i in (1, 0):
                    res, total = pieces[1 - i]
                    far_r[i, h] = res
                    far_t[i, h] = jnp.exp2(-total)

        @pl.when(me == 2)
        def _():
            rest = middle_block(g)
            for h in range(2):
                note(2, g, h, *rest[h][0])
            o_out[1, g] = pair(rest[0][0][0], rest[1][0][0]).astype(bf16)
            send(o_out.at[1, g], o_in.at[1, g], o_send.at[1, g], o_recv.at[1, g], {"sp": 3}).start()

        @pl.when(g == 1)
        def _():
            channel_norm()
            far_blocks()

        @pl.when(g == 2)
        def _():
            conv_product()

        @pl.when(me == 1)
        def _():
            for t in range(2):
                kv_from(t, g).wait_recv()
            keys = split_keys(kv_in[0, g])
            values = split_values(kv_in[1, g])
            parts = [[], []]
            for h in range(2):
                pieces = attend([q_in[1, g], q_in[0, g], packet[0, g]], keys[h], values[h],
                                off_rows[1, pl.ds(2 * g + h, 1), :], False)
                for i in (1, 0):
                    res = far_r[i, h] + far_t[i, h] * pieces[1 - i][0]
                    note(1 + i, g, h, res, res)
                    parts[i].append(res)
                res = own_r[g, h] + own_t[g, h] * pieces[2][0]
                own_r[g, h] = res
                note(0, g, h, res, res)
            for i in (1, 0):
                o_out[i, g] = pair(*parts[i]).astype(bf16)
            for i in (1, 0):
                send(o_out.at[i, g], o_in.at[0, g], o_send.at[i, g], o_recv.at[0, g], {"sp": i + 2}).start()

    def stat_rows(which):
        t = jnp.transpose(masses[which])
        return jnp.concatenate([t[0:8], t[HEAD_DIM:HEAD_DIM + 8]], axis=0)

    @pl.when(me == 1)
    def _():
        for i in (1, 0):
            stat_out[i] = stat_rows(1 + i)
            stat_copy(1, i + 2).start()

    @pl.when(me == 2)
    def _():
        stat_out[1] = stat_rows(2)
        stat_copy(2, 3).start()

    @pl.when(me == 1)
    def _():
        for t in range(2):
            kv_from(t, far_g).wait_recv()
        keys = split_keys(kv_in[0, far_g])
        values = split_values(kv_in[1, far_g])
        for h in range(2):
            res, _ = attend([packet[0, far_g]], keys[h], values[h], off_rows[1, 2 * far_g + h:2 * far_g + h + 1, :], False)[0]
            res = own_r[far_g, h] + own_t[far_g, h] * res
            own_r[far_g, h] = res
            note(0, far_g, h, res, res)

    blocks = (lax.broadcasted_iota(jnp.int32, (LANES, LANES), 0) // HEAD_DIM
              == lax.broadcasted_iota(jnp.int32, (LANES, LANES), 1) // HEAD_DIM).astype(bf16)

    @pl.when(me == 3)
    def _():
        stat_copy(2, 3).wait_recv()
        rest = jnp.zeros((LANES - 16, rows), f32)
        far_t[0, 0] = jnp.transpose(jnp.concatenate([stat_in[1], rest], axis=0))

    def finish(g):
        cols = slice(g * LANES, (g + 1) * LANES)

        def close(o):
            sq = jnp.dot((o * o).astype(bf16), blocks, preferred_element_type=f32)
            gain = gain_ref[cols].astype(f32).reshape(1, LANES)
            heads_ref[:, cols] = (o * lax.rsqrt(sq * (1.0 / HEAD_DIM) + rms_eps) * gain).astype(bf16)

        own = pair(own_r[g, 0], own_r[g, 1])

        @pl.when(me < 2)
        def _():
            close(own)

        @pl.when(me == 2)
        def _():
            if g == far_g:
                close(own)
            else:
                through = pair(own_t[g, 0], own_t[g, 1])
                send(o_out.at[0, g], o_in.at[0, g], o_send.at[0, g], o_recv.at[0, g], {"sp": 1}).wait_recv()
                close(own + through * o_in[0, g].astype(f32))

        @pl.when(me == 3)
        def _():
            through = pair(own_t[g, 0], own_t[g, 1])
            send(o_out.at[1, g], o_in.at[1, g], o_send.at[1, g], o_recv.at[1, g], {"sp": 2}).wait_recv()
            inner = o_in[1, g].astype(f32)
            if g != far_g:
                tot = far_t[0, 0]
                middle = jnp.exp2(-pair(tot[:, 12 + g:13 + g], tot[:, 4 + g:5 + g]))
                send(o_out.at[1, g], o_in.at[0, g], o_send.at[1, g], o_recv.at[0, g], {"sp": 1}).wait_recv()
                inner = inner + middle * o_in[0, g].astype(f32)
            close(own + through * inner)

    out_copies[1].wait()
    early = groups // 2
    for g in range(early):
        finish(g)
    cut = early * LANES
    for c in range(0, model, tile):
        conv_share[:, c:c + tile] += jnp.dot(
            heads_ref[:, :cut], out_weights[1, :cut, c:c + tile], preferred_element_type=f32)
    for g in range(early, groups):
        finish(g)
    share = rows // tp
    theirs = pl.ds(pl.multiple_of(partner * share, share), share)
    ours = pl.ds(pl.multiple_of(core * share, share), share)
    leaves = []
    for c in range(0, model, tile):
        cols = slice(c, c + tile)
        leaving[:, cols] = (conv_share[theirs, cols] + jnp.dot(
            heads_ref[theirs, cut:], out_weights[1, cut:, cols], preferred_element_type=f32)).astype(bf16)
        copy = send(leaving.at[:, pl.ds(c, tile)], arrived_ref.at[:, pl.ds(c, tile)],
                    out_send.at[c // tile], out_recv.at[c // tile], {"tp": partner})
        copy.start()
        leaves.append(copy)
    for c in range(0, model, tile):
        cols = slice(c, c + tile)
        conv_share[ours, cols] += jnp.dot(
            heads_ref[ours, cut:], out_weights[1, cut:, cols], preferred_element_type=f32)

    mine = stat_rows(0)

    def write_log(m_odd, m_even):
        for g in range(groups):
            log_ref[2 * g:2 * g + 1] = jnp.log(jnp.maximum(m_even[g:g + 1], mass_floor))
            log_ref[2 * g + 1:2 * g + 2] = jnp.log(jnp.maximum(m_odd[g:g + 1], mass_floor))

    @pl.when(me < 2)
    def _():
        write_log(mine[0:4], mine[8:12])

    @pl.when(me == 2)
    def _():
        stat_copy(1, 2).wait_recv()
        far = stat_in[0]
        write_log(mine[0:4] + jnp.exp2(-mine[4:8]) * far[0:4], mine[8:12] + jnp.exp2(-mine[12:16]) * far[8:12])

    @pl.when(me == 3)
    def _():
        send(stat_out.at[1], stat_in.at[0], stat_send.at[1], stat_recv.at[0], {"sp": 1}).wait_recv()
        far, mid = stat_in[0], stat_in[1]
        odd = mid[0:4] + jnp.exp2(-mid[4:8]) * far[0:4]
        even = mid[8:12] + jnp.exp2(-mid[12:16]) * far[8:12]
        write_log(mine[0:4] + jnp.exp2(-mine[4:8]) * odd, mine[8:12] + jnp.exp2(-mine[12:16]) * even)

    for c in range(0, model, tile):
        cols = slice(c, c + tile)
        leaves[c // tile].wait()
        out_ref[:, cols] = (conv_share[ours, cols] + arrived_ref[:, cols].astype(f32)).astype(bf16)

    @pl.when(me < n - 1)
    def _():
        halo_copy.wait_send()

    @pl.when(me == 0)
    def _():
        offs_copy(0, 1).wait_send()
        offs_copy(0, 2).wait_send()
        for t in range(2):
            for g in range(groups):
                kv_copy(t, g).wait_send()
            kv_last(t, 0).wait_send()

    @pl.when(me == 1)
    def _():
        offs_copy(1, 2).wait_send()
        for t in range(2):
            kv_last(t, 1).wait_send()
        for i in (1, 0):
            for g in dev1_groups:
                o_copy(1, i + 2, g).wait_send()
            stat_copy(1, i + 2).wait_send()

    @pl.when(me == 2)
    def _():
        for g in dev1_groups:
            q_copy(2, 1, g).wait_send()
        for g in range(groups):
            o_copy(2, 3, g).wait_send()
        stat_copy(2, 3).wait_send()

    @pl.when(me == 3)
    def _():
        for g in range(groups):
            if g in dev1_groups:
                q_copy(3, 1, g).wait_send()
            q_copy(3, 2, g).wait_send()


def place(mixed, mass_log, out_ref, log_ref, sem):
    copies = [
        pltpu.make_async_copy(mixed, out_ref, sem.at[0]),
        pltpu.make_async_copy(mass_log, log_ref, sem.at[1]),
    ]
    for copy in copies:
        copy.start()
    for copy in copies:
        copy.wait()


def local(n, tp,
    stream, norm_gain, query_weight, key_weight, value_weight, filter_input, filter_gate,
    score_offset, head_gain, filter_taps, channel_gain, channel_shift, attend_out, filter_out,
):
    f32, bf16 = jnp.float32, jnp.bfloat16
    rows = stream.shape[1]
    heads = score_offset.shape[2]
    groups = heads * HEAD_DIM // LANES
    chans = filter_input.shape[1]
    slabs = chans // LANES
    taps = filter_taps.shape[0]
    model = stream.shape[2]
    share = rows // tp
    tiles = model // min(1024, model)

    vmem = pl.BlockSpec(memory_space=pltpu.VMEM)
    hbm = pl.BlockSpec(memory_space=pltpu.HBM)
    dma = pltpu.SemaphoreType.DMA
    mixed, mass_log = pl.pallas_call(
        functools.partial(kernel, n, tp, taps, chans * tp),
        out_shape=(pltpu.VMEM((share, model), bf16), pltpu.VMEM((heads, rows), f32)),
        in_specs=[hbm] * 14,
        out_specs=(vmem,) * 2,
        scratch_shapes=[
            pltpu.VMEM((model,), bf16),
            pltpu.VMEM((heads, rows), bf16),
            pltpu.VMEM((taps, chans), bf16),
            pltpu.VMEM((chans,), bf16),
            pltpu.VMEM((chans,), bf16),
            pltpu.VMEM((chans,), bf16),
            pltpu.VMEM((rows, model), bf16),
            pltpu.VMEM((rows, model), bf16),
            pltpu.VMEM((5, model, chans), bf16),
            pltpu.VMEM((2, chans, model), bf16),
            pltpu.VMEM((3, groups, rows, LANES), bf16),
            pltpu.VMEM((2, groups, rows, LANES), bf16),
            pltpu.VMEM((2, groups, rows, LANES), bf16),
            pltpu.VMEM((2, heads, rows), bf16),
            pltpu.VMEM((2, groups, rows, LANES), bf16),
            pltpu.VMEM((2, groups, rows, LANES), bf16),
            pltpu.VMEM((2, 16, rows), f32),
            pltpu.VMEM((2, 16, rows), f32),
            pltpu.VMEM((groups, 2, rows, LANES), f32),
            pltpu.VMEM((groups, 2, rows, LANES), f32),
            pltpu.VMEM((2, 2, rows, LANES), f32),
            pltpu.VMEM((2, 2, rows, LANES), f32),
            pltpu.VMEM((3, rows, LANES), f32),
            pltpu.VMEM((3, heads, rows), f32),
            pltpu.VMEM((slabs, taps + -taps % 8, LANES), f32),
            pltpu.VMEM((rows, heads * HEAD_DIM), bf16),
            pltpu.VMEM((rows, chans), bf16),
            pltpu.VMEM((rows, model), f32),
            pltpu.VMEM((share, model), bf16),
            pltpu.VMEM((share, model), bf16),
            pltpu.VMEM((HALO, chans), bf16),
            pltpu.VMEM((HALO, chans), bf16),
            pltpu.VMEM((slabs, HALO + rows, LANES), f32),
            pltpu.VMEM((slabs, rows, LANES), f32),
            pltpu.VMEM((rows, LANES), f32),
            pltpu.VMEM((rows, LANES), f32),
            dma((6,)), dma((rows // min(64, rows),)), dma((5, chans // (2 * LANES))), dma((2,)), dma((2, groups)), dma((2, groups)), dma((2, groups)), dma((2, groups)), dma((2,)), dma((2, 2)), dma((2,)), dma((2,)),
            dma((2, groups)), dma((2, groups)), dma((2,)), dma((2,)), dma((tiles,)), dma((tiles,)), dma, dma, dma, dma,
        ],
        compiler_params=pltpu.CompilerParams(
            collective_id=0, has_side_effects=True, vmem_limit_bytes=56 * 1024 * 1024),
    )(stream[0], norm_gain, score_offset[0].T, filter_taps, head_gain, channel_gain, channel_shift,
      query_weight, key_weight, value_weight, filter_input, filter_gate, attend_out, filter_out)
    mixed, mass_log = pl.pallas_call(
        place,
        out_shape=(
            jax.ShapeDtypeStruct((share, model), bf16),
            jax.ShapeDtypeStruct((heads, rows), f32),
        ),
        in_specs=[vmem] * 2,
        out_specs=(hbm,) * 2,
        scratch_shapes=[dma((2,))],
    )(*[pltpu.with_memory_space_constraint(a, pltpu.VMEM) for a in (mixed, mass_log)])
    return (mixed[None], mass_log.T[None])


def shifted(value, axis, steps):
    count = lax.axis_size(axis)
    first, last = (max(0, -steps), min(count, count - steps))
    return lax.ppermute(value, axis, [(source, source + steps) for source in range(first, last)])


def local_ring(
    stream,
    norm_gain,
    query_weight,
    key_weight,
    value_weight,
    filter_input,
    filter_gate,
    score_offset,
    head_gain,
    filter_taps,
    channel_gain,
    channel_shift,
    attend_out,
    filter_out,
):
    rows_here = stream.shape[1]
    total_channels = filter_input.shape[1] * lax.axis_size("tp")
    xfloat = stream[0].astype(jnp.float32)
    normed = xfloat * lax.rsqrt(jnp.mean(xfloat * xfloat, axis=-1, keepdims=True) + rms_eps)
    normed = (normed * norm_gain.astype(jnp.float32)).astype(jnp.bfloat16)

    def project(weight):
        return jnp.dot(normed, weight, preferred_element_type=jnp.float32).astype(jnp.bfloat16)

    queries = project(query_weight)
    keys_here = project(key_weight)
    values_here = project(value_weight)
    conv_in = project(filter_input)
    conv_gate = project(filter_gate)
    offsets_here = score_offset[0]
    heads_here = offsets_here.shape[1]
    first_pos = lax.axis_index("sp") * rows_here
    position = first_pos + jnp.arange(rows_here, dtype=jnp.int32)
    qheads = queries.reshape(rows_here, heads_here, HEAD_DIM)

    def absorb(state_now, kblock, vblock, oblock, first_key):
        attended, weight_mass, survive = state_now
        span = kblock.shape[0]
        kblock = kblock.reshape(span, heads_here, HEAD_DIM)
        vblock = vblock.reshape(span, heads_here, HEAD_DIM)
        scores = jnp.einsum(
            "thd,shd->hts", qheads, kblock, preferred_element_type=jnp.float32
        ) * HEAD_DIM ** (-0.5)
        scores = scores + oblock.astype(jnp.float32).T[:, None, :]
        key_pos = first_key + jnp.arange(span, dtype=jnp.int32)
        strict = ((key_pos[None, :] < position[:, None]) & (key_pos[None, :] >= 0))[None]
        losing = jnp.where(strict, jax.nn.log_sigmoid(-scores), 0.0)
        beyond = lax.cumsum(losing, axis=2, reverse=True) - losing + survive[:, :, None]
        weights = jnp.where(strict, jnp.exp(jax.nn.log_sigmoid(scores) + beyond), 0.0)
        weight_mass = weight_mass + jnp.sum(weights, axis=2)
        attended = attended + jnp.einsum(
            "hts,shd->thd", weights.astype(jnp.bfloat16), vblock, preferred_element_type=jnp.float32
        )
        survive = survive + jnp.sum(losing, axis=2)
        return (attended, weight_mass, survive)

    initial = (
        jnp.zeros((rows_here, heads_here, HEAD_DIM), jnp.float32),
        jnp.zeros((heads_here, rows_here), jnp.float32),
        jnp.zeros((heads_here, rows_here), jnp.float32),
    )
    state_now = absorb(initial, keys_here, values_here, offsets_here, first_pos)

    def pass_turn(turn_index, carried):
        state_now, travelling = carried
        travelling = shifted((travelling[0], travelling[1], travelling[2]), "sp", 1)
        first_key = first_pos - (turn_index + 1) * rows_here
        state_now = absorb(state_now, travelling[0], travelling[1], travelling[2], first_key)
        return (state_now, travelling)

    state_now, travelling = lax.fori_loop(
        0, lax.axis_size("sp") - 1, pass_turn, (state_now, (keys_here, values_here, offsets_here))
    )
    attended, weight_mass, survive = state_now
    head_scale = lax.rsqrt(jnp.mean(attended * attended, axis=-1, keepdims=True) + rms_eps)
    heads_flat = attended * head_scale * head_gain.astype(jnp.float32).reshape(heads_here, HEAD_DIM)
    heads_flat = heads_flat.astype(jnp.bfloat16).reshape(rows_here, heads_here * HEAD_DIM)
    mass_log = jnp.log(jnp.maximum(weight_mass.T, mass_floor))
    gated_rows = (
        conv_in.astype(jnp.float32) * jax.nn.sigmoid(conv_gate.astype(jnp.float32))
    ).astype(jnp.bfloat16)
    reach_back = filter_taps.shape[0] - 1
    earlier = shifted(gated_rows[rows_here - reach_back :], "sp", 1)
    extended = jnp.concatenate([earlier, gated_rows], axis=0).astype(jnp.float32)
    tap_values = filter_taps.astype(jnp.float32)
    filtered = jnp.zeros((rows_here, gated_rows.shape[1]), jnp.float32)
    for tap_index in range(reach_back + 1):
        filtered = filtered + extended[tap_index : tap_index + rows_here] * tap_values[tap_index]
    center = lax.psum(jnp.sum(filtered, axis=-1), "tp") / total_channels
    deviation = filtered - center[:, None]
    spread = lax.psum(jnp.sum(deviation * deviation, axis=-1), "tp") / total_channels
    conv_out = jax.nn.silu(
        deviation * lax.rsqrt(spread[:, None] + norm_eps) * channel_gain.astype(jnp.float32)
        + channel_shift.astype(jnp.float32)
    ).astype(jnp.bfloat16)
    mixed_out = lax.psum_scatter(
        (
            jnp.dot(heads_flat, attend_out, preferred_element_type=jnp.float32)
            + jnp.dot(conv_out, filter_out, preferred_element_type=jnp.float32)
        ).astype(jnp.bfloat16),
        "tp",
        scatter_dimension=0,
        tiled=True,
    )
    return (mixed_out[None], mass_log[None])


def solution(mesh):
    n, tp = mesh.shape["sp"], mesh.shape["tp"]

    def choose(*args):
        rows, heads, chans = args[0].shape[1], args[7].shape[2], args[5].shape[1]
        same = args[2].shape[1] == chans and heads * HEAD_DIM == 4 * LANES == chans
        if n == 4 and tp == 2 and same and rows % 128 == 0:
            return local(n, tp, *args)
        return local_ring(*args)

    return jax.shard_map(
        choose,
        mesh=mesh,
        in_specs=(
            P("fs", "sp", None), P(), P(None, "tp"), P(None, "tp"), P(None, "tp"),
            P(None, "tp"), P(None, "tp"), P("fs", "sp", "tp"), P("tp"), P(None, "tp"),
            P("tp"), P("tp"), P("tp", None), P("tp", None),
        ),
        out_specs=(P("fs", ("sp", "tp"), None), P("fs", "sp", "tp")),
        check_vma=False,
    )
```

```python
import functools

import jax
import jax.numpy as jnp
from jax import lax
from jax.experimental import pallas as pl
from jax.experimental.pallas import tpu as pltpu
from jax.sharding import PartitionSpec as P

HEAD_DIM = 64

rms_eps = 1e-06
norm_eps = 1e-05
mass_floor = 0.01
HALO = 32
LANES = 128
LOG2E = 1.4426950408889634
MESH = pl.DeviceIdType.MESH


def kernel(
    n, tp, taps, total_channels,
    stream_hbm, ngain_hbm, offs_hbm, taps_hbm, gain_hbm, cgain_hbm, cshift_hbm,
    q_hbm, k_hbm, v_hbm, in_hbm, gate_hbm, attend_hbm, filter_hbm,
    out_ref, log_ref,
    ngain, offs, raw_taps, gain_ref, cgain_ref, cshift_ref,
    stream, normed, weights, out_weights, packet, q_in, kv_in, offs_in, o_out, o_in, stat_out, stat_in,
    own_r, own_t, far_r, far_t, masses, off_rows, tap_ref, heads_ref, conv_ref, conv_share, leaving, arrived_ref,
    gated, halo, ext, filt, stats, stats_got,
    small_sem, stream_sem, weight_sem, out_weight_sem, q_send, q_recv, kv_send, kv_recv, kv_last_send, kv_last_recv, offs_send, offs_recv,
    o_send, o_recv, stat_send, stat_recv, out_send, out_recv, halo_send, halo_recv, chan_send, chan_recv, entered,
):
    f32, bf16 = jnp.float32, jnp.bfloat16
    me = lax.axis_index("sp")
    core = lax.axis_index("tp")
    partner = 1 - core
    rows, model = normed.shape
    chans = in_hbm.shape[1]
    groups = packet.shape[1]
    slabs = chans // LANES
    lane = lax.broadcasted_iota(jnp.int32, (rows, LANES), 1)
    low = lane < HEAD_DIM

    def local_copy(src, dst, sem):
        return pltpu.make_async_copy(src, dst, sem)

    def send(src, dst, send_sem, recv_sem, to):
        return pltpu.make_async_remote_copy(
            src_ref=src, dst_ref=dst, send_sem=send_sem, recv_sem=recv_sem,
            device_id=to, device_id_type=MESH)

    projections = (q_hbm, k_hbm, v_hbm)
    first_order, other_order = (1, 2, 0), (0, 1, 2)

    def slot_of(t):
        return jnp.where(me == 0, first_order[t], other_order[t])

    wide = 2 * LANES
    halves = chans // wide

    def weight_copy(w, slot, half):
        cols = pl.ds(half * wide, wide)
        return local_copy(w.at[:, cols], weights.at[slot, :, cols], weight_sem.at[slot, half])

    def fetch(t, half):
        for order, here in ((first_order, me == 0), (other_order, me != 0)):
            @pl.when(here)
            def _(s=order[t]):
                weight_copy(projections[s], s, half).start()

    band = min(64, rows)

    def stream_copy(c):
        some = pl.ds(pl.multiple_of(c * band, band), band)
        return local_copy(stream_hbm.at[some], stream.at[some], stream_sem.at[c])

    small = [local_copy(a, b, small_sem.at[t]) for t, (a, b) in enumerate((
        (ngain_hbm, ngain), (offs_hbm, offs), (taps_hbm, raw_taps), (gain_hbm, gain_ref),
        (cgain_hbm, cgain_ref), (cshift_hbm, cshift_ref)))]
    gate_copies = [weight_copy(w, 3 + t, half) for half in range(halves) for t, w in enumerate((in_hbm, gate_hbm))]
    out_copies = [local_copy(w, out_weights.at[t], out_weight_sem.at[t]) for t, w in enumerate((filter_hbm, attend_hbm))]
    for c in range(rows // band):
        stream_copy(c).start()
    small[0].start()
    for t in range(2):
        fetch(t, 0)
    for copy in small[1:]:
        copy.start()

    barrier = pltpu.get_barrier_semaphore()
    peers = {0: (1,), 1: (0, 2, 3), 2: (1, 3), 3: (1, 2)}
    pl.semaphore_signal(barrier, inc=1, device_id={"tp": partner}, device_id_type=MESH)
    for d in range(n):
        @pl.when(me == d)
        def _(d=d):
            for p in peers[d]:
                pl.semaphore_signal(barrier, inc=1, device_id={"sp": p}, device_id_type=MESH)

    small[0].wait()
    norm_gain = ngain[...].astype(f32).reshape(1, -1)

    @pl.loop(0, rows // band)
    def _(c):
        stream_copy(c).wait()

        @pl.when(c == 0)
        def _():
            for half in range(1, halves):
                for t in range(2):
                    fetch(t, half)
            for copy in gate_copies:
                copy.start()

        some = pl.ds(pl.multiple_of(c * band, band), band)
        x = stream[some, :].astype(f32)
        x = x * lax.rsqrt(jnp.mean(x * x, axis=-1, keepdims=True) + rms_eps)
        normed[some, :] = (x * norm_gain).astype(bf16)

    for half in range(halves):
        fetch(2, half)
    for copy in small[1:]:
        copy.wait()

    def q_copy(src_dev, dst_dev, g):
        return send(packet.at[0, g], q_in.at[src_dev - 2, g], q_send.at[dst_dev - 1, g],
                    q_recv.at[src_dev - 2, g], {"sp": dst_dev})

    far_g = 0
    dev1_groups = range(1, groups)

    def kv_copy(src_dev, t, g):
        return send(packet.at[1 + t, g], kv_in.at[t, g], kv_send.at[t, g], kv_recv.at[t, g], {"sp": src_dev + 1})

    def kv_last(t, src_dev):
        return send(packet.at[1 + t, far_g], kv_in.at[t, src_dev],
                    kv_last_send.at[t], kv_last_recv.at[t, src_dev], {"sp": 2})

    def offs_copy(src_dev, dst_dev):
        return send(offs, offs_in.at[src_dev], offs_send.at[dst_dev - 1], offs_recv.at[src_dev], {"sp": dst_dev})

    def o_copy(src_dev, dst_dev, g):
        return send(o_out.at[dst_dev - 2, g], o_in.at[src_dev - 1, g], o_send.at[dst_dev - 2, g],
                    o_recv.at[src_dev - 1, g], {"sp": dst_dev})

    def stat_copy(src_dev, dst_dev):
        return send(stat_out.at[dst_dev - 2], stat_in.at[src_dev - 1], stat_send.at[dst_dev - 2],
                    stat_recv.at[src_dev - 1], {"sp": dst_dev})

    def keep(slot, half, y):
        factor = jnp.where(slot == 0, LOG2E * HEAD_DIM ** (-0.5), 1.0).astype(f32)
        y = (y * factor).astype(bf16)
        for u in range(2):
            packet[slot, 2 * half + u] = y[:, u * LANES:(u + 1) * LANES]

    def project(jobs):
        for t, half in jobs:
            slot = slot_of(t)
            weight_copy(q_hbm, slot, half).wait()
        for t, half in jobs:
            slot = slot_of(t)
            keep(slot, half, jnp.dot(
                normed[...], weights[slot, :, half * wide:(half + 1) * wide], preferred_element_type=f32))

    for half in range(halves):
        project([(0, half), (1, half)])

        if half == 0:
            for d in range(n):
                @pl.when(me == d)
                def _(d=d):
                    pl.semaphore_wait(barrier, len(peers[d]) + tp - 1)

        groups_here = (2 * half, 2 * half + 1)

        @pl.when(me == 0)
        def _():
            if half == 0:
                offs_copy(0, 1).start()
                for t in range(2):
                    kv_copy(0, t, 1).start()

        @pl.when(me == 1)
        def _():
            if half == 0:
                pl.semaphore_signal(entered, inc=1, device_id={"sp": 0}, device_id_type=MESH)
                offs_copy(1, 2).start()

        @pl.when(me == 2)
        def _():
            if half == 0:
                offs_copy(2, 3).start()
            q_copy(2, 1, 1 + half).start()
            for g in groups_here:
                if g in dev1_groups:
                    kv_copy(2, 0, g).start()

        @pl.when(me == 3)
        def _():
            q_copy(3, 1, 1 + half).start()
            if half == 1:
                q_copy(3, 2, far_g).start()

    for copy in out_copies:
        copy.start()
    tap_ref[...] = jnp.zeros_like(tap_ref)
    for c in range(slabs):
        tap_ref[c, :taps] = raw_taps[:, c * LANES:(c + 1) * LANES].astype(f32)
    off_rows[0] = offs[...].astype(f32) * LOG2E
    masses[...] = jnp.zeros_like(masses)
    for copy in gate_copies:
        copy.wait()

    @pl.loop(0, halves)
    def _(c):
        cols = pl.ds(pl.multiple_of(c * wide, wide), wide)
        x = normed[...]
        value = jnp.dot(x, weights[3, :, cols], preferred_element_type=f32).astype(bf16).astype(f32)
        gate = jnp.dot(x, weights[4, :, cols], preferred_element_type=f32).astype(bf16).astype(f32)
        g = (value * jax.nn.sigmoid(gate)).astype(bf16)
        gated[:, cols] = g[rows - HALO:]
        g = g.astype(f32)
        for u in range(2):
            ext[2 * c + u, HALO:, :] = g[:, u * LANES:(u + 1) * LANES]

    halo_copy = send(gated, halo, halo_send, halo_recv, {"sp": lax.rem(me + 1, n)})

    @pl.when(me == 0)
    def _():
        pl.semaphore_wait(entered, 1)
        offs_copy(0, 2).start()
        for t in range(2):
            kv_last(t, 0).start()
        for g in dev1_groups[1:]:
            for t in range(2):
                kv_copy(0, t, g).start()

    for d in (2, 3):
        @pl.when(me == d)
        def _(d=d):
            for g in dev1_groups[2:]:
                q_copy(d, 1, g).start()

    @pl.when(me < n - 1)
    def _():
        halo_copy.start()

    @pl.when(me == 0)
    def _():
        for t in range(2):
            kv_copy(0, t, far_g).start()

    project([(2, half) for half in range(halves)])

    @pl.when(me == 1)
    def _():
        for t in range(2):
            kv_last(t, 1).start()

    @pl.when(me == 2)
    def _():
        for g in dev1_groups:
            kv_copy(2, 1, g).start()

    step = min(128, rows)

    def convolve(starts):
        @pl.loop(0, slabs)
        def _(c):
            for r0 in starts:
                acc = jnp.zeros((step, LANES), f32)
                for k in range(taps):
                    start = HALO - (taps - 1) + k + r0
                    acc = acc + ext[c, start:start + step, :] * tap_ref[c, k:k + 1, :]
                filt[c, r0:r0 + step, :] = acc

    chan_copy = send(stats, stats_got, chan_send, chan_recv, {"tp": partner})

    def convolve_first():
        @pl.when(me > 0)
        def _():
            halo_copy.wait_recv()
            for c in range(slabs):
                ext[c, :HALO, :] = halo[:, c * LANES:(c + 1) * LANES].astype(f32)

        @pl.when(me == 0)
        def _():
            for c in range(slabs):
                ext[c, :HALO, :] = jnp.zeros((HALO, LANES), f32)

        convolve([0])
        total = filt[0]
        for c in range(1, slabs):
            total = total + filt[c]
        lsum = jnp.sum(total, axis=1, keepdims=True)
        mean = lsum * (1.0 / chans)
        square = jnp.zeros((rows, LANES), f32)
        for c in range(slabs):
            dev = filt[c] - mean
            square = square + dev * dev
        lsq = jnp.sum(square, axis=1, keepdims=True)
        stats[...] = jnp.where(low, lsum, lsq)
        chan_copy.start()

    def channel_norm():
        chan_copy.wait()
        mine, other = stats[...], stats_got[...]
        mean = (mine[:, 0:1] + other[:, 0:1]) * (1.0 / total_channels)
        spread = jnp.zeros((rows, 1), f32)
        for s in (mine, other):
            apart = s[:, 0:1] * (1.0 / chans) - mean
            spread = spread + s[:, HEAD_DIM:HEAD_DIM + 1] + chans * apart * apart
        scale = lax.rsqrt(spread * (1.0 / total_channels) + norm_eps)
        for c in range(slabs):
            cols = slice(c * LANES, (c + 1) * LANES)
            y = (filt[c] - mean) * scale * cgain_ref[cols].astype(f32).reshape(1, -1) + cshift_ref[cols].astype(f32).reshape(1, -1)
            conv_ref[:, cols] = (y * jax.nn.sigmoid(y)).astype(bf16)

    tile = min(1024, model)

    def conv_product():
        out_copies[0].wait()
        for c in range(0, model, tile):
            conv_share[:, c:c + tile] = jnp.dot(
                conv_ref[...], out_weights[0, :, c:c + tile], preferred_element_type=f32)

    ri = lax.broadcasted_iota(jnp.int32, (rows, rows), 0)
    ci = lax.broadcasted_iota(jnp.int32, (rows, rows), 1)
    tri = (ri >= ci).astype(bf16)

    def split_keys(k):
        zero = jnp.zeros_like(k)
        return jnp.where(low, k, zero), jnp.where(low, zero, k)

    def split_values(v):
        one = jnp.ones_like(v)
        return jnp.where(low, v, one), jnp.where(low, one, v)

    strict = ci < ri

    def attend(blocks_q, k, v, off, own_first):
        q = jnp.concatenate(blocks_q, axis=0)
        z = lax.dot_general(q, k, (((1,), (1,)), ((), ())), preferred_element_type=f32) + off
        lose = jnp.maximum(z, jnp.log(1.0 + jnp.exp2(jnp.minimum(z, 100.0))) * LOG2E)

        def masked(x):
            if not own_first:
                return x
            head = jnp.where(strict, x[:rows], 0.0)
            return jnp.concatenate([head, x[rows:]], axis=0) if len(blocks_q) > 1 else head

        cum = jnp.dot(masked(lose).astype(bf16), tri, preferred_element_type=f32)
        w = masked(jnp.exp2(z - cum))
        res = jnp.dot(w.astype(bf16), v, preferred_element_type=f32)
        pieces = []
        for r in range(len(blocks_q)):
            some = slice(r * rows, (r + 1) * rows)
            pieces.append((res[some], jnp.broadcast_to(cum[some, 0:1], (rows, LANES))))
        return pieces

    def note(which, g, h, res, total):
        base = 0 if h else HEAD_DIM
        masses[which] = jnp.where(lane == base + g, res, jnp.where(lane == base + 4 + g, total, masses[which]))

    def pair(a, b):
        return jnp.where(low, a, b)

    def near_blocks(g, others):
        keys = split_keys(packet[1, g])
        values = split_values(packet[2, g])
        rest = []
        for h in range(2):
            first, *more = attend([packet[0, g]] + others, keys[h], values[h], off_rows[0, pl.ds(2 * g + h, 1), :], True)
            res, total = first
            own_r[g, h] = res
            own_t[g, h] = jnp.exp2(-total)
            note(0, g, h, res, total)
            rest.append(more)
        return rest

    convolve(range(step, rows, step))

    def q_from(src_dev, dst_dev, g):
        return send(packet.at[0, g], q_in.at[src_dev - 2, g], q_send.at[dst_dev - 1, g],
                    q_recv.at[src_dev - 2, g], {"sp": src_dev})

    def kv_from(src_dev, g):
        for t in range(2):
            send(packet.at[1 + t, g], kv_in.at[t, g], kv_send.at[t, g], kv_recv.at[t, g], {"sp": src_dev}).wait_recv()
        return split_keys(kv_in[0, g]), split_values(kv_in[1, g])

    def offs_from(src_dev, dst_dev, row):
        send(offs, offs_in.at[src_dev], offs_send.at[dst_dev - 1], offs_recv.at[src_dev], {"sp": src_dev}).wait_recv()
        off_rows[row] = offs_in[src_dev].astype(f32) * LOG2E

    def off_of(row, g, h):
        return off_rows[row, pl.ds(2 * g + h, 1), :]

    def stat_rows(which):
        t = jnp.transpose(masses[which])
        return jnp.concatenate([t[0:8], t[HEAD_DIM:HEAD_DIM + 8]], axis=0)

    @pl.when((me == 0) | (me == 3))
    def _():
        @pl.loop(0, groups // 2)
        def _(half):
            for u in range(2):
                near_blocks(2 * half + u, [])

    @pl.when(me == 1)
    def _():
        near_blocks(far_g, [])
        offs_from(0, 1, 1)

        @pl.loop(1, groups)
        def _(g):
            for i in (1, 0):
                q_from(i + 2, 1, g).wait_recv()
            rest = near_blocks(g, [q_in[1, g], q_in[0, g]])
            for h in range(2):
                for i in (1, 0):
                    res, total = rest[h][1 - i]
                    far_r[i, h] = res
                    far_t[i, h] = jnp.exp2(-total)
            keys, values = kv_from(0, g)
            parts = [[], []]
            for h in range(2):
                pieces = attend([q_in[1, g], q_in[0, g], packet[0, g]], keys[h], values[h], off_of(1, g, h), False)
                for i in (1, 0):
                    res = far_r[i, h] + far_t[i, h] * pieces[1 - i][0]
                    note(1 + i, g, h, res, res)
                    parts[i].append(res)
                res = own_r[g, h] + own_t[g, h] * pieces[2][0]
                own_r[g, h] = res
                note(0, g, h, res, res)
            for i in (1, 0):
                o_out[i, g] = pair(*parts[i]).astype(bf16)
            for i in (1, 0):
                send(o_out.at[i, g], o_in.at[0, g], o_send.at[i, g], o_recv.at[0, g], {"sp": i + 2}).start()

        for i in (1, 0):
            stat_out[i] = stat_rows(1 + i)
            stat_copy(1, i + 2).start()

    @pl.when(me == 2)
    def _():
        near_blocks(1, [])

        @pl.loop(1, 2)
        def _(half):
            for u in range(2):
                near_blocks(2 * half + u, [])

    convolve_first()

    @pl.when(me == 2)
    def _():
        q_from(3, 2, far_g).wait_recv()
        rest = near_blocks(far_g, [q_in[1, far_g]])
        for h in range(2):
            res, total = rest[h][0]
            far_r[1, h] = res
            far_t[1, h] = jnp.exp2(-total)
        offs_from(1, 2, 2)
        offs_from(0, 2, 1)
        for src in (1, 0):
            for t in range(2):
                send(packet.at[1 + t, far_g], kv_in.at[t, src], kv_last_send.at[t],
                     kv_last_recv.at[t, src], {"sp": src}).wait_recv()
            keys = split_keys(kv_in[0, src])
            values = split_values(kv_in[1, src])
            parts = []
            for h in range(2):
                (own, own_total), (far, far_total) = attend(
                    [packet[0, far_g], q_in[1, far_g]], keys[h], values[h], off_rows[1 + src, 2 * far_g + h:2 * far_g + h + 1, :], False)
                own = own_r[far_g, h] + own_t[far_g, h] * own
                far = far_r[1, h] + far_t[1, h] * far
                own_r[far_g, h] = own
                if src:
                    far_r[1, h] = far
                    own_t[far_g, h] = own_t[far_g, h] * jnp.exp2(-own_total)
                    far_t[1, h] = far_t[1, h] * jnp.exp2(-far_total)
                else:
                    note(0, far_g, h, own, own)
                    note(2, far_g, h, far, far)
                    parts.append(far)
        o_out[1, far_g] = pair(*parts).astype(bf16)
        o_out[1, far_g] = pair(*parts).astype(bf16)
        o_copy(2, 3, far_g).start()
        stat_out[1] = stat_rows(2)
        stat_copy(2, 3).start()

    channel_norm()
    conv_product()

    @pl.when(me == 1)
    def _():
        keys, values = kv_from(0, far_g)
        for h in range(2):
            res, _ = attend([packet[0, far_g]], keys[h], values[h], off_of(1, far_g, h), False)[0]
            res = own_r[far_g, h] + own_t[far_g, h] * res
            own_r[far_g, h] = res
            note(0, far_g, h, res, res)

    @pl.when(me == 3)
    def _():
        offs_from(2, 3, 1)
        for g in dev1_groups:
            keys, values = kv_from(2, g)
            for h in range(2):
                res, total = attend([packet[0, g]], keys[h], values[h], off_of(1, g, h), False)[0]
                through = own_t[g, h]
                res = own_r[g, h] + through * res
                own_r[g, h] = res
                own_t[g, h] = through * jnp.exp2(-total)
                near = masses[0][:, (HEAD_DIM, 0)[h] + 4 + g:(HEAD_DIM, 0)[h] + 5 + g]
                note(0, g, h, res, total + near)

    blocks = (lax.broadcasted_iota(jnp.int32, (LANES, LANES), 0) // HEAD_DIM
              == lax.broadcasted_iota(jnp.int32, (LANES, LANES), 1) // HEAD_DIM).astype(bf16)

    def finish(g):
        cols = slice(g * LANES, (g + 1) * LANES)

        def close(o):
            sq = jnp.dot((o * o).astype(bf16), blocks, preferred_element_type=f32)
            gain = gain_ref[cols].astype(f32).reshape(1, LANES)
            heads_ref[:, cols] = (o * lax.rsqrt(sq * (1.0 / HEAD_DIM) + rms_eps) * gain).astype(bf16)

        own = pair(own_r[g, 0], own_r[g, 1])

        @pl.when(me < 2)
        def _():
            close(own)

        @pl.when(me == 2)
        def _():
            if g == far_g:
                close(own)
            else:
                through = pair(own_t[g, 0], own_t[g, 1])
                send(o_out.at[0, g], o_in.at[0, g], o_send.at[0, g], o_recv.at[0, g], {"sp": 1}).wait_recv()
                close(own + through * o_in[0, g].astype(f32))

        @pl.when(me == 3)
        def _():
            through = pair(own_t[g, 0], own_t[g, 1])
            src = 2 if g == far_g else 1
            send(o_out.at[1, g], o_in.at[src - 1, g], o_send.at[1, g], o_recv.at[src - 1, g], {"sp": src}).wait_recv()
            close(own + through * o_in[src - 1, g].astype(f32))

    out_copies[1].wait()
    early = groups // 2
    for g in range(early):
        finish(g)
    cut = early * LANES
    for c in range(0, model, tile):
        conv_share[:, c:c + tile] += jnp.dot(
            heads_ref[:, :cut], out_weights[1, :cut, c:c + tile], preferred_element_type=f32)
    for g in range(early, groups):
        finish(g)
    share = rows // tp
    theirs = pl.ds(pl.multiple_of(partner * share, share), share)
    ours = pl.ds(pl.multiple_of(core * share, share), share)
    leaves = []
    for c in range(0, model, tile):
        cols = slice(c, c + tile)
        leaving[:, cols] = (conv_share[theirs, cols] + jnp.dot(
            heads_ref[theirs, cut:], out_weights[1, cut:, cols], preferred_element_type=f32)).astype(bf16)
        copy = send(leaving.at[:, pl.ds(c, tile)], arrived_ref.at[:, pl.ds(c, tile)],
                    out_send.at[c // tile], out_recv.at[c // tile], {"tp": partner})
        copy.start()
        leaves.append(copy)
    for c in range(0, model, tile):
        cols = slice(c, c + tile)
        conv_share[ours, cols] += jnp.dot(
            heads_ref[ours, cut:], out_weights[1, cut:, cols], preferred_element_type=f32)

    mine = stat_rows(0)

    def write_log(m_odd, m_even):
        for g in range(groups):
            log_ref[2 * g:2 * g + 1] = jnp.log(jnp.maximum(m_even[g:g + 1], mass_floor))
            log_ref[2 * g + 1:2 * g + 2] = jnp.log(jnp.maximum(m_odd[g:g + 1], mass_floor))

    @pl.when(me < 2)
    def _():
        write_log(mine[0:4], mine[8:12])

    @pl.when(me == 2)
    def _():
        stat_copy(1, 2).wait_recv()
        far = stat_in[0]
        write_log(mine[0:4] + jnp.exp2(-mine[4:8]) * far[0:4], mine[8:12] + jnp.exp2(-mine[12:16]) * far[8:12])

    @pl.when(me == 3)
    def _():
        for src in (1, 2):
            send(stat_out.at[1], stat_in.at[src - 1], stat_send.at[1], stat_recv.at[src - 1], {"sp": src}).wait_recv()
        far = stat_in[0] + stat_in[1]
        write_log(mine[0:4] + jnp.exp2(-mine[4:8]) * far[0:4], mine[8:12] + jnp.exp2(-mine[12:16]) * far[8:12])

    for c in range(0, model, tile):
        cols = slice(c, c + tile)
        leaves[c // tile].wait()
        out_ref[:, cols] = (conv_share[ours, cols] + arrived_ref[:, cols].astype(f32)).astype(bf16)

    @pl.when(me < n - 1)
    def _():
        halo_copy.wait_send()

    @pl.when(me == 0)
    def _():
        offs_copy(0, 1).wait_send()
        offs_copy(0, 2).wait_send()
        for t in range(2):
            for g in range(groups):
                kv_copy(0, t, g).wait_send()
            kv_last(t, 0).wait_send()

    @pl.when(me == 1)
    def _():
        offs_copy(1, 2).wait_send()
        for t in range(2):
            kv_last(t, 1).wait_send()
        for i in (1, 0):
            for g in dev1_groups:
                o_copy(1, i + 2, g).wait_send()
            stat_copy(1, i + 2).wait_send()

    @pl.when(me == 2)
    def _():
        offs_copy(2, 3).wait_send()
        for g in dev1_groups:
            q_copy(2, 1, g).wait_send()
            for t in range(2):
                kv_copy(2, t, g).wait_send()
        o_copy(2, 3, far_g).wait_send()
        stat_copy(2, 3).wait_send()

    @pl.when(me == 3)
    def _():
        for g in dev1_groups:
            q_copy(3, 1, g).wait_send()
        q_copy(3, 2, far_g).wait_send()


def place(mixed, mass_log, out_ref, log_ref, sem):
    copies = [
        pltpu.make_async_copy(mixed, out_ref, sem.at[0]),
        pltpu.make_async_copy(mass_log, log_ref, sem.at[1]),
    ]
    for copy in copies:
        copy.start()
    for copy in copies:
        copy.wait()


def local(n, tp,
    stream, norm_gain, query_weight, key_weight, value_weight, filter_input, filter_gate,
    score_offset, head_gain, filter_taps, channel_gain, channel_shift, attend_out, filter_out,
):
    f32, bf16 = jnp.float32, jnp.bfloat16
    rows = stream.shape[1]
    heads = score_offset.shape[2]
    groups = heads * HEAD_DIM // LANES
    chans = filter_input.shape[1]
    slabs = chans // LANES
    taps = filter_taps.shape[0]
    model = stream.shape[2]
    share = rows // tp
    tiles = model // min(1024, model)

    vmem = pl.BlockSpec(memory_space=pltpu.VMEM)
    hbm = pl.BlockSpec(memory_space=pltpu.HBM)
    dma = pltpu.SemaphoreType.DMA
    mixed, mass_log = pl.pallas_call(
        functools.partial(kernel, n, tp, taps, chans * tp),
        out_shape=(pltpu.VMEM((share, model), bf16), pltpu.VMEM((heads, rows), f32)),
        in_specs=[hbm] * 14,
        out_specs=(vmem,) * 2,
        scratch_shapes=[
            pltpu.VMEM((model,), bf16),
            pltpu.VMEM((heads, rows), bf16),
            pltpu.VMEM((taps, chans), bf16),
            pltpu.VMEM((chans,), bf16),
            pltpu.VMEM((chans,), bf16),
            pltpu.VMEM((chans,), bf16),
            pltpu.VMEM((rows, model), bf16),
            pltpu.VMEM((rows, model), bf16),
            pltpu.VMEM((5, model, chans), bf16),
            pltpu.VMEM((2, chans, model), bf16),
            pltpu.VMEM((3, groups, rows, LANES), bf16),
            pltpu.VMEM((2, groups, rows, LANES), bf16),
            pltpu.VMEM((2, groups, rows, LANES), bf16),
            pltpu.VMEM((3, heads, rows), bf16),
            pltpu.VMEM((2, groups, rows, LANES), bf16),
            pltpu.VMEM((2, groups, rows, LANES), bf16),
            pltpu.VMEM((2, 16, rows), f32),
            pltpu.VMEM((2, 16, rows), f32),
            pltpu.VMEM((groups, 2, rows, LANES), f32),
            pltpu.VMEM((groups, 2, rows, LANES), f32),
            pltpu.VMEM((2, 2, rows, LANES), f32),
            pltpu.VMEM((2, 2, rows, LANES), f32),
            pltpu.VMEM((3, rows, LANES), f32),
            pltpu.VMEM((3, heads, rows), f32),
            pltpu.VMEM((slabs, taps + -taps % 8, LANES), f32),
            pltpu.VMEM((rows, heads * HEAD_DIM), bf16),
            pltpu.VMEM((rows, chans), bf16),
            pltpu.VMEM((rows, model), f32),
            pltpu.VMEM((share, model), bf16),
            pltpu.VMEM((share, model), bf16),
            pltpu.VMEM((HALO, chans), bf16),
            pltpu.VMEM((HALO, chans), bf16),
            pltpu.VMEM((slabs, HALO + rows, LANES), f32),
            pltpu.VMEM((slabs, rows, LANES), f32),
            pltpu.VMEM((rows, LANES), f32),
            pltpu.VMEM((rows, LANES), f32),
            dma((6,)), dma((rows // min(64, rows),)), dma((5, chans // (2 * LANES))), dma((2,)), dma((2, groups)), dma((2, groups)), dma((2, groups)), dma((2, groups)), dma((2,)), dma((2, 2)), dma((3,)), dma((3,)),
            dma((2, groups)), dma((2, groups)), dma((2,)), dma((2,)), dma((tiles,)), dma((tiles,)), dma, dma, dma, dma,
            pltpu.SemaphoreType.REGULAR,
        ],
        compiler_params=pltpu.CompilerParams(
            collective_id=0, has_side_effects=True, vmem_limit_bytes=56 * 1024 * 1024),
    )(stream[0], norm_gain, score_offset[0].T, filter_taps, head_gain, channel_gain, channel_shift,
      query_weight, key_weight, value_weight, filter_input, filter_gate, attend_out, filter_out)
    mixed, mass_log = pl.pallas_call(
        place,
        out_shape=(
            jax.ShapeDtypeStruct((share, model), bf16),
            jax.ShapeDtypeStruct((heads, rows), f32),
        ),
        in_specs=[vmem] * 2,
        out_specs=(hbm,) * 2,
        scratch_shapes=[dma((2,))],
    )(*[pltpu.with_memory_space_constraint(a, pltpu.VMEM) for a in (mixed, mass_log)])
    return (mixed[None], mass_log.T[None])


def shifted(value, axis, steps):
    count = lax.axis_size(axis)
    first, last = (max(0, -steps), min(count, count - steps))
    return lax.ppermute(value, axis, [(source, source + steps) for source in range(first, last)])


def local_ring(
    stream,
    norm_gain,
    query_weight,
    key_weight,
    value_weight,
    filter_input,
    filter_gate,
    score_offset,
    head_gain,
    filter_taps,
    channel_gain,
    channel_shift,
    attend_out,
    filter_out,
):
    rows_here = stream.shape[1]
    total_channels = filter_input.shape[1] * lax.axis_size("tp")
    xfloat = stream[0].astype(jnp.float32)
    normed = xfloat * lax.rsqrt(jnp.mean(xfloat * xfloat, axis=-1, keepdims=True) + rms_eps)
    normed = (normed * norm_gain.astype(jnp.float32)).astype(jnp.bfloat16)

    def project(weight):
        return jnp.dot(normed, weight, preferred_element_type=jnp.float32).astype(jnp.bfloat16)

    queries = project(query_weight)
    keys_here = project(key_weight)
    values_here = project(value_weight)
    conv_in = project(filter_input)
    conv_gate = project(filter_gate)
    offsets_here = score_offset[0]
    heads_here = offsets_here.shape[1]
    first_pos = lax.axis_index("sp") * rows_here
    position = first_pos + jnp.arange(rows_here, dtype=jnp.int32)
    qheads = queries.reshape(rows_here, heads_here, HEAD_DIM)

    def absorb(state_now, kblock, vblock, oblock, first_key):
        attended, weight_mass, survive = state_now
        span = kblock.shape[0]
        kblock = kblock.reshape(span, heads_here, HEAD_DIM)
        vblock = vblock.reshape(span, heads_here, HEAD_DIM)
        scores = jnp.einsum(
            "thd,shd->hts", qheads, kblock, preferred_element_type=jnp.float32
        ) * HEAD_DIM ** (-0.5)
        scores = scores + oblock.astype(jnp.float32).T[:, None, :]
        key_pos = first_key + jnp.arange(span, dtype=jnp.int32)
        strict = ((key_pos[None, :] < position[:, None]) & (key_pos[None, :] >= 0))[None]
        losing = jnp.where(strict, jax.nn.log_sigmoid(-scores), 0.0)
        beyond = lax.cumsum(losing, axis=2, reverse=True) - losing + survive[:, :, None]
        weights = jnp.where(strict, jnp.exp(jax.nn.log_sigmoid(scores) + beyond), 0.0)
        weight_mass = weight_mass + jnp.sum(weights, axis=2)
        attended = attended + jnp.einsum(
            "hts,shd->thd", weights.astype(jnp.bfloat16), vblock, preferred_element_type=jnp.float32
        )
        survive = survive + jnp.sum(losing, axis=2)
        return (attended, weight_mass, survive)

    initial = (
        jnp.zeros((rows_here, heads_here, HEAD_DIM), jnp.float32),
        jnp.zeros((heads_here, rows_here), jnp.float32),
        jnp.zeros((heads_here, rows_here), jnp.float32),
    )
    state_now = absorb(initial, keys_here, values_here, offsets_here, first_pos)

    def pass_turn(turn_index, carried):
        state_now, travelling = carried
        travelling = shifted((travelling[0], travelling[1], travelling[2]), "sp", 1)
        first_key = first_pos - (turn_index + 1) * rows_here
        state_now = absorb(state_now, travelling[0], travelling[1], travelling[2], first_key)
        return (state_now, travelling)

    state_now, travelling = lax.fori_loop(
        0, lax.axis_size("sp") - 1, pass_turn, (state_now, (keys_here, values_here, offsets_here))
    )
    attended, weight_mass, survive = state_now
    head_scale = lax.rsqrt(jnp.mean(attended * attended, axis=-1, keepdims=True) + rms_eps)
    heads_flat = attended * head_scale * head_gain.astype(jnp.float32).reshape(heads_here, HEAD_DIM)
    heads_flat = heads_flat.astype(jnp.bfloat16).reshape(rows_here, heads_here * HEAD_DIM)
    mass_log = jnp.log(jnp.maximum(weight_mass.T, mass_floor))
    gated_rows = (
        conv_in.astype(jnp.float32) * jax.nn.sigmoid(conv_gate.astype(jnp.float32))
    ).astype(jnp.bfloat16)
    reach_back = filter_taps.shape[0] - 1
    earlier = shifted(gated_rows[rows_here - reach_back :], "sp", 1)
    extended = jnp.concatenate([earlier, gated_rows], axis=0).astype(jnp.float32)
    tap_values = filter_taps.astype(jnp.float32)
    filtered = jnp.zeros((rows_here, gated_rows.shape[1]), jnp.float32)
    for tap_index in range(reach_back + 1):
        filtered = filtered + extended[tap_index : tap_index + rows_here] * tap_values[tap_index]
    center = lax.psum(jnp.sum(filtered, axis=-1), "tp") / total_channels
    deviation = filtered - center[:, None]
    spread = lax.psum(jnp.sum(deviation * deviation, axis=-1), "tp") / total_channels
    conv_out = jax.nn.silu(
        deviation * lax.rsqrt(spread[:, None] + norm_eps) * channel_gain.astype(jnp.float32)
        + channel_shift.astype(jnp.float32)
    ).astype(jnp.bfloat16)
    mixed_out = lax.psum_scatter(
        (
            jnp.dot(heads_flat, attend_out, preferred_element_type=jnp.float32)
            + jnp.dot(conv_out, filter_out, preferred_element_type=jnp.float32)
        ).astype(jnp.bfloat16),
        "tp",
        scatter_dimension=0,
        tiled=True,
    )
    return (mixed_out[None], mass_log[None])


def solution(mesh):
    n, tp = mesh.shape["sp"], mesh.shape["tp"]

    def choose(*args):
        rows, heads, chans = args[0].shape[1], args[7].shape[2], args[5].shape[1]
        same = args[2].shape[1] == chans and heads * HEAD_DIM == 4 * LANES == chans
        if n == 4 and tp == 2 and same and rows % 128 == 0:
            return local(n, tp, *args)
        return local_ring(*args)

    return jax.shard_map(
        choose,
        mesh=mesh,
        in_specs=(
            P("fs", "sp", None), P(), P(None, "tp"), P(None, "tp"), P(None, "tp"),
            P(None, "tp"), P(None, "tp"), P("fs", "sp", "tp"), P("tp"), P(None, "tp"),
            P("tp"), P("tp"), P("tp", None), P("tp", None),
        ),
        out_specs=(P("fs", ("sp", "tp"), None), P("fs", "sp", "tp")),
        check_vma=False,
    )
```

```python
import functools

import jax
import jax.numpy as jnp
from jax import lax
from jax.experimental import pallas as pl
from jax.experimental.pallas import tpu as pltpu
from jax.sharding import PartitionSpec as P

HEAD_DIM = 64

rms_eps = 1e-06
norm_eps = 1e-05
mass_floor = 0.01
HALO = 32
LANES = 128
LOG2E = 1.4426950408889634
MESH = pl.DeviceIdType.MESH


def kernel(
    n, tp, taps, total_channels,
    stream_hbm, ngain_hbm, offs_hbm, taps_hbm, gain_hbm, cgain_hbm, cshift_hbm,
    q_hbm, k_hbm, v_hbm, in_hbm, gate_hbm, attend_hbm, filter_hbm,
    out_ref, log_ref,
    ngain, offs, raw_taps, gain_ref, cgain_ref, cshift_ref,
    stream, normed, weights, out_weights, packet, q_in, kv_in, offs_in, o_out, o_in, stat_out, stat_in,
    own_r, own_t, far_r, far_t, masses, off_rows, tap_ref, heads_ref, conv_ref, conv_share, leaving, arrived_ref, heads_last, partner_heads, partner_weights,
    gated, halo, ext, filt, stats, stats_got,
    small_sem, stream_sem, weight_sem, out_weight_sem, q_send, q_recv, kv_send, kv_recv, kv_last_send, kv_last_recv, offs_send, offs_recv,
    o_send, o_recv, stat_send, stat_recv, out_send, out_recv, halo_send, halo_recv, chan_send, chan_recv, entered, swap_send, swap_recv,
):
    f32, bf16 = jnp.float32, jnp.bfloat16
    me = lax.axis_index("sp")
    core = lax.axis_index("tp")
    partner = 1 - core
    rows, model = normed.shape
    chans = in_hbm.shape[1]
    groups = packet.shape[1]
    slabs = chans // LANES
    lane = lax.broadcasted_iota(jnp.int32, (rows, LANES), 1)
    low = lane < HEAD_DIM

    def local_copy(src, dst, sem):
        return pltpu.make_async_copy(src, dst, sem)

    def send(src, dst, send_sem, recv_sem, to):
        return pltpu.make_async_remote_copy(
            src_ref=src, dst_ref=dst, send_sem=send_sem, recv_sem=recv_sem,
            device_id=to, device_id_type=MESH)

    projections = (q_hbm, k_hbm, v_hbm)
    first_order, other_order = (1, 2, 0), (0, 1, 2)

    def slot_of(t):
        return jnp.where(me == 0, first_order[t], other_order[t])

    wide = 2 * LANES
    halves = chans // wide

    def weight_copy(w, slot, half):
        cols = pl.ds(half * wide, wide)
        return local_copy(w.at[:, cols], weights.at[slot, :, cols], weight_sem.at[slot, half])

    def fetch(t, half):
        for order, here in ((first_order, me == 0), (other_order, me != 0)):
            @pl.when(here)
            def _(s=order[t]):
                weight_copy(projections[s], s, half).start()

    band = min(64, rows)

    def stream_copy(c):
        some = pl.ds(pl.multiple_of(c * band, band), band)
        return local_copy(stream_hbm.at[some], stream.at[some], stream_sem.at[c])

    small = [local_copy(a, b, small_sem.at[t]) for t, (a, b) in enumerate((
        (ngain_hbm, ngain), (offs_hbm, offs), (taps_hbm, raw_taps), (gain_hbm, gain_ref),
        (cgain_hbm, cgain_ref), (cshift_hbm, cshift_ref)))]
    gate_copies = [weight_copy(w, 3 + t, half) for half in range(halves) for t, w in enumerate((in_hbm, gate_hbm))]
    filter_copy = local_copy(filter_hbm, out_weights.at[0], out_weight_sem.at[0])
    final = groups - 1
    cut = final * LANES

    def attend_copies(first):
        early = local_copy(attend_hbm.at[pl.ds(LANES if first else 0, cut)], out_weights.at[1, pl.ds(0, cut)], out_weight_sem.at[1])
        late = local_copy(attend_hbm.at[pl.ds(0 if first else cut, LANES)], out_weights.at[1, pl.ds(cut, LANES)], out_weight_sem.at[2])
        return early, late
    for c in range(rows // band):
        stream_copy(c).start()
    small[0].start()
    for t in range(2):
        fetch(t, 0)
    for copy in small[1:]:
        copy.start()

    barrier = pltpu.get_barrier_semaphore()
    peers = {0: (1,), 1: (0, 2, 3), 2: (1, 3), 3: (1, 2)}
    pl.semaphore_signal(barrier, inc=1, device_id={"tp": partner}, device_id_type=MESH)
    for d in range(n):
        @pl.when(me == d)
        def _(d=d):
            for p in peers[d]:
                pl.semaphore_signal(barrier, inc=1, device_id={"sp": p}, device_id_type=MESH)

    small[0].wait()
    norm_gain = ngain[...].astype(f32).reshape(1, -1)

    @pl.loop(0, rows // band)
    def _(c):
        stream_copy(c).wait()

        @pl.when(c == 0)
        def _():
            for half in range(1, halves):
                for t in range(2):
                    fetch(t, half)
            for copy in gate_copies:
                copy.start()

        some = pl.ds(pl.multiple_of(c * band, band), band)
        x = stream[some, :].astype(f32)
        x = x * lax.rsqrt(jnp.mean(x * x, axis=-1, keepdims=True) + rms_eps)
        normed[some, :] = (x * norm_gain).astype(bf16)

    for half in range(halves):
        fetch(2, half)
    for copy in small[1:]:
        copy.wait()

    def q_copy(src_dev, dst_dev, g):
        return send(packet.at[0, g], q_in.at[src_dev - 2, g], q_send.at[dst_dev - 1, g],
                    q_recv.at[src_dev - 2, g], {"sp": dst_dev})

    far_g = 0
    dev1_groups = range(1, groups)

    def kv_copy(src_dev, t, g):
        return send(packet.at[1 + t, g], kv_in.at[t, g], kv_send.at[t, g], kv_recv.at[t, g], {"sp": src_dev + 1})

    def kv_last(t, src_dev):
        return send(packet.at[1 + t, far_g], kv_in.at[t, src_dev],
                    kv_last_send.at[t], kv_last_recv.at[t, src_dev], {"sp": 2})

    def offs_copy(src_dev, dst_dev):
        return send(offs, offs_in.at[src_dev], offs_send.at[dst_dev - 1], offs_recv.at[src_dev], {"sp": dst_dev})

    def o_copy(src_dev, dst_dev, g):
        return send(o_out.at[dst_dev - 2, g], o_in.at[src_dev - 1, g], o_send.at[dst_dev - 2, g],
                    o_recv.at[src_dev - 1, g], {"sp": dst_dev})

    def stat_copy(src_dev, dst_dev):
        return send(stat_out.at[dst_dev - 2], stat_in.at[src_dev - 1], stat_send.at[dst_dev - 2],
                    stat_recv.at[src_dev - 1], {"sp": dst_dev})

    def keep(slot, half, y):
        factor = jnp.where(slot == 0, LOG2E * HEAD_DIM ** (-0.5), 1.0).astype(f32)
        y = (y * factor).astype(bf16)
        for u in range(2):
            packet[slot, 2 * half + u] = y[:, u * LANES:(u + 1) * LANES]

    def project(jobs):
        for t, half in jobs:
            slot = slot_of(t)
            weight_copy(q_hbm, slot, half).wait()
        for t, half in jobs:
            slot = slot_of(t)
            keep(slot, half, jnp.dot(
                normed[...], weights[slot, :, half * wide:(half + 1) * wide], preferred_element_type=f32))

    for half in range(halves):
        project([(0, half), (1, half)])

        if half == 0:
            for d in range(n):
                @pl.when(me == d)
                def _(d=d):
                    pl.semaphore_wait(barrier, len(peers[d]) + tp - 1)

        groups_here = (2 * half, 2 * half + 1)

        @pl.when(me == 0)
        def _():
            if half == 0:
                offs_copy(0, 1).start()
                for t in range(2):
                    kv_copy(0, t, 1).start()

        @pl.when(me == 1)
        def _():
            if half == 0:
                pl.semaphore_signal(entered, inc=1, device_id={"sp": 0}, device_id_type=MESH)
                offs_copy(1, 2).start()

        @pl.when(me == 2)
        def _():
            if half == 0:
                offs_copy(2, 3).start()
            if half == 0:
                q_copy(2, 1, 1).start()
            for g in groups_here:
                if g in dev1_groups:
                    kv_copy(2, 0, g).start()

        @pl.when(me == 3)
        def _():
            if half == 0:
                q_copy(3, 1, 1).start()
            else:
                q_copy(3, 2, far_g).start()

    filter_copy.start()
    for first, here in ((True, me == 1), (False, me != 1)):
        @pl.when(here)
        def _(first=first):
            for copy in attend_copies(first):
                copy.start()
    tap_ref[...] = jnp.zeros_like(tap_ref)
    for c in range(slabs):
        tap_ref[c, :taps] = raw_taps[:, c * LANES:(c + 1) * LANES].astype(f32)
    off_rows[0] = offs[...].astype(f32) * LOG2E
    masses[...] = jnp.zeros_like(masses)
    for copy in gate_copies:
        copy.wait()

    @pl.loop(0, halves)
    def _(c):
        cols = pl.ds(pl.multiple_of(c * wide, wide), wide)
        x = normed[...]
        value = jnp.dot(x, weights[3, :, cols], preferred_element_type=f32).astype(bf16).astype(f32)
        gate = jnp.dot(x, weights[4, :, cols], preferred_element_type=f32).astype(bf16).astype(f32)
        g = (value * jax.nn.sigmoid(gate)).astype(bf16)
        gated[:, cols] = g[rows - HALO:]
        g = g.astype(f32)
        for u in range(2):
            ext[2 * c + u, HALO:, :] = g[:, u * LANES:(u + 1) * LANES]

    halo_copy = send(gated, halo, halo_send, halo_recv, {"sp": lax.rem(me + 1, n)})

    @pl.when(me == 0)
    def _():
        pl.semaphore_wait(entered, 1)
        offs_copy(0, 2).start()
        for t in range(2):
            kv_last(t, 0).start()
        for g in dev1_groups[1:]:
            for t in range(2):
                kv_copy(0, t, g).start()

    for d in (2, 3):
        @pl.when(me == d)
        def _(d=d):
            q_copy(d, 1, 2).start()

    @pl.when(me < n - 1)
    def _():
        halo_copy.start()

    @pl.when(me == 0)
    def _():
        for t in range(2):
            kv_copy(0, t, far_g).start()

    project([(2, half) for half in range(halves)])

    @pl.when(me == 1)
    def _():
        for t in range(2):
            kv_last(t, 1).start()

    @pl.when(me == 2)
    def _():
        for g in dev1_groups:
            kv_copy(2, 1, g).start()

    step = min(128, rows)

    def convolve(starts):
        @pl.loop(0, slabs)
        def _(c):
            for r0 in starts:
                acc = jnp.zeros((step, LANES), f32)
                for k in range(taps):
                    start = HALO - (taps - 1) + k + r0
                    acc = acc + ext[c, start:start + step, :] * tap_ref[c, k:k + 1, :]
                filt[c, r0:r0 + step, :] = acc

    chan_copy = send(stats, stats_got, chan_send, chan_recv, {"tp": partner})

    def convolve_first():
        @pl.when(me > 0)
        def _():
            halo_copy.wait_recv()
            for c in range(slabs):
                ext[c, :HALO, :] = halo[:, c * LANES:(c + 1) * LANES].astype(f32)

        @pl.when(me == 0)
        def _():
            for c in range(slabs):
                ext[c, :HALO, :] = jnp.zeros((HALO, LANES), f32)

        convolve([0])
        total = filt[0]
        for c in range(1, slabs):
            total = total + filt[c]
        lsum = jnp.sum(total, axis=1, keepdims=True)
        mean = lsum * (1.0 / chans)
        square = jnp.zeros((rows, LANES), f32)
        for c in range(slabs):
            dev = filt[c] - mean
            square = square + dev * dev
        lsq = jnp.sum(square, axis=1, keepdims=True)
        stats[...] = jnp.where(low, lsum, lsq)
        chan_copy.start()

    def channel_norm():
        chan_copy.wait()
        mine, other = stats[...], stats_got[...]
        mean = (mine[:, 0:1] + other[:, 0:1]) * (1.0 / total_channels)
        spread = jnp.zeros((rows, 1), f32)
        for s in (mine, other):
            apart = s[:, 0:1] * (1.0 / chans) - mean
            spread = spread + s[:, HEAD_DIM:HEAD_DIM + 1] + chans * apart * apart
        scale = lax.rsqrt(spread * (1.0 / total_channels) + norm_eps)
        for c in range(slabs):
            cols = slice(c * LANES, (c + 1) * LANES)
            y = (filt[c] - mean) * scale * cgain_ref[cols].astype(f32).reshape(1, -1) + cshift_ref[cols].astype(f32).reshape(1, -1)
            conv_ref[:, cols] = (y * jax.nn.sigmoid(y)).astype(bf16)

    tile = min(1024, model)

    def conv_product():
        filter_copy.wait()
        for c in range(0, model, tile):
            conv_share[:, c:c + tile] = jnp.dot(
                conv_ref[...], out_weights[0, :, c:c + tile], preferred_element_type=f32)

    ri = lax.broadcasted_iota(jnp.int32, (rows, rows), 0)
    ci = lax.broadcasted_iota(jnp.int32, (rows, rows), 1)
    tri = (ri >= ci).astype(bf16)

    def split_keys(k):
        zero = jnp.zeros_like(k)
        return jnp.where(low, k, zero), jnp.where(low, zero, k)

    def split_values(v):
        one = jnp.ones_like(v)
        return jnp.where(low, v, one), jnp.where(low, one, v)

    strict = ci < ri

    def attend(blocks_q, k, v, off, own_first):
        q = jnp.concatenate(blocks_q, axis=0)
        z = lax.dot_general(q, k, (((1,), (1,)), ((), ())), preferred_element_type=f32) + off
        lose = jnp.maximum(z, jnp.log(1.0 + jnp.exp2(jnp.minimum(z, 100.0))) * LOG2E)

        def masked(x):
            if not own_first:
                return x
            head = jnp.where(strict, x[:rows], 0.0)
            return jnp.concatenate([head, x[rows:]], axis=0) if len(blocks_q) > 1 else head

        cum = jnp.dot(masked(lose).astype(bf16), tri, preferred_element_type=f32)
        w = masked(jnp.exp2(z - cum))
        res = jnp.dot(w.astype(bf16), v, preferred_element_type=f32)
        pieces = []
        for r in range(len(blocks_q)):
            some = slice(r * rows, (r + 1) * rows)
            pieces.append((res[some], jnp.broadcast_to(cum[some, 0:1], (rows, LANES))))
        return pieces

    def note(which, g, h, res, total):
        base = 0 if h else HEAD_DIM
        masses[which] = jnp.where(lane == base + g, res, jnp.where(lane == base + 4 + g, total, masses[which]))

    def pair(a, b):
        return jnp.where(low, a, b)

    def near_blocks(g, others):
        keys = split_keys(packet[1, g])
        values = split_values(packet[2, g])
        rest = []
        for h in range(2):
            first, *more = attend([packet[0, g]] + others, keys[h], values[h], off_rows[0, pl.ds(2 * g + h, 1), :], True)
            res, total = first
            own_r[g, h] = res
            own_t[g, h] = jnp.exp2(-total)
            note(0, g, h, res, total)
            rest.append(more)
        return rest

    convolve(range(step, rows, step))

    def q_from(src_dev, dst_dev, g):
        return send(packet.at[0, g], q_in.at[src_dev - 2, g], q_send.at[dst_dev - 1, g],
                    q_recv.at[src_dev - 2, g], {"sp": src_dev})

    def kv_from(src_dev, g):
        for t in range(2):
            send(packet.at[1 + t, g], kv_in.at[t, g], kv_send.at[t, g], kv_recv.at[t, g], {"sp": src_dev}).wait_recv()
        return split_keys(kv_in[0, g]), split_values(kv_in[1, g])

    def offs_from(src_dev, dst_dev, row):
        send(offs, offs_in.at[src_dev], offs_send.at[dst_dev - 1], offs_recv.at[src_dev], {"sp": src_dev}).wait_recv()
        off_rows[row] = offs_in[src_dev].astype(f32) * LOG2E

    def off_of(row, g, h):
        return off_rows[row, pl.ds(2 * g + h, 1), :]

    def stat_rows(which):
        t = jnp.transpose(masses[which])
        return jnp.concatenate([t[0:8], t[HEAD_DIM:HEAD_DIM + 8]], axis=0)

    blocks = (lax.broadcasted_iota(jnp.int32, (LANES, LANES), 0) // HEAD_DIM
              == lax.broadcasted_iota(jnp.int32, (LANES, LANES), 1) // HEAD_DIM).astype(bf16)

    def close(place_at, g, o):
        sq = jnp.dot((o * o).astype(bf16), blocks, preferred_element_type=f32)
        gain = gain_ref[g * LANES:(g + 1) * LANES].astype(f32).reshape(1, LANES)
        cols = slice(place_at * LANES, (place_at + 1) * LANES)
        heads_ref[:, cols] = (o * lax.rsqrt(sq * (1.0 / HEAD_DIM) + rms_eps) * gain).astype(bf16)

    @pl.when((me == 0) | (me == 3))
    def _():
        @pl.loop(0, groups // 2)
        def _(half):
            for u in range(2):
                near_blocks(2 * half + u, [])

            @pl.when((me == 3) & (half == 0))
            def _():
                q_copy(3, 1, 3).start()

    @pl.when(me == 1)
    def _():
        near_blocks(far_g, [])
        offs_from(0, 1, 1)

        @pl.loop(1, groups)
        def _(g):
            q_from(2, 1, g).wait_recv()
            q_from(3, 1, g).wait_recv()
            rest = near_blocks(g, [q_in[1, g], q_in[0, g]])
            for h in range(2):
                for i in (1, 0):
                    res, total = rest[h][1 - i]
                    far_r[i, h] = res
                    far_t[i, h] = jnp.exp2(-total)
            keys, values = kv_from(0, g)
            parts = [[], []]
            for h in range(2):
                pieces = attend([q_in[1, g], q_in[0, g], packet[0, g]], keys[h], values[h], off_of(1, g, h), False)
                for i in (1, 0):
                    res = far_r[i, h] + far_t[i, h] * pieces[1 - i][0]
                    note(1 + i, g, h, res, res)
                    parts[i].append(res)
                res = own_r[g, h] + own_t[g, h] * pieces[2][0]
                own_r[g, h] = res
                note(0, g, h, res, res)
            for i in (1, 0):
                o_out[i, g] = pair(*parts[i]).astype(bf16)
            for i in (1, 0):
                send(o_out.at[i, g], o_in.at[0, g], o_send.at[i, g], o_recv.at[0, g], {"sp": i + 2}).start()

        for i in (1, 0):
            stat_out[i] = stat_rows(1 + i)
            stat_copy(1, i + 2).start()

    @pl.when(me == 2)
    def _():
        near_blocks(1, [])
        q_copy(2, 1, 3).start()

        @pl.loop(1, 2)
        def _(half):
            for u in range(2):
                near_blocks(2 * half + u, [])

    convolve_first()

    @pl.when(me == 2)
    def _():
        q_from(3, 2, far_g).wait_recv()
        rest = near_blocks(far_g, [q_in[1, far_g]])
        for h in range(2):
            res, total = rest[h][0]
            far_r[1, h] = res
            far_t[1, h] = jnp.exp2(-total)
        offs_from(1, 2, 2)
        offs_from(0, 2, 1)
        for src in (1, 0):
            for t in range(2):
                send(packet.at[1 + t, far_g], kv_in.at[t, src], kv_last_send.at[t],
                     kv_last_recv.at[t, src], {"sp": src}).wait_recv()
            keys = split_keys(kv_in[0, src])
            values = split_values(kv_in[1, src])
            parts = []
            for h in range(2):
                (own, own_total), (far, far_total) = attend(
                    [packet[0, far_g], q_in[1, far_g]], keys[h], values[h], off_rows[1 + src, 2 * far_g + h:2 * far_g + h + 1, :], False)
                own = own_r[far_g, h] + own_t[far_g, h] * own
                far = far_r[1, h] + far_t[1, h] * far
                own_r[far_g, h] = own
                if src:
                    far_r[1, h] = far
                    own_t[far_g, h] = own_t[far_g, h] * jnp.exp2(-own_total)
                    far_t[1, h] = far_t[1, h] * jnp.exp2(-far_total)
                else:
                    note(0, far_g, h, own, own)
                    note(2, far_g, h, far, far)
                    parts.append(far)
        o_out[1, far_g] = pair(*parts).astype(bf16)
        o_out[1, far_g] = pair(*parts).astype(bf16)
        o_copy(2, 3, far_g).start()
        stat_out[1] = stat_rows(2)
        stat_copy(2, 3).start()

    @pl.when(me == 1)
    def _():
        for g in dev1_groups:
            close(g - 1, g, pair(own_r[g, 0], own_r[g, 1]))

    channel_norm()
    conv_product()

    @pl.when(me == 3)
    def _():
        offs_from(2, 3, 1)
        for g in dev1_groups:
            keys, values = kv_from(2, g)
            for h in range(2):
                res, total = attend([packet[0, g]], keys[h], values[h], off_of(1, g, h), False)[0]
                through = own_t[g, h]
                res = own_r[g, h] + through * res
                own_r[g, h] = res
                own_t[g, h] = through * jnp.exp2(-total)
                near = masses[0][:, (HEAD_DIM, 0)[h] + 4 + g:(HEAD_DIM, 0)[h] + 5 + g]
                note(0, g, h, res, total + near)

    def finish(g):
        own = pair(own_r[g, 0], own_r[g, 1])

        @pl.when(me == 0)
        def _():
            close(g, g, own)

        @pl.when(me == 2)
        def _():
            if g == far_g:
                close(g, g, own)
            else:
                through = pair(own_t[g, 0], own_t[g, 1])
                send(o_out.at[0, g], o_in.at[0, g], o_send.at[0, g], o_recv.at[0, g], {"sp": 1}).wait_recv()
                close(g, g, own + through * o_in[0, g].astype(f32))

        @pl.when(me == 3)
        def _():
            through = pair(own_t[g, 0], own_t[g, 1])
            src = 2 if g == far_g else 1
            send(o_out.at[1, g], o_in.at[src - 1, g], o_send.at[1, g], o_recv.at[src - 1, g], {"sp": src}).wait_recv()
            close(g, g, own + through * o_in[src - 1, g].astype(f32))

    for copy in attend_copies(False):
        copy.wait()
    share = rows // tp
    theirs = pl.ds(pl.multiple_of(partner * share, share), share)
    ours = pl.ds(pl.multiple_of(core * share, share), share)
    weight_swap = send(out_weights.at[1, pl.ds(cut, LANES)], partner_weights, swap_send.at[0], swap_recv.at[0], {"tp": partner})
    heads_swap = send(heads_last.at[theirs], partner_heads, swap_send.at[1], swap_recv.at[1], {"tp": partner})
    weight_swap.start()
    for g in range(final):
        finish(g)
    leaves = []
    for c in range(0, model, tile):
        cols = slice(c, c + tile)
        leaving[:, cols] = (conv_share[theirs, cols] + jnp.dot(
            heads_ref[theirs, :cut], out_weights[1, :cut, cols], preferred_element_type=f32)).astype(bf16)
        copy = send(leaving.at[:, pl.ds(c, tile)], arrived_ref.at[:, pl.ds(c, tile)],
                    out_send.at[c // tile], out_recv.at[c // tile], {"tp": partner})
        copy.start()
        leaves.append(copy)
    for c in range(0, model, tile):
        cols = slice(c, c + tile)
        conv_share[ours, cols] += jnp.dot(
            heads_ref[ours, :cut], out_weights[1, :cut, cols], preferred_element_type=f32)
    @pl.when(me == 1)
    def _():
        keys, values = kv_from(0, far_g)
        parts = []
        for h in range(2):
            res, _ = attend([packet[0, far_g]], keys[h], values[h], off_of(1, far_g, h), False)[0]
            res = own_r[far_g, h] + own_t[far_g, h] * res
            note(0, far_g, h, res, res)
            parts.append(res)
        close(final, far_g, pair(*parts))

    finish(final)
    heads_last[...] = heads_ref[:, cut:]
    heads_swap.start()
    for copy in leaves:
        copy.wait()
    weight_swap.wait()
    for c in range(0, model, tile):
        cols = slice(c, c + tile)
        conv_share[ours, cols] += arrived_ref[:, cols].astype(f32) + jnp.dot(
            heads_ref[ours, cut:], out_weights[1, cut:, cols], preferred_element_type=f32)

    mine = stat_rows(0)

    def write_log(m_odd, m_even):
        for g in range(groups):
            log_ref[2 * g:2 * g + 1] = jnp.log(jnp.maximum(m_even[g:g + 1], mass_floor))
            log_ref[2 * g + 1:2 * g + 2] = jnp.log(jnp.maximum(m_odd[g:g + 1], mass_floor))

    @pl.when(me < 2)
    def _():
        write_log(mine[0:4], mine[8:12])

    @pl.when(me == 2)
    def _():
        stat_copy(1, 2).wait_recv()
        far = stat_in[0]
        write_log(mine[0:4] + jnp.exp2(-mine[4:8]) * far[0:4], mine[8:12] + jnp.exp2(-mine[12:16]) * far[8:12])

    @pl.when(me == 3)
    def _():
        for src in (1, 2):
            send(stat_out.at[1], stat_in.at[src - 1], stat_send.at[1], stat_recv.at[src - 1], {"sp": src}).wait_recv()
        far = stat_in[0] + stat_in[1]
        write_log(mine[0:4] + jnp.exp2(-mine[4:8]) * far[0:4], mine[8:12] + jnp.exp2(-mine[12:16]) * far[8:12])

    heads_swap.wait()
    for c in range(0, model, tile):
        cols = slice(c, c + tile)
        out_ref[:, cols] = (conv_share[ours, cols] + jnp.dot(
            partner_heads[...], partner_weights[:, cols], preferred_element_type=f32)).astype(bf16)

    @pl.when(me < n - 1)
    def _():
        halo_copy.wait_send()

    @pl.when(me == 0)
    def _():
        offs_copy(0, 1).wait_send()
        offs_copy(0, 2).wait_send()
        for t in range(2):
            for g in range(groups):
                kv_copy(0, t, g).wait_send()
            kv_last(t, 0).wait_send()

    @pl.when(me == 1)
    def _():
        offs_copy(1, 2).wait_send()
        for t in range(2):
            kv_last(t, 1).wait_send()
        for i in (1, 0):
            for g in dev1_groups:
                o_copy(1, i + 2, g).wait_send()
            stat_copy(1, i + 2).wait_send()

    @pl.when(me == 2)
    def _():
        offs_copy(2, 3).wait_send()
        for g in dev1_groups:
            q_copy(2, 1, g).wait_send()
            for t in range(2):
                kv_copy(2, t, g).wait_send()
        o_copy(2, 3, far_g).wait_send()
        stat_copy(2, 3).wait_send()

    @pl.when(me == 3)
    def _():
        for g in dev1_groups:
            q_copy(3, 1, g).wait_send()
        q_copy(3, 2, far_g).wait_send()


def place(mixed, mass_log, out_ref, log_ref, sem):
    copies = [
        pltpu.make_async_copy(mixed, out_ref, sem.at[0]),
        pltpu.make_async_copy(mass_log, log_ref, sem.at[1]),
    ]
    for copy in copies:
        copy.start()
    for copy in copies:
        copy.wait()


def local(n, tp,
    stream, norm_gain, query_weight, key_weight, value_weight, filter_input, filter_gate,
    score_offset, head_gain, filter_taps, channel_gain, channel_shift, attend_out, filter_out,
):
    f32, bf16 = jnp.float32, jnp.bfloat16
    rows = stream.shape[1]
    heads = score_offset.shape[2]
    groups = heads * HEAD_DIM // LANES
    chans = filter_input.shape[1]
    slabs = chans // LANES
    taps = filter_taps.shape[0]
    model = stream.shape[2]
    share = rows // tp
    tiles = model // min(1024, model)

    vmem = pl.BlockSpec(memory_space=pltpu.VMEM)
    hbm = pl.BlockSpec(memory_space=pltpu.HBM)
    dma = pltpu.SemaphoreType.DMA
    mixed, mass_log = pl.pallas_call(
        functools.partial(kernel, n, tp, taps, chans * tp),
        out_shape=(pltpu.VMEM((share, model), bf16), pltpu.VMEM((heads, rows), f32)),
        in_specs=[hbm] * 14,
        out_specs=(vmem,) * 2,
        scratch_shapes=[
            pltpu.VMEM((model,), bf16),
            pltpu.VMEM((heads, rows), bf16),
            pltpu.VMEM((taps, chans), bf16),
            pltpu.VMEM((chans,), bf16),
            pltpu.VMEM((chans,), bf16),
            pltpu.VMEM((chans,), bf16),
            pltpu.VMEM((rows, model), bf16),
            pltpu.VMEM((rows, model), bf16),
            pltpu.VMEM((5, model, chans), bf16),
            pltpu.VMEM((2, chans, model), bf16),
            pltpu.VMEM((3, groups, rows, LANES), bf16),
            pltpu.VMEM((2, groups, rows, LANES), bf16),
            pltpu.VMEM((2, groups, rows, LANES), bf16),
            pltpu.VMEM((3, heads, rows), bf16),
            pltpu.VMEM((2, groups, rows, LANES), bf16),
            pltpu.VMEM((2, groups, rows, LANES), bf16),
            pltpu.VMEM((2, 16, rows), f32),
            pltpu.VMEM((2, 16, rows), f32),
            pltpu.VMEM((groups, 2, rows, LANES), f32),
            pltpu.VMEM((groups, 2, rows, LANES), f32),
            pltpu.VMEM((2, 2, rows, LANES), f32),
            pltpu.VMEM((2, 2, rows, LANES), f32),
            pltpu.VMEM((3, rows, LANES), f32),
            pltpu.VMEM((3, heads, rows), f32),
            pltpu.VMEM((slabs, taps + -taps % 8, LANES), f32),
            pltpu.VMEM((rows, heads * HEAD_DIM), bf16),
            pltpu.VMEM((rows, chans), bf16),
            pltpu.VMEM((rows, model), f32),
            pltpu.VMEM((share, model), bf16),
            pltpu.VMEM((share, model), bf16),
            pltpu.VMEM((rows, LANES), bf16),
            pltpu.VMEM((share, LANES), bf16),
            pltpu.VMEM((LANES, model), bf16),
            pltpu.VMEM((HALO, chans), bf16),
            pltpu.VMEM((HALO, chans), bf16),
            pltpu.VMEM((slabs, HALO + rows, LANES), f32),
            pltpu.VMEM((slabs, rows, LANES), f32),
            pltpu.VMEM((rows, LANES), f32),
            pltpu.VMEM((rows, LANES), f32),
            dma((6,)), dma((rows // min(64, rows),)), dma((5, chans // (2 * LANES))), dma((3,)), dma((2, groups)), dma((2, groups)), dma((2, groups)), dma((2, groups)), dma((2,)), dma((2, 2)), dma((3,)), dma((3,)),
            dma((2, groups)), dma((2, groups)), dma((2,)), dma((2,)), dma((tiles,)), dma((tiles,)), dma, dma, dma, dma,
            pltpu.SemaphoreType.REGULAR, dma((2,)), dma((2,)),
        ],
        compiler_params=pltpu.CompilerParams(
            collective_id=0, has_side_effects=True, vmem_limit_bytes=56 * 1024 * 1024),
    )(stream[0], norm_gain, score_offset[0].T, filter_taps, head_gain, channel_gain, channel_shift,
      query_weight, key_weight, value_weight, filter_input, filter_gate, attend_out, filter_out)
    mixed, mass_log = pl.pallas_call(
        place,
        out_shape=(
            jax.ShapeDtypeStruct((share, model), bf16),
            jax.ShapeDtypeStruct((heads, rows), f32),
        ),
        in_specs=[vmem] * 2,
        out_specs=(hbm,) * 2,
        scratch_shapes=[dma((2,))],
    )(*[pltpu.with_memory_space_constraint(a, pltpu.VMEM) for a in (mixed, mass_log)])
    return (mixed[None], mass_log.T[None])


def shifted(value, axis, steps):
    count = lax.axis_size(axis)
    first, last = (max(0, -steps), min(count, count - steps))
    return lax.ppermute(value, axis, [(source, source + steps) for source in range(first, last)])


def local_ring(
    stream,
    norm_gain,
    query_weight,
    key_weight,
    value_weight,
    filter_input,
    filter_gate,
    score_offset,
    head_gain,
    filter_taps,
    channel_gain,
    channel_shift,
    attend_out,
    filter_out,
):
    rows_here = stream.shape[1]
    total_channels = filter_input.shape[1] * lax.axis_size("tp")
    xfloat = stream[0].astype(jnp.float32)
    normed = xfloat * lax.rsqrt(jnp.mean(xfloat * xfloat, axis=-1, keepdims=True) + rms_eps)
    normed = (normed * norm_gain.astype(jnp.float32)).astype(jnp.bfloat16)

    def project(weight):
        return jnp.dot(normed, weight, preferred_element_type=jnp.float32).astype(jnp.bfloat16)

    queries = project(query_weight)
    keys_here = project(key_weight)
    values_here = project(value_weight)
    conv_in = project(filter_input)
    conv_gate = project(filter_gate)
    offsets_here = score_offset[0]
    heads_here = offsets_here.shape[1]
    first_pos = lax.axis_index("sp") * rows_here
    position = first_pos + jnp.arange(rows_here, dtype=jnp.int32)
    qheads = queries.reshape(rows_here, heads_here, HEAD_DIM)

    def absorb(state_now, kblock, vblock, oblock, first_key):
        attended, weight_mass, survive = state_now
        span = kblock.shape[0]
        kblock = kblock.reshape(span, heads_here, HEAD_DIM)
        vblock = vblock.reshape(span, heads_here, HEAD_DIM)
        scores = jnp.einsum(
            "thd,shd->hts", qheads, kblock, preferred_element_type=jnp.float32
        ) * HEAD_DIM ** (-0.5)
        scores = scores + oblock.astype(jnp.float32).T[:, None, :]
        key_pos = first_key + jnp.arange(span, dtype=jnp.int32)
        strict = ((key_pos[None, :] < position[:, None]) & (key_pos[None, :] >= 0))[None]
        losing = jnp.where(strict, jax.nn.log_sigmoid(-scores), 0.0)
        beyond = lax.cumsum(losing, axis=2, reverse=True) - losing + survive[:, :, None]
        weights = jnp.where(strict, jnp.exp(jax.nn.log_sigmoid(scores) + beyond), 0.0)
        weight_mass = weight_mass + jnp.sum(weights, axis=2)
        attended = attended + jnp.einsum(
            "hts,shd->thd", weights.astype(jnp.bfloat16), vblock, preferred_element_type=jnp.float32
        )
        survive = survive + jnp.sum(losing, axis=2)
        return (attended, weight_mass, survive)

    initial = (
        jnp.zeros((rows_here, heads_here, HEAD_DIM), jnp.float32),
        jnp.zeros((heads_here, rows_here), jnp.float32),
        jnp.zeros((heads_here, rows_here), jnp.float32),
    )
    state_now = absorb(initial, keys_here, values_here, offsets_here, first_pos)

    def pass_turn(turn_index, carried):
        state_now, travelling = carried
        travelling = shifted((travelling[0], travelling[1], travelling[2]), "sp", 1)
        first_key = first_pos - (turn_index + 1) * rows_here
        state_now = absorb(state_now, travelling[0], travelling[1], travelling[2], first_key)
        return (state_now, travelling)

    state_now, travelling = lax.fori_loop(
        0, lax.axis_size("sp") - 1, pass_turn, (state_now, (keys_here, values_here, offsets_here))
    )
    attended, weight_mass, survive = state_now
    head_scale = lax.rsqrt(jnp.mean(attended * attended, axis=-1, keepdims=True) + rms_eps)
    heads_flat = attended * head_scale * head_gain.astype(jnp.float32).reshape(heads_here, HEAD_DIM)
    heads_flat = heads_flat.astype(jnp.bfloat16).reshape(rows_here, heads_here * HEAD_DIM)
    mass_log = jnp.log(jnp.maximum(weight_mass.T, mass_floor))
    gated_rows = (
        conv_in.astype(jnp.float32) * jax.nn.sigmoid(conv_gate.astype(jnp.float32))
    ).astype(jnp.bfloat16)
    reach_back = filter_taps.shape[0] - 1
    earlier = shifted(gated_rows[rows_here - reach_back :], "sp", 1)
    extended = jnp.concatenate([earlier, gated_rows], axis=0).astype(jnp.float32)
    tap_values = filter_taps.astype(jnp.float32)
    filtered = jnp.zeros((rows_here, gated_rows.shape[1]), jnp.float32)
    for tap_index in range(reach_back + 1):
        filtered = filtered + extended[tap_index : tap_index + rows_here] * tap_values[tap_index]
    center = lax.psum(jnp.sum(filtered, axis=-1), "tp") / total_channels
    deviation = filtered - center[:, None]
    spread = lax.psum(jnp.sum(deviation * deviation, axis=-1), "tp") / total_channels
    conv_out = jax.nn.silu(
        deviation * lax.rsqrt(spread[:, None] + norm_eps) * channel_gain.astype(jnp.float32)
        + channel_shift.astype(jnp.float32)
    ).astype(jnp.bfloat16)
    mixed_out = lax.psum_scatter(
        (
            jnp.dot(heads_flat, attend_out, preferred_element_type=jnp.float32)
            + jnp.dot(conv_out, filter_out, preferred_element_type=jnp.float32)
        ).astype(jnp.bfloat16),
        "tp",
        scatter_dimension=0,
        tiled=True,
    )
    return (mixed_out[None], mass_log[None])


def solution(mesh):
    n, tp = mesh.shape["sp"], mesh.shape["tp"]

    def choose(*args):
        rows, heads, chans = args[0].shape[1], args[7].shape[2], args[5].shape[1]
        same = args[2].shape[1] == chans and heads * HEAD_DIM == 4 * LANES == chans
        if n == 4 and tp == 2 and same and rows % 128 == 0:
            return local(n, tp, *args)
        return local_ring(*args)

    return jax.shard_map(
        choose,
        mesh=mesh,
        in_specs=(
            P("fs", "sp", None), P(), P(None, "tp"), P(None, "tp"), P(None, "tp"),
            P(None, "tp"), P(None, "tp"), P("fs", "sp", "tp"), P("tp"), P(None, "tp"),
            P("tp"), P("tp"), P("tp", None), P("tp", None),
        ),
        out_specs=(P("fs", ("sp", "tp"), None), P("fs", "sp", "tp")),
        check_vma=False,
    )
```

```python
import functools

import jax
import jax.numpy as jnp
from jax import lax
from jax.experimental import pallas as pl
from jax.experimental.pallas import tpu as pltpu
from jax.sharding import PartitionSpec as P

HEAD_DIM = 64

rms_eps = 1e-06
norm_eps = 1e-05
mass_floor = 0.01
HALO = 32
LANES = 128
LOG2E = 1.4426950408889634
MESH = pl.DeviceIdType.MESH


class Slots:
    def __init__(self, pick):
        self.pick = pick

    @property
    def at(self):
        return self

    def __getitem__(self, index):
        return self.pick(*index) if isinstance(index, tuple) else self.pick(index)


def kernel(
    n, tp, taps, total_channels,
    stream_hbm, ngain_hbm, offs_hbm, taps_hbm, gain_hbm, cgain_hbm, cshift_hbm,
    q_hbm, k_hbm, v_hbm, in_hbm, gate_hbm, attend_hbm, filter_hbm,
    out_ref, log_ref,
    ngain, offs, raw_taps, gain_ref, cgain_ref, cshift_ref,
    stream, normed, weights, out_weights, packet, q_in, kv_in, offs_in, o_out, o_in, stat_out, stat_in,
    own_r, own_t, far_r, far_t, masses, off_rows, tap_ref, heads_ref, conv_ref, conv_share, leaving, arrived_ref, heads_last, partner_heads, partner_weights,
    gated, halo, ext, filt, stats, stats_got,
    weight_sem, out_weight_sem, flow_send, flow_recv, offs_sem_send, offs_sem_recv,
    out_send, out_recv, halo_send, halo_recv, chan_send, chan_recv, entered, swap_send, swap_recv,
):
    f32, bf16 = jnp.float32, jnp.bfloat16
    small_sem = Slots(lambda t: (out_weight_sem.at[t] if t < 3 else out_send.at[t - 3] if t < 5 else swap_send.at[0]))
    stream_sem = Slots(lambda c: flow_send.at[0, c])
    kv_send, o_send = flow_send, flow_send
    q_send = Slots(lambda i, g: flow_send.at[2, g])
    kv_last_send = Slots(lambda t: flow_send.at[2, t])
    kv_recv, kv_last_recv = flow_recv, flow_recv
    q_recv = Slots(lambda i, g: flow_recv.at[2 + i, g])
    o_recv = q_recv
    stat_recv = Slots(lambda i: flow_recv.at[3, 1 + i])
    me = lax.axis_index("sp")
    core = lax.axis_index("tp")
    partner = 1 - core
    rows, model = normed.shape
    chans = in_hbm.shape[1]
    groups = packet.shape[1]
    slabs = chans // LANES
    lane = lax.broadcasted_iota(jnp.int32, (rows, LANES), 1)
    low = lane < HEAD_DIM

    def local_copy(src, dst, sem):
        return pltpu.make_async_copy(src, dst, sem)

    def send(src, dst, send_sem, recv_sem, to):
        return pltpu.make_async_remote_copy(
            src_ref=src, dst_ref=dst, send_sem=send_sem, recv_sem=recv_sem,
            device_id=to, device_id_type=MESH)

    projections = (q_hbm, k_hbm, v_hbm)
    first_order, other_order = (1, 2, 0), (0, 1, 2)

    def slot_of(t):
        return jnp.where(me == 0, first_order[t], other_order[t])

    wide = 2 * LANES
    halves = chans // wide

    def weight_copy(w, slot, half):
        cols = pl.ds(half * wide, wide)
        return local_copy(w.at[:, cols], weights.at[slot, :, cols], weight_sem.at[slot, half])

    def fetch(t, half):
        for order, here in ((first_order, me == 0), (other_order, me != 0)):
            @pl.when(here)
            def _(s=order[t]):
                weight_copy(projections[s], s, half).start()

    band = rows // packet.shape[1]

    def stream_copy(c):
        some = pl.ds(pl.multiple_of(c * band, band), band)
        return local_copy(stream_hbm.at[some], stream.at[some], stream_sem.at[c])

    small = [local_copy(a, b, small_sem.at[t]) for t, (a, b) in enumerate((
        (ngain_hbm, ngain), (offs_hbm, offs), (taps_hbm, raw_taps), (gain_hbm, gain_ref),
        (cgain_hbm, cgain_ref), (cshift_hbm, cshift_ref)))]
    gate_copies = [weight_copy(w, 3 + t, half) for half in range(halves) for t, w in enumerate((in_hbm, gate_hbm))]
    filter_copy = local_copy(filter_hbm, out_weights.at[0], out_weight_sem.at[0])
    final = groups - 1
    cut = final * LANES

    def attend_copies(first):
        early = local_copy(attend_hbm.at[pl.ds(LANES if first else 0, cut)], out_weights.at[1, pl.ds(0, cut)], out_weight_sem.at[1])
        late = local_copy(attend_hbm.at[pl.ds(0 if first else cut, LANES)], out_weights.at[1, pl.ds(cut, LANES)], out_weight_sem.at[2])
        return early, late
    for c in range(rows // band):
        stream_copy(c).start()
    small[0].start()
    for t in range(2):
        fetch(t, 0)
    for copy in small[1:]:
        copy.start()

    barrier = pltpu.get_barrier_semaphore()
    peers = {0: (1,), 1: (0, 2, 3), 2: (1, 3), 3: (1, 2)}
    pl.semaphore_signal(barrier, inc=1, device_id={"tp": partner}, device_id_type=MESH)
    for d in range(n):
        @pl.when(me == d)
        def _(d=d):
            for p in peers[d]:
                pl.semaphore_signal(barrier, inc=1, device_id={"sp": p}, device_id_type=MESH)

    small[0].wait()
    norm_gain = ngain[...].astype(f32).reshape(1, -1)

    @pl.loop(0, rows // band)
    def _(c):
        stream_copy(c).wait()

        @pl.when(c == 0)
        def _():
            for half in range(1, halves):
                for t in range(2):
                    fetch(t, half)
            for copy in gate_copies:
                copy.start()

        some = pl.ds(pl.multiple_of(c * band, band), band)
        x = stream[some, :].astype(f32)
        x = x * lax.rsqrt(jnp.mean(x * x, axis=-1, keepdims=True) + rms_eps)
        normed[some, :] = (x * norm_gain).astype(bf16)

    for half in range(halves):
        fetch(2, half)
    for copy in small[1:]:
        copy.wait()

    def q_copy(src_dev, dst_dev, g):
        return send(packet.at[0, g], q_in.at[src_dev - 2, g], q_send.at[dst_dev - 1, g],
                    q_recv.at[src_dev - 2, g], {"sp": dst_dev})

    far_g = 0
    dev1_groups = range(1, groups)

    def kv_copy(src_dev, t, g):
        return send(packet.at[1 + t, g], kv_in.at[t, g], kv_send.at[t, g], kv_recv.at[t, g], {"sp": src_dev + 1})

    def kv_last(t, src_dev):
        return send(packet.at[1 + t, far_g], kv_in.at[t, src_dev],
                    kv_last_send.at[t], kv_last_recv.at[t, src_dev], {"sp": 2})

    def offs_copy(src_dev, dst_dev):
        return send(offs, offs_in.at[src_dev], offs_sem_send.at[int((src_dev, dst_dev) == (0, 2))], offs_sem_recv.at[src_dev % 2],
                    {"sp": dst_dev})

    def o_copy(src_dev, dst_dev, g):
        return send(o_out.at[dst_dev - 2, g], o_in.at[src_dev - 1, g], o_send.at[dst_dev - 2, g],
                    o_recv.at[src_dev - 1, g], {"sp": dst_dev})

    def stat_copy(src_dev, dst_dev):
        return send(stat_out.at[dst_dev - 2], stat_in.at[src_dev - 1],
                    flow_send.at[2, dst_dev] if src_dev == 1 else flow_send.at[0, 0],
                    stat_recv.at[src_dev - 1], {"sp": dst_dev})

    def keep(slot, half, y):
        factor = jnp.where(slot == 0, LOG2E * HEAD_DIM ** (-0.5), 1.0).astype(f32)
        y = (y * factor).astype(bf16)
        for u in range(2):
            packet[slot, 2 * half + u] = y[:, u * LANES:(u + 1) * LANES]

    def project(jobs):
        for t, half in jobs:
            slot = slot_of(t)
            weight_copy(q_hbm, slot, half).wait()
        for t, half in jobs:
            slot = slot_of(t)
            keep(slot, half, jnp.dot(
                normed[...], weights[slot, :, half * wide:(half + 1) * wide], preferred_element_type=f32))

    for half in range(halves):
        project([(0, half), (1, half)])

        if half == 0:
            for d in range(n):
                @pl.when(me == d)
                def _(d=d):
                    pl.semaphore_wait(barrier, len(peers[d]) + tp - 1)

        groups_here = (2 * half, 2 * half + 1)

        @pl.when(me == 0)
        def _():
            if half == 0:
                offs_copy(0, 1).start()
                for t in range(2):
                    kv_copy(0, t, 1).start()

        @pl.when(me == 1)
        def _():
            if half == 0:
                pl.semaphore_signal(entered, inc=1, device_id={"sp": 0}, device_id_type=MESH)
                offs_copy(1, 2).start()

        @pl.when(me == 2)
        def _():
            if half == 0:
                offs_copy(2, 3).start()
            if half == 0:
                q_copy(2, 1, 1).start()
            for g in groups_here:
                if g in dev1_groups:
                    kv_copy(2, 0, g).start()

        @pl.when(me == 3)
        def _():
            if half == 0:
                q_copy(3, 1, 1).start()
            else:
                q_copy(3, 2, far_g).start()

    filter_copy.start()
    for first, here in ((True, me == 1), (False, me != 1)):
        @pl.when(here)
        def _(first=first):
            for copy in attend_copies(first):
                copy.start()
    tap_ref[...] = jnp.zeros_like(tap_ref)
    for c in range(slabs):
        tap_ref[c, :taps] = raw_taps[:, c * LANES:(c + 1) * LANES].astype(f32)
    off_rows[0] = offs[...].astype(f32) * LOG2E
    masses[...] = jnp.zeros_like(masses)
    for copy in gate_copies:
        copy.wait()

    @pl.loop(0, halves)
    def _(c):
        cols = pl.ds(pl.multiple_of(c * wide, wide), wide)
        x = normed[...]
        value = jnp.dot(x, weights[3, :, cols], preferred_element_type=f32).astype(bf16).astype(f32)
        gate = jnp.dot(x, weights[4, :, cols], preferred_element_type=f32).astype(bf16).astype(f32)
        g = (value * jax.nn.sigmoid(gate)).astype(bf16)
        gated[:, cols] = g[rows - HALO:]
        g = g.astype(f32)
        for u in range(2):
            ext[2 * c + u, HALO:, :] = g[:, u * LANES:(u + 1) * LANES]

    halo_copy = send(gated, halo, halo_send, halo_recv, {"sp": lax.rem(me + 1, n)})

    @pl.when(me == 0)
    def _():
        pl.semaphore_wait(entered, 1)
        offs_copy(0, 2).start()
        for t in range(2):
            kv_last(t, 0).start()
        for g in dev1_groups[1:]:
            for t in range(2):
                kv_copy(0, t, g).start()

    for d in (2, 3):
        @pl.when(me == d)
        def _(d=d):
            q_copy(d, 1, 2).start()

    @pl.when(me < n - 1)
    def _():
        halo_copy.start()

    @pl.when(me == 0)
    def _():
        for t in range(2):
            kv_copy(0, t, far_g).start()

    project([(2, half) for half in range(halves)])

    @pl.when(me == 1)
    def _():
        for t in range(2):
            kv_last(t, 1).start()

    @pl.when(me == 2)
    def _():
        for g in dev1_groups:
            kv_copy(2, 1, g).start()

    step = min(128, rows)

    def convolve(starts):
        @pl.loop(0, slabs)
        def _(c):
            for r0 in starts:
                acc = jnp.zeros((step, LANES), f32)
                for k in range(taps):
                    start = HALO - (taps - 1) + k + r0
                    acc = acc + ext[c, start:start + step, :] * tap_ref[c, k:k + 1, :]
                filt[c, r0:r0 + step, :] = acc

    chan_copy = send(stats, stats_got, chan_send, chan_recv, {"tp": partner})

    def convolve_first():
        @pl.when(me > 0)
        def _():
            halo_copy.wait_recv()
            for c in range(slabs):
                ext[c, :HALO, :] = halo[:, c * LANES:(c + 1) * LANES].astype(f32)

        @pl.when(me == 0)
        def _():
            for c in range(slabs):
                ext[c, :HALO, :] = jnp.zeros((HALO, LANES), f32)

        convolve([0])
        total = filt[0]
        for c in range(1, slabs):
            total = total + filt[c]
        lsum = jnp.sum(total, axis=1, keepdims=True)
        mean = lsum * (1.0 / chans)
        square = jnp.zeros((rows, LANES), f32)
        for c in range(slabs):
            dev = filt[c] - mean
            square = square + dev * dev
        lsq = jnp.sum(square, axis=1, keepdims=True)
        stats[...] = jnp.where(low, lsum, lsq)
        chan_copy.start()

    def channel_norm():
        chan_copy.wait()
        mine, other = stats[...], stats_got[...]
        mean = (mine[:, 0:1] + other[:, 0:1]) * (1.0 / total_channels)
        spread = jnp.zeros((rows, 1), f32)
        for s in (mine, other):
            apart = s[:, 0:1] * (1.0 / chans) - mean
            spread = spread + s[:, HEAD_DIM:HEAD_DIM + 1] + chans * apart * apart
        scale = lax.rsqrt(spread * (1.0 / total_channels) + norm_eps)
        for c in range(slabs):
            cols = slice(c * LANES, (c + 1) * LANES)
            y = (filt[c] - mean) * scale * cgain_ref[cols].astype(f32).reshape(1, -1) + cshift_ref[cols].astype(f32).reshape(1, -1)
            conv_ref[:, cols] = (y * jax.nn.sigmoid(y)).astype(bf16)

    tile = min(1024, model)

    def conv_product():
        filter_copy.wait()
        for c in range(0, model, tile):
            conv_share[:, c:c + tile] = jnp.dot(
                conv_ref[...], out_weights[0, :, c:c + tile], preferred_element_type=f32)

    ri = lax.broadcasted_iota(jnp.int32, (rows, rows), 0)
    ci = lax.broadcasted_iota(jnp.int32, (rows, rows), 1)
    tri = (ri >= ci).astype(bf16)

    def split_keys(k):
        zero = jnp.zeros_like(k)
        return jnp.where(low, k, zero), jnp.where(low, zero, k)

    def split_values(v):
        one = jnp.ones_like(v)
        return jnp.where(low, v, one), jnp.where(low, one, v)

    strict = ci < ri

    def attend(blocks_q, k, v, off, own_first):
        q = jnp.concatenate(blocks_q, axis=0)
        z = lax.dot_general(q, k, (((1,), (1,)), ((), ())), preferred_element_type=f32) + off
        lose = jnp.maximum(z, jnp.log(1.0 + jnp.exp2(jnp.minimum(z, 100.0))) * LOG2E)

        def masked(x):
            if not own_first:
                return x
            head = jnp.where(strict, x[:rows], 0.0)
            return jnp.concatenate([head, x[rows:]], axis=0) if len(blocks_q) > 1 else head

        cum = jnp.dot(masked(lose).astype(bf16), tri, preferred_element_type=f32)
        w = masked(jnp.exp2(z - cum))
        res = jnp.dot(w.astype(bf16), v, preferred_element_type=f32)
        pieces = []
        for r in range(len(blocks_q)):
            some = slice(r * rows, (r + 1) * rows)
            pieces.append((res[some], jnp.broadcast_to(cum[some, 0:1], (rows, LANES))))
        return pieces

    def note(which, g, h, res, total):
        base = 0 if h else HEAD_DIM
        masses[which] = jnp.where(lane == base + g, res, jnp.where(lane == base + 4 + g, total, masses[which]))

    def pair(a, b):
        return jnp.where(low, a, b)

    def near_blocks(g, others):
        keys = split_keys(packet[1, g])
        values = split_values(packet[2, g])
        rest = []
        for h in range(2):
            first, *more = attend([packet[0, g]] + others, keys[h], values[h], off_rows[0, pl.ds(2 * g + h, 1), :], True)
            res, total = first
            own_r[g, h] = res
            own_t[g, h] = jnp.exp2(-total)
            note(0, g, h, res, total)
            rest.append(more)
        return rest

    convolve(range(step, rows, step))

    def q_from(src_dev, dst_dev, g):
        return send(packet.at[0, g], q_in.at[src_dev - 2, g], q_send.at[dst_dev - 1, g],
                    q_recv.at[src_dev - 2, g], {"sp": src_dev})

    def kv_from(src_dev, g):
        for t in range(2):
            send(packet.at[1 + t, g], kv_in.at[t, g], kv_send.at[t, g], kv_recv.at[t, g], {"sp": src_dev}).wait_recv()
        return split_keys(kv_in[0, g]), split_values(kv_in[1, g])

    def offs_from(src_dev, dst_dev, row):
        send(offs, offs_in.at[src_dev], offs_sem_send.at[0], offs_sem_recv.at[src_dev % 2], {"sp": src_dev}).wait_recv()
        off_rows[row] = offs_in[src_dev].astype(f32) * LOG2E

    def off_of(row, g, h):
        return off_rows[row, pl.ds(2 * g + h, 1), :]

    def stat_rows(which):
        t = jnp.transpose(masses[which])
        return jnp.concatenate([t[0:8], t[HEAD_DIM:HEAD_DIM + 8]], axis=0)

    blocks = (lax.broadcasted_iota(jnp.int32, (LANES, LANES), 0) // HEAD_DIM
              == lax.broadcasted_iota(jnp.int32, (LANES, LANES), 1) // HEAD_DIM).astype(bf16)

    def close(place_at, g, o):
        sq = jnp.dot((o * o).astype(bf16), blocks, preferred_element_type=f32)
        gain = gain_ref[g * LANES:(g + 1) * LANES].astype(f32).reshape(1, LANES)
        cols = slice(place_at * LANES, (place_at + 1) * LANES)
        heads_ref[:, cols] = (o * lax.rsqrt(sq * (1.0 / HEAD_DIM) + rms_eps) * gain).astype(bf16)

    @pl.when((me == 0) | (me == 3))
    def _():
        @pl.loop(0, groups // 2)
        def _(half):
            for u in range(2):
                near_blocks(2 * half + u, [])

            @pl.when((me == 3) & (half == 0))
            def _():
                q_copy(3, 1, 3).start()

    @pl.when(me == 1)
    def _():
        near_blocks(far_g, [])
        offs_from(0, 1, 1)

        @pl.loop(1, groups)
        def _(g):
            q_from(2, 1, g).wait_recv()
            q_from(3, 1, g).wait_recv()
            rest = near_blocks(g, [q_in[1, g], q_in[0, g]])
            for h in range(2):
                for i in (1, 0):
                    res, total = rest[h][1 - i]
                    far_r[i, h] = res
                    far_t[i, h] = jnp.exp2(-total)
            keys, values = kv_from(0, g)
            parts = [[], []]
            for h in range(2):
                pieces = attend([q_in[1, g], q_in[0, g], packet[0, g]], keys[h], values[h], off_of(1, g, h), False)
                for i in (1, 0):
                    res = far_r[i, h] + far_t[i, h] * pieces[1 - i][0]
                    note(1 + i, g, h, res, res)
                    parts[i].append(res)
                res = own_r[g, h] + own_t[g, h] * pieces[2][0]
                own_r[g, h] = res
                note(0, g, h, res, res)
            for i in (1, 0):
                o_out[i, g] = pair(*parts[i]).astype(bf16)
            for i in (1, 0):
                send(o_out.at[i, g], o_in.at[0, g], o_send.at[i, g], o_recv.at[0, g], {"sp": i + 2}).start()

        for i in (1, 0):
            stat_out[i] = stat_rows(1 + i)
            stat_copy(1, i + 2).start()

    @pl.when(me == 2)
    def _():
        near_blocks(1, [])
        q_copy(2, 1, 3).start()

        @pl.loop(1, 2)
        def _(half):
            for u in range(2):
                near_blocks(2 * half + u, [])

    convolve_first()

    @pl.when(me == 2)
    def _():
        q_from(3, 2, far_g).wait_recv()
        rest = near_blocks(far_g, [q_in[1, far_g]])
        for h in range(2):
            res, total = rest[h][0]
            far_r[1, h] = res
            far_t[1, h] = jnp.exp2(-total)
        offs_from(1, 2, 2)
        offs_from(0, 2, 1)
        for src in (1, 0):
            for t in range(2):
                send(packet.at[1 + t, far_g], kv_in.at[t, src], kv_last_send.at[t],
                     kv_last_recv.at[t, src], {"sp": src}).wait_recv()
            keys = split_keys(kv_in[0, src])
            values = split_values(kv_in[1, src])
            parts = []
            for h in range(2):
                (own, own_total), (far, far_total) = attend(
                    [packet[0, far_g], q_in[1, far_g]], keys[h], values[h], off_rows[1 + src, 2 * far_g + h:2 * far_g + h + 1, :], False)
                own = own_r[far_g, h] + own_t[far_g, h] * own
                far = far_r[1, h] + far_t[1, h] * far
                own_r[far_g, h] = own
                if src:
                    far_r[1, h] = far
                    own_t[far_g, h] = own_t[far_g, h] * jnp.exp2(-own_total)
                    far_t[1, h] = far_t[1, h] * jnp.exp2(-far_total)
                else:
                    note(0, far_g, h, own, own)
                    note(2, far_g, h, far, far)
                    parts.append(far)
        o_out[1, far_g] = pair(*parts).astype(bf16)
        o_out[1, far_g] = pair(*parts).astype(bf16)
        o_copy(2, 3, far_g).start()
        stat_out[1] = stat_rows(2)
        stat_copy(2, 3).start()

    @pl.when(me == 1)
    def _():
        for g in dev1_groups:
            close(g - 1, g, pair(own_r[g, 0], own_r[g, 1]))

    channel_norm()
    conv_product()

    @pl.when(me == 3)
    def _():
        offs_from(2, 3, 1)
        for g in dev1_groups:
            keys, values = kv_from(2, g)
            for h in range(2):
                res, total = attend([packet[0, g]], keys[h], values[h], off_of(1, g, h), False)[0]
                through = own_t[g, h]
                res = own_r[g, h] + through * res
                own_r[g, h] = res
                own_t[g, h] = through * jnp.exp2(-total)
                near = masses[0][:, (HEAD_DIM, 0)[h] + 4 + g:(HEAD_DIM, 0)[h] + 5 + g]
                note(0, g, h, res, total + near)

    def finish(g):
        own = pair(own_r[g, 0], own_r[g, 1])

        @pl.when(me == 0)
        def _():
            close(g, g, own)

        @pl.when(me == 2)
        def _():
            if g == far_g:
                close(g, g, own)
            else:
                through = pair(own_t[g, 0], own_t[g, 1])
                send(o_out.at[0, g], o_in.at[0, g], o_send.at[0, g], o_recv.at[0, g], {"sp": 1}).wait_recv()
                close(g, g, own + through * o_in[0, g].astype(f32))

        @pl.when(me == 3)
        def _():
            through = pair(own_t[g, 0], own_t[g, 1])
            src = 2 if g == far_g else 1
            send(o_out.at[1, g], o_in.at[src - 1, g], o_send.at[1, g], o_recv.at[src - 1, g], {"sp": src}).wait_recv()
            close(g, g, own + through * o_in[src - 1, g].astype(f32))

    for copy in attend_copies(False):
        copy.wait()
    share = rows // tp
    theirs = pl.ds(pl.multiple_of(partner * share, share), share)
    ours = pl.ds(pl.multiple_of(core * share, share), share)
    weight_swap = send(out_weights.at[1, pl.ds(cut, LANES)], partner_weights, swap_send.at[0], swap_recv.at[0], {"tp": partner})
    heads_swap = send(heads_last.at[theirs], partner_heads, swap_send.at[1], swap_recv.at[1], {"tp": partner})
    weight_swap.start()
    for g in range(final):
        finish(g)
    leaves = []
    for c in range(0, model, tile):
        cols = slice(c, c + tile)
        leaving[:, cols] = (conv_share[theirs, cols] + jnp.dot(
            heads_ref[theirs, :cut], out_weights[1, :cut, cols], preferred_element_type=f32)).astype(bf16)
        copy = send(leaving.at[:, pl.ds(c, tile)], arrived_ref.at[:, pl.ds(c, tile)],
                    out_send.at[c // tile], out_recv.at[c // tile], {"tp": partner})
        copy.start()
        leaves.append(copy)
    for c in range(0, model, tile):
        cols = slice(c, c + tile)
        conv_share[ours, cols] += jnp.dot(
            heads_ref[ours, :cut], out_weights[1, :cut, cols], preferred_element_type=f32)
    @pl.when(me == 1)
    def _():
        keys, values = kv_from(0, far_g)
        parts = []
        for h in range(2):
            res, _ = attend([packet[0, far_g]], keys[h], values[h], off_of(1, far_g, h), False)[0]
            res = own_r[far_g, h] + own_t[far_g, h] * res
            note(0, far_g, h, res, res)
            parts.append(res)
        close(final, far_g, pair(*parts))

    finish(final)
    heads_last[...] = heads_ref[:, cut:]
    heads_swap.start()
    for copy in leaves:
        copy.wait()
    weight_swap.wait()
    for c in range(0, model, tile):
        cols = slice(c, c + tile)
        conv_share[ours, cols] += arrived_ref[:, cols].astype(f32) + jnp.dot(
            heads_ref[ours, cut:], out_weights[1, cut:, cols], preferred_element_type=f32)

    mine = stat_rows(0)

    def write_log(m_odd, m_even):
        for g in range(groups):
            log_ref[2 * g:2 * g + 1] = jnp.log(jnp.maximum(m_even[g:g + 1], mass_floor))
            log_ref[2 * g + 1:2 * g + 2] = jnp.log(jnp.maximum(m_odd[g:g + 1], mass_floor))

    @pl.when(me < 2)
    def _():
        write_log(mine[0:4], mine[8:12])

    @pl.when(me == 2)
    def _():
        stat_copy(1, 2).wait_recv()
        far = stat_in[0]
        write_log(mine[0:4] + jnp.exp2(-mine[4:8]) * far[0:4], mine[8:12] + jnp.exp2(-mine[12:16]) * far[8:12])

    @pl.when(me == 3)
    def _():
        for src in (1, 2):
            send(stat_out.at[1], stat_in.at[src - 1], flow_send.at[2, 2], stat_recv.at[src - 1], {"sp": src}).wait_recv()
        far = stat_in[0] + stat_in[1]
        write_log(mine[0:4] + jnp.exp2(-mine[4:8]) * far[0:4], mine[8:12] + jnp.exp2(-mine[12:16]) * far[8:12])

    heads_swap.wait()
    for c in range(0, model, tile):
        cols = slice(c, c + tile)
        out_ref[:, cols] = (conv_share[ours, cols] + jnp.dot(
            partner_heads[...], partner_weights[:, cols], preferred_element_type=f32)).astype(bf16)

    @pl.when(me < n - 1)
    def _():
        halo_copy.wait_send()

    @pl.when(me == 0)
    def _():
        offs_copy(0, 1).wait_send()
        offs_copy(0, 2).wait_send()
        for t in range(2):
            for g in range(groups):
                kv_copy(0, t, g).wait_send()
            kv_last(t, 0).wait_send()

    @pl.when(me == 1)
    def _():
        offs_copy(1, 2).wait_send()
        for t in range(2):
            kv_last(t, 1).wait_send()
        for i in (1, 0):
            for g in dev1_groups:
                o_copy(1, i + 2, g).wait_send()
            stat_copy(1, i + 2).wait_send()

    @pl.when(me == 2)
    def _():
        offs_copy(2, 3).wait_send()
        for g in dev1_groups:
            q_copy(2, 1, g).wait_send()
            for t in range(2):
                kv_copy(2, t, g).wait_send()
        o_copy(2, 3, far_g).wait_send()
        stat_copy(2, 3).wait_send()

    @pl.when(me == 3)
    def _():
        for g in dev1_groups:
            q_copy(3, 1, g).wait_send()
        q_copy(3, 2, far_g).wait_send()


def place(mixed, mass_log, out_ref, log_ref, sem):
    copies = [
        pltpu.make_async_copy(mixed, out_ref, sem.at[0]),
        pltpu.make_async_copy(mass_log, log_ref, sem.at[1]),
    ]
    for copy in copies:
        copy.start()
    for copy in copies:
        copy.wait()


def local(n, tp,
    stream, norm_gain, query_weight, key_weight, value_weight, filter_input, filter_gate,
    score_offset, head_gain, filter_taps, channel_gain, channel_shift, attend_out, filter_out,
):
    f32, bf16 = jnp.float32, jnp.bfloat16
    rows = stream.shape[1]
    heads = score_offset.shape[2]
    groups = heads * HEAD_DIM // LANES
    chans = filter_input.shape[1]
    slabs = chans // LANES
    taps = filter_taps.shape[0]
    model = stream.shape[2]
    share = rows // tp
    tiles = model // min(1024, model)

    vmem = pl.BlockSpec(memory_space=pltpu.VMEM)
    hbm = pl.BlockSpec(memory_space=pltpu.HBM)
    dma = pltpu.SemaphoreType.DMA
    mixed, mass_log = pl.pallas_call(
        functools.partial(kernel, n, tp, taps, chans * tp),
        out_shape=(pltpu.VMEM((share, model), bf16), pltpu.VMEM((heads, rows), f32)),
        in_specs=[hbm] * 14,
        out_specs=(vmem,) * 2,
        scratch_shapes=[
            pltpu.VMEM((model,), bf16),
            pltpu.VMEM((heads, rows), bf16),
            pltpu.VMEM((taps, chans), bf16),
            pltpu.VMEM((chans,), bf16),
            pltpu.VMEM((chans,), bf16),
            pltpu.VMEM((chans,), bf16),
            pltpu.VMEM((rows, model), bf16),
            pltpu.VMEM((rows, model), bf16),
            pltpu.VMEM((5, model, chans), bf16),
            pltpu.VMEM((2, chans, model), bf16),
            pltpu.VMEM((3, groups, rows, LANES), bf16),
            pltpu.VMEM((2, groups, rows, LANES), bf16),
            pltpu.VMEM((2, groups, rows, LANES), bf16),
            pltpu.VMEM((3, heads, rows), bf16),
            pltpu.VMEM((2, groups, rows, LANES), bf16),
            pltpu.VMEM((2, groups, rows, LANES), bf16),
            pltpu.VMEM((2, 16, rows), f32),
            pltpu.VMEM((2, 16, rows), f32),
            pltpu.VMEM((groups, 2, rows, LANES), f32),
            pltpu.VMEM((groups, 2, rows, LANES), f32),
            pltpu.VMEM((2, 2, rows, LANES), f32),
            pltpu.VMEM((2, 2, rows, LANES), f32),
            pltpu.VMEM((3, rows, LANES), f32),
            pltpu.VMEM((3, heads, rows), f32),
            pltpu.VMEM((slabs, taps + -taps % 8, LANES), f32),
            pltpu.VMEM((rows, heads * HEAD_DIM), bf16),
            pltpu.VMEM((rows, chans), bf16),
            pltpu.VMEM((rows, model), f32),
            pltpu.VMEM((share, model), bf16),
            pltpu.VMEM((share, model), bf16),
            pltpu.VMEM((rows, LANES), bf16),
            pltpu.VMEM((share, LANES), bf16),
            pltpu.VMEM((LANES, model), bf16),
            pltpu.VMEM((HALO, chans), bf16),
            pltpu.VMEM((HALO, chans), bf16),
            pltpu.VMEM((slabs, HALO + rows, LANES), f32),
            pltpu.VMEM((slabs, rows, LANES), f32),
            pltpu.VMEM((rows, LANES), f32),
            pltpu.VMEM((rows, LANES), f32),
            dma((5, chans // (2 * LANES))), dma((3,)), dma((3, groups)), dma((4, groups)), dma((2,)), dma((2,)),
            dma((tiles,)), dma((tiles,)), dma, dma, dma, dma, pltpu.SemaphoreType.REGULAR, dma((2,)), dma((2,)),
        ],
        compiler_params=pltpu.CompilerParams(
            collective_id=0, has_side_effects=True, vmem_limit_bytes=56 * 1024 * 1024),
    )(stream[0], norm_gain, score_offset[0].T, filter_taps, head_gain, channel_gain, channel_shift,
      query_weight, key_weight, value_weight, filter_input, filter_gate, attend_out, filter_out)
    mixed, mass_log = pl.pallas_call(
        place,
        out_shape=(
            jax.ShapeDtypeStruct((share, model), bf16),
            jax.ShapeDtypeStruct((heads, rows), f32),
        ),
        in_specs=[vmem] * 2,
        out_specs=(hbm,) * 2,
        scratch_shapes=[dma((2,))],
    )(*[pltpu.with_memory_space_constraint(a, pltpu.VMEM) for a in (mixed, mass_log)])
    return (mixed[None], mass_log.T[None])


def shifted(value, axis, steps):
    count = lax.axis_size(axis)
    first, last = (max(0, -steps), min(count, count - steps))
    return lax.ppermute(value, axis, [(source, source + steps) for source in range(first, last)])


def local_ring(
    stream,
    norm_gain,
    query_weight,
    key_weight,
    value_weight,
    filter_input,
    filter_gate,
    score_offset,
    head_gain,
    filter_taps,
    channel_gain,
    channel_shift,
    attend_out,
    filter_out,
):
    rows_here = stream.shape[1]
    total_channels = filter_input.shape[1] * lax.axis_size("tp")
    xfloat = stream[0].astype(jnp.float32)
    normed = xfloat * lax.rsqrt(jnp.mean(xfloat * xfloat, axis=-1, keepdims=True) + rms_eps)
    normed = (normed * norm_gain.astype(jnp.float32)).astype(jnp.bfloat16)

    def project(weight):
        return jnp.dot(normed, weight, preferred_element_type=jnp.float32).astype(jnp.bfloat16)

    queries = project(query_weight)
    keys_here = project(key_weight)
    values_here = project(value_weight)
    conv_in = project(filter_input)
    conv_gate = project(filter_gate)
    offsets_here = score_offset[0]
    heads_here = offsets_here.shape[1]
    first_pos = lax.axis_index("sp") * rows_here
    position = first_pos + jnp.arange(rows_here, dtype=jnp.int32)
    qheads = queries.reshape(rows_here, heads_here, HEAD_DIM)

    def absorb(state_now, kblock, vblock, oblock, first_key):
        attended, weight_mass, survive = state_now
        span = kblock.shape[0]
        kblock = kblock.reshape(span, heads_here, HEAD_DIM)
        vblock = vblock.reshape(span, heads_here, HEAD_DIM)
        scores = jnp.einsum(
            "thd,shd->hts", qheads, kblock, preferred_element_type=jnp.float32
        ) * HEAD_DIM ** (-0.5)
        scores = scores + oblock.astype(jnp.float32).T[:, None, :]
        key_pos = first_key + jnp.arange(span, dtype=jnp.int32)
        strict = ((key_pos[None, :] < position[:, None]) & (key_pos[None, :] >= 0))[None]
        losing = jnp.where(strict, jax.nn.log_sigmoid(-scores), 0.0)
        beyond = lax.cumsum(losing, axis=2, reverse=True) - losing + survive[:, :, None]
        weights = jnp.where(strict, jnp.exp(jax.nn.log_sigmoid(scores) + beyond), 0.0)
        weight_mass = weight_mass + jnp.sum(weights, axis=2)
        attended = attended + jnp.einsum(
            "hts,shd->thd", weights.astype(jnp.bfloat16), vblock, preferred_element_type=jnp.float32
        )
        survive = survive + jnp.sum(losing, axis=2)
        return (attended, weight_mass, survive)

    initial = (
        jnp.zeros((rows_here, heads_here, HEAD_DIM), jnp.float32),
        jnp.zeros((heads_here, rows_here), jnp.float32),
        jnp.zeros((heads_here, rows_here), jnp.float32),
    )
    state_now = absorb(initial, keys_here, values_here, offsets_here, first_pos)

    def pass_turn(turn_index, carried):
        state_now, travelling = carried
        travelling = shifted((travelling[0], travelling[1], travelling[2]), "sp", 1)
        first_key = first_pos - (turn_index + 1) * rows_here
        state_now = absorb(state_now, travelling[0], travelling[1], travelling[2], first_key)
        return (state_now, travelling)

    state_now, travelling = lax.fori_loop(
        0, lax.axis_size("sp") - 1, pass_turn, (state_now, (keys_here, values_here, offsets_here))
    )
    attended, weight_mass, survive = state_now
    head_scale = lax.rsqrt(jnp.mean(attended * attended, axis=-1, keepdims=True) + rms_eps)
    heads_flat = attended * head_scale * head_gain.astype(jnp.float32).reshape(heads_here, HEAD_DIM)
    heads_flat = heads_flat.astype(jnp.bfloat16).reshape(rows_here, heads_here * HEAD_DIM)
    mass_log = jnp.log(jnp.maximum(weight_mass.T, mass_floor))
    gated_rows = (
        conv_in.astype(jnp.float32) * jax.nn.sigmoid(conv_gate.astype(jnp.float32))
    ).astype(jnp.bfloat16)
    reach_back = filter_taps.shape[0] - 1
    earlier = shifted(gated_rows[rows_here - reach_back :], "sp", 1)
    extended = jnp.concatenate([earlier, gated_rows], axis=0).astype(jnp.float32)
    tap_values = filter_taps.astype(jnp.float32)
    filtered = jnp.zeros((rows_here, gated_rows.shape[1]), jnp.float32)
    for tap_index in range(reach_back + 1):
        filtered = filtered + extended[tap_index : tap_index + rows_here] * tap_values[tap_index]
    center = lax.psum(jnp.sum(filtered, axis=-1), "tp") / total_channels
    deviation = filtered - center[:, None]
    spread = lax.psum(jnp.sum(deviation * deviation, axis=-1), "tp") / total_channels
    conv_out = jax.nn.silu(
        deviation * lax.rsqrt(spread[:, None] + norm_eps) * channel_gain.astype(jnp.float32)
        + channel_shift.astype(jnp.float32)
    ).astype(jnp.bfloat16)
    mixed_out = lax.psum_scatter(
        (
            jnp.dot(heads_flat, attend_out, preferred_element_type=jnp.float32)
            + jnp.dot(conv_out, filter_out, preferred_element_type=jnp.float32)
        ).astype(jnp.bfloat16),
        "tp",
        scatter_dimension=0,
        tiled=True,
    )
    return (mixed_out[None], mass_log[None])


def solution(mesh):
    n, tp = mesh.shape["sp"], mesh.shape["tp"]

    def choose(*args):
        rows, heads, chans = args[0].shape[1], args[7].shape[2], args[5].shape[1]
        same = args[2].shape[1] == chans and heads * HEAD_DIM == 4 * LANES == chans
        if n == 4 and tp == 2 and same and rows % 128 == 0:
            return local(n, tp, *args)
        return local_ring(*args)

    return jax.shard_map(
        choose,
        mesh=mesh,
        in_specs=(
            P("fs", "sp", None), P(), P(None, "tp"), P(None, "tp"), P(None, "tp"),
            P(None, "tp"), P(None, "tp"), P("fs", "sp", "tp"), P("tp"), P(None, "tp"),
            P("tp"), P("tp"), P("tp", None), P("tp", None),
        ),
        out_specs=(P("fs", ("sp", "tp"), None), P("fs", "sp", "tp")),
        check_vma=False,
    )
```

```python
import functools

import jax
import jax.numpy as jnp
from jax import lax
from jax.experimental import pallas as pl
from jax.experimental.pallas import tpu as pltpu
from jax.sharding import PartitionSpec as P

HEAD_DIM = 64

rms_eps = 1e-06
norm_eps = 1e-05
mass_floor = 0.01
HALO = 32
LANES = 128
LOG2E = 1.4426950408889634
MESH = pl.DeviceIdType.MESH


class Slots:
    def __init__(self, pick):
        self.pick = pick

    @property
    def at(self):
        return self

    def __getitem__(self, index):
        return self.pick(*index) if isinstance(index, tuple) else self.pick(index)


def kernel(
    n, tp, taps, total_channels,
    stream_hbm, ngain_hbm, offs_hbm, taps_hbm, gain_hbm, cgain_hbm, cshift_hbm,
    q_hbm, k_hbm, v_hbm, in_hbm, gate_hbm, attend_hbm, filter_hbm,
    out_ref, log_ref,
    ngain, offs, raw_taps, gain_ref, cgain_ref, cshift_ref,
    stream, normed, weights, out_weights, packet, q_in, kv_in, offs_in, o_out, o_in, stat_out, stat_in,
    own_r, own_t, far_r, far_t, masses, off_rows, tap_ref, heads_ref, conv_ref, conv_share, leaving, arrived_ref, heads_last, partner_heads, partner_weights,
    gated, halo, ext, filt, stats, stats_got,
    weight_sem, out_weight_sem, flow_send, flow_recv, offs_sem_send, offs_sem_recv,
    out_send, out_recv, halo_send, halo_recv, chan_send, chan_recv, entered, swap_send, swap_recv,
):
    f32, bf16 = jnp.float32, jnp.bfloat16
    small_sem = Slots(lambda t: (out_weight_sem.at[t] if t < 3 else out_send.at[t - 3] if t < 5 else swap_send.at[0]))
    stream_sem = Slots(lambda c: flow_send.at[0, c])
    kv_send, o_send = flow_send, flow_send
    q_send = Slots(lambda i, g: flow_send.at[2, g])
    kv_last_send = Slots(lambda t: flow_send.at[2, t])
    kv_recv, kv_last_recv = flow_recv, flow_recv
    q_recv = Slots(lambda i, g: flow_recv.at[2 + i, g])
    o_recv = q_recv
    stat_recv = Slots(lambda i: flow_recv.at[3, 1 + i])
    me = lax.axis_index("sp")
    core = lax.axis_index("tp")
    partner = 1 - core
    rows, model = normed.shape
    chans = in_hbm.shape[1]
    groups = packet.shape[1]
    slabs = chans // LANES
    lane = lax.broadcasted_iota(jnp.int32, (rows, LANES), 1)
    low = lane < HEAD_DIM

    def local_copy(src, dst, sem):
        return pltpu.make_async_copy(src, dst, sem)

    def send(src, dst, send_sem, recv_sem, to):
        return pltpu.make_async_remote_copy(
            src_ref=src, dst_ref=dst, send_sem=send_sem, recv_sem=recv_sem,
            device_id=to, device_id_type=MESH)

    projections = (q_hbm, k_hbm, v_hbm)
    first_order, other_order = (1, 2, 0), (0, 1, 2)

    def slot_of(t):
        return jnp.where(me == 0, first_order[t], other_order[t])

    wide = 2 * LANES
    halves = chans // wide

    def weight_copy(w, slot, half):
        cols = pl.ds(half * wide, wide)
        return local_copy(w.at[:, cols], weights.at[slot, :, cols], weight_sem.at[slot, half])

    def fetch(t, half):
        for order, here in ((first_order, me == 0), (other_order, me != 0)):
            @pl.when(here)
            def _(s=order[t]):
                weight_copy(projections[s], s, half).start()

    band = rows // packet.shape[1]

    def stream_copy(c):
        some = pl.ds(pl.multiple_of(c * band, band), band)
        return local_copy(stream_hbm.at[some], stream.at[some], stream_sem.at[c])

    small = [local_copy(a, b, small_sem.at[t]) for t, (a, b) in enumerate((
        (ngain_hbm, ngain), (offs_hbm, offs), (taps_hbm, raw_taps), (gain_hbm, gain_ref),
        (cgain_hbm, cgain_ref), (cshift_hbm, cshift_ref)))]
    gate_copies = [weight_copy(w, 3 + t, half) for half in range(halves) for t, w in enumerate((in_hbm, gate_hbm))]
    filter_copy = local_copy(filter_hbm, out_weights.at[0], out_weight_sem.at[0])
    final = groups - 1
    cut = final * LANES

    def attend_copies(first):
        early = local_copy(attend_hbm.at[pl.ds(LANES if first else 0, cut)], out_weights.at[1, pl.ds(0, cut)], out_weight_sem.at[1])
        late = local_copy(attend_hbm.at[pl.ds(0 if first else cut, LANES)], out_weights.at[1, pl.ds(cut, LANES)], out_weight_sem.at[2])
        return early, late
    for c in range(rows // band):
        stream_copy(c).start()
    small[0].start()
    for t in range(2):
        fetch(t, 0)
    for copy in small[1:]:
        copy.start()

    barrier = pltpu.get_barrier_semaphore()
    peers = {0: (1,), 1: (0, 2, 3), 2: (1, 3), 3: (1, 2)}
    pl.semaphore_signal(barrier, inc=1, device_id={"tp": partner}, device_id_type=MESH)
    for d in range(n):
        @pl.when(me == d)
        def _(d=d):
            for p in peers[d]:
                pl.semaphore_signal(barrier, inc=1, device_id={"sp": p}, device_id_type=MESH)

    small[0].wait()
    norm_gain = ngain[...].astype(f32).reshape(1, -1)

    @pl.loop(0, rows // band)
    def _(c):
        stream_copy(c).wait()

        @pl.when(c == 0)
        def _():
            for half in range(1, halves):
                for t in range(2):
                    fetch(t, half)
            for copy in gate_copies:
                copy.start()

        some = pl.ds(pl.multiple_of(c * band, band), band)
        x = stream[some, :].astype(f32)
        x = x * lax.rsqrt(jnp.mean(x * x, axis=-1, keepdims=True) + rms_eps)
        normed[some, :] = (x * norm_gain).astype(bf16)

    for half in range(halves):
        fetch(2, half)
    for copy in small[1:]:
        copy.wait()

    def q_copy(src_dev, dst_dev, g):
        return send(packet.at[0, g], q_in.at[src_dev - 2, g], q_send.at[dst_dev - 1, g],
                    q_recv.at[src_dev - 2, g], {"sp": dst_dev})

    far_g = 0
    dev1_groups = range(1, groups)

    def kv_copy(src_dev, t, g):
        return send(packet.at[1 + t, g], kv_in.at[t, g], kv_send.at[t, g], kv_recv.at[t, g], {"sp": src_dev + 1})

    def kv_last(t, src_dev):
        return send(packet.at[1 + t, far_g], kv_in.at[t, src_dev],
                    kv_last_send.at[t], kv_last_recv.at[t, src_dev], {"sp": 2})

    def offs_copy(src_dev, dst_dev):
        return send(offs, offs_in.at[src_dev], offs_sem_send.at[int((src_dev, dst_dev) == (0, 2))], offs_sem_recv.at[src_dev % 2],
                    {"sp": dst_dev})

    def o_copy(src_dev, dst_dev, g):
        return send(o_out.at[dst_dev - 2, g], o_in.at[src_dev - 1, g], o_send.at[dst_dev - 2, g],
                    o_recv.at[src_dev - 1, g], {"sp": dst_dev})

    def stat_copy(src_dev, dst_dev):
        return send(stat_out.at[dst_dev - 2], stat_in.at[src_dev - 1],
                    flow_send.at[2, dst_dev] if src_dev == 1 else flow_send.at[0, 0],
                    stat_recv.at[src_dev - 1], {"sp": dst_dev})

    def keep(slot, half, y):
        factor = jnp.where(slot == 0, LOG2E * HEAD_DIM ** (-0.5), 1.0).astype(f32)
        y = (y * factor).astype(bf16)
        for u in range(2):
            packet[slot, 2 * half + u] = y[:, u * LANES:(u + 1) * LANES]

    def project(jobs):
        for t, half in jobs:
            slot = slot_of(t)
            weight_copy(q_hbm, slot, half).wait()
        for t, half in jobs:
            slot = slot_of(t)
            keep(slot, half, jnp.dot(
                normed[...], weights[slot, :, half * wide:(half + 1) * wide], preferred_element_type=f32))

    for half in range(halves):
        project([(0, half), (1, half)])

        if half == 0:
            for d in range(n):
                @pl.when(me == d)
                def _(d=d):
                    pl.semaphore_wait(barrier, len(peers[d]) + tp - 1)

        groups_here = (2 * half, 2 * half + 1)

        @pl.when(me == 0)
        def _():
            if half == 0:
                offs_copy(0, 1).start()
                for t in range(2):
                    kv_copy(0, t, 1).start()

        @pl.when(me == 1)
        def _():
            if half == 0:
                pl.semaphore_signal(entered, inc=1, device_id={"sp": 0}, device_id_type=MESH)
                offs_copy(1, 2).start()

        @pl.when(me == 2)
        def _():
            if half == 0:
                offs_copy(2, 3).start()
            if half == 0:
                q_copy(2, 1, 1).start()
            for g in groups_here:
                if g in dev1_groups:
                    kv_copy(2, 0, g).start()

        @pl.when(me == 3)
        def _():
            if half == 0:
                q_copy(3, 1, 1).start()
            else:
                q_copy(3, 2, far_g).start()

    filter_copy.start()
    for first, here in ((True, me == 1), (False, me != 1)):
        @pl.when(here)
        def _(first=first):
            for copy in attend_copies(first):
                copy.start()
    tap_ref[...] = jnp.zeros_like(tap_ref)
    for c in range(slabs):
        tap_ref[c, :taps] = raw_taps[:, c * LANES:(c + 1) * LANES].astype(f32)
    off_rows[0] = offs[...].astype(f32) * LOG2E
    masses[...] = jnp.zeros_like(masses)
    for copy in gate_copies:
        copy.wait()

    @pl.loop(0, halves)
    def _(c):
        cols = pl.ds(pl.multiple_of(c * wide, wide), wide)
        x = normed[...]
        value = jnp.dot(x, weights[3, :, cols], preferred_element_type=f32).astype(bf16).astype(f32)
        gate = jnp.dot(x, weights[4, :, cols], preferred_element_type=f32).astype(bf16).astype(f32)
        g = (value * jax.nn.sigmoid(gate)).astype(bf16)
        gated[:, cols] = g[rows - HALO:]
        g = g.astype(f32)
        for u in range(2):
            ext[2 * c + u, HALO:, :] = g[:, u * LANES:(u + 1) * LANES]

    halo_copy = send(gated, halo, halo_send, halo_recv, {"sp": lax.rem(me + 1, n)})

    @pl.when(me == 0)
    def _():
        pl.semaphore_wait(entered, 1)
        offs_copy(0, 2).start()
        for t in range(2):
            kv_last(t, 0).start()
        for g in dev1_groups[1:]:
            for t in range(2):
                kv_copy(0, t, g).start()

    for d in (2, 3):
        @pl.when(me == d)
        def _(d=d):
            q_copy(d, 1, 2).start()

    @pl.when(me < n - 1)
    def _():
        halo_copy.start()

    @pl.when(me == 0)
    def _():
        for t in range(2):
            kv_copy(0, t, far_g).start()

    project([(2, half) for half in range(halves)])

    @pl.when(me == 1)
    def _():
        for t in range(2):
            kv_last(t, 1).start()

    @pl.when(me == 2)
    def _():
        for g in dev1_groups:
            kv_copy(2, 1, g).start()

    step = min(128, rows)

    def convolve(starts):
        @pl.loop(0, slabs)
        def _(c):
            for r0 in starts:
                acc = jnp.zeros((step, LANES), f32)
                for k in range(taps):
                    start = HALO - (taps - 1) + k + r0
                    acc = acc + ext[c, start:start + step, :] * tap_ref[c, k:k + 1, :]
                filt[c, r0:r0 + step, :] = acc

    chan_copy = send(stats, stats_got, chan_send, chan_recv, {"tp": partner})

    def convolve_first():
        @pl.when(me > 0)
        def _():
            halo_copy.wait_recv()
            for c in range(slabs):
                ext[c, :HALO, :] = halo[:, c * LANES:(c + 1) * LANES].astype(f32)

        @pl.when(me == 0)
        def _():
            for c in range(slabs):
                ext[c, :HALO, :] = jnp.zeros((HALO, LANES), f32)

        convolve([0])
        total = filt[0]
        for c in range(1, slabs):
            total = total + filt[c]
        lsum = jnp.sum(total, axis=1, keepdims=True)
        mean = lsum * (1.0 / chans)
        square = jnp.zeros((rows, LANES), f32)
        for c in range(slabs):
            dev = filt[c] - mean
            square = square + dev * dev
        lsq = jnp.sum(square, axis=1, keepdims=True)
        stats[...] = jnp.where(low, lsum, lsq)
        chan_copy.start()

    def channel_norm():
        chan_copy.wait()
        mine, other = stats[...], stats_got[...]
        mean = (mine[:, 0:1] + other[:, 0:1]) * (1.0 / total_channels)
        spread = jnp.zeros((rows, 1), f32)
        for s in (mine, other):
            apart = s[:, 0:1] * (1.0 / chans) - mean
            spread = spread + s[:, HEAD_DIM:HEAD_DIM + 1] + chans * apart * apart
        scale = lax.rsqrt(spread * (1.0 / total_channels) + norm_eps)
        for c in range(slabs):
            cols = slice(c * LANES, (c + 1) * LANES)
            y = (filt[c] - mean) * scale * cgain_ref[cols].astype(f32).reshape(1, -1) + cshift_ref[cols].astype(f32).reshape(1, -1)
            conv_ref[:, cols] = (y * jax.nn.sigmoid(y)).astype(bf16)

    tile = min(1024, model)

    def conv_product():
        filter_copy.wait()
        for c in range(0, model, tile):
            conv_share[:, c:c + tile] = jnp.dot(
                conv_ref[...], out_weights[0, :, c:c + tile], preferred_element_type=f32)

    ri = lax.broadcasted_iota(jnp.int32, (rows, rows), 0)
    ci = lax.broadcasted_iota(jnp.int32, (rows, rows), 1)
    tri = (ri > ci).astype(bf16)

    def split_keys(k):
        zero = jnp.zeros_like(k)
        return jnp.where(low, k, zero), jnp.where(low, zero, k)

    def split_values(v):
        one = jnp.ones_like(v)
        return jnp.where(low, v, one), jnp.where(low, one, v)

    strict = ci < ri

    def attend(blocks_q, k, v, off, own_first):
        q = jnp.concatenate(blocks_q, axis=0)
        z = lax.dot_general(q, k, (((1,), (1,)), ((), ())), preferred_element_type=f32) + off
        lose = jnp.maximum(z, jnp.log(1.0 + jnp.exp2(jnp.minimum(z, 100.0))) * LOG2E)

        def masked(x):
            if not own_first:
                return x
            head = jnp.where(strict, x[:rows], 0.0)
            return jnp.concatenate([head, x[rows:]], axis=0) if len(blocks_q) > 1 else head

        gain = z - lose
        lose = masked(lose)
        beyond = jnp.dot(lose.astype(bf16), tri, preferred_element_type=f32)
        w = masked(jnp.exp2(gain - beyond))
        res = jnp.dot(w.astype(bf16), v, preferred_element_type=f32)
        pieces = []
        for r in range(len(blocks_q)):
            some = slice(r * rows, (r + 1) * rows)
            pieces.append((res[some], jnp.broadcast_to(beyond[some, 0:1] + lose[some, 0:1], (rows, LANES))))
        return pieces

    def note(which, g, h, res, total):
        base = 0 if h else HEAD_DIM
        masses[which] = jnp.where(lane == base + g, res, jnp.where(lane == base + 4 + g, total, masses[which]))

    def pair(a, b):
        return jnp.where(low, a, b)

    def near_blocks(g, others):
        keys = split_keys(packet[1, g])
        values = split_values(packet[2, g])
        rest = []
        for h in range(2):
            first, *more = attend([packet[0, g]] + others, keys[h], values[h], off_rows[0, pl.ds(2 * g + h, 1), :], True)
            res, total = first
            own_r[g, h] = res
            own_t[g, h] = jnp.exp2(-total)
            note(0, g, h, res, total)
            rest.append(more)
        return rest

    convolve(range(step, rows, step))

    def q_from(src_dev, dst_dev, g):
        return send(packet.at[0, g], q_in.at[src_dev - 2, g], q_send.at[dst_dev - 1, g],
                    q_recv.at[src_dev - 2, g], {"sp": src_dev})

    def kv_from(src_dev, g):
        for t in range(2):
            send(packet.at[1 + t, g], kv_in.at[t, g], kv_send.at[t, g], kv_recv.at[t, g], {"sp": src_dev}).wait_recv()
        return split_keys(kv_in[0, g]), split_values(kv_in[1, g])

    def offs_from(src_dev, dst_dev, row):
        send(offs, offs_in.at[src_dev], offs_sem_send.at[0], offs_sem_recv.at[src_dev % 2], {"sp": src_dev}).wait_recv()
        off_rows[row] = offs_in[src_dev].astype(f32) * LOG2E

    def off_of(row, g, h):
        return off_rows[row, pl.ds(2 * g + h, 1), :]

    def stat_rows(which):
        t = jnp.transpose(masses[which])
        return jnp.concatenate([t[0:8], t[HEAD_DIM:HEAD_DIM + 8]], axis=0)

    blocks = (lax.broadcasted_iota(jnp.int32, (LANES, LANES), 0) // HEAD_DIM
              == lax.broadcasted_iota(jnp.int32, (LANES, LANES), 1) // HEAD_DIM).astype(bf16)

    def close(place_at, g, o):
        sq = jnp.dot((o * o).astype(bf16), blocks, preferred_element_type=f32)
        gain = gain_ref[g * LANES:(g + 1) * LANES].astype(f32).reshape(1, LANES)
        cols = slice(place_at * LANES, (place_at + 1) * LANES)
        heads_ref[:, cols] = (o * lax.rsqrt(sq * (1.0 / HEAD_DIM) + rms_eps) * gain).astype(bf16)

    @pl.when((me == 0) | (me == 3))
    def _():
        @pl.loop(0, groups // 2)
        def _(half):
            for u in range(2):
                near_blocks(2 * half + u, [])

            @pl.when((me == 3) & (half == 0))
            def _():
                q_copy(3, 1, 3).start()

    @pl.when(me == 1)
    def _():
        near_blocks(far_g, [])
        offs_from(0, 1, 1)

        @pl.loop(1, groups)
        def _(g):
            q_from(2, 1, g).wait_recv()
            q_from(3, 1, g).wait_recv()
            rest = near_blocks(g, [q_in[1, g], q_in[0, g]])
            for h in range(2):
                for i in (1, 0):
                    res, total = rest[h][1 - i]
                    far_r[i, h] = res
                    far_t[i, h] = jnp.exp2(-total)
            keys, values = kv_from(0, g)
            parts = [[], []]
            for h in range(2):
                pieces = attend([q_in[1, g], q_in[0, g], packet[0, g]], keys[h], values[h], off_of(1, g, h), False)
                for i in (1, 0):
                    res = far_r[i, h] + far_t[i, h] * pieces[1 - i][0]
                    note(1 + i, g, h, res, res)
                    parts[i].append(res)
                res = own_r[g, h] + own_t[g, h] * pieces[2][0]
                own_r[g, h] = res
                note(0, g, h, res, res)
            for i in (1, 0):
                o_out[i, g] = pair(*parts[i]).astype(bf16)
            for i in (1, 0):
                send(o_out.at[i, g], o_in.at[0, g], o_send.at[i, g], o_recv.at[0, g], {"sp": i + 2}).start()

        for i in (1, 0):
            stat_out[i] = stat_rows(1 + i)
            stat_copy(1, i + 2).start()

    @pl.when(me == 2)
    def _():
        near_blocks(1, [])
        q_copy(2, 1, 3).start()

        @pl.loop(1, 2)
        def _(half):
            for u in range(2):
                near_blocks(2 * half + u, [])

    convolve_first()

    @pl.when(me == 2)
    def _():
        q_from(3, 2, far_g).wait_recv()
        rest = near_blocks(far_g, [q_in[1, far_g]])
        for h in range(2):
            res, total = rest[h][0]
            far_r[1, h] = res
            far_t[1, h] = jnp.exp2(-total)
        offs_from(1, 2, 2)
        offs_from(0, 2, 1)
        for src in (1, 0):
            for t in range(2):
                send(packet.at[1 + t, far_g], kv_in.at[t, src], kv_last_send.at[t],
                     kv_last_recv.at[t, src], {"sp": src}).wait_recv()
            keys = split_keys(kv_in[0, src])
            values = split_values(kv_in[1, src])
            parts = []
            for h in range(2):
                (own, own_total), (far, far_total) = attend(
                    [packet[0, far_g], q_in[1, far_g]], keys[h], values[h], off_rows[1 + src, 2 * far_g + h:2 * far_g + h + 1, :], False)
                own = own_r[far_g, h] + own_t[far_g, h] * own
                far = far_r[1, h] + far_t[1, h] * far
                own_r[far_g, h] = own
                if src:
                    far_r[1, h] = far
                    own_t[far_g, h] = own_t[far_g, h] * jnp.exp2(-own_total)
                    far_t[1, h] = far_t[1, h] * jnp.exp2(-far_total)
                else:
                    note(0, far_g, h, own, own)
                    note(2, far_g, h, far, far)
                    parts.append(far)
        o_out[1, far_g] = pair(*parts).astype(bf16)
        o_out[1, far_g] = pair(*parts).astype(bf16)
        o_copy(2, 3, far_g).start()
        stat_out[1] = stat_rows(2)
        stat_copy(2, 3).start()

    @pl.when(me == 1)
    def _():
        for g in dev1_groups:
            close(g - 1, g, pair(own_r[g, 0], own_r[g, 1]))

    channel_norm()
    conv_product()

    @pl.when(me == 3)
    def _():
        offs_from(2, 3, 1)
        for g in dev1_groups:
            keys, values = kv_from(2, g)
            for h in range(2):
                res, total = attend([packet[0, g]], keys[h], values[h], off_of(1, g, h), False)[0]
                through = own_t[g, h]
                res = own_r[g, h] + through * res
                own_r[g, h] = res
                own_t[g, h] = through * jnp.exp2(-total)
                near = masses[0][:, (HEAD_DIM, 0)[h] + 4 + g:(HEAD_DIM, 0)[h] + 5 + g]
                note(0, g, h, res, total + near)

    def finish(g):
        own = pair(own_r[g, 0], own_r[g, 1])

        @pl.when(me == 0)
        def _():
            close(g, g, own)

        @pl.when(me == 2)
        def _():
            if g == far_g:
                close(g, g, own)
            else:
                through = pair(own_t[g, 0], own_t[g, 1])
                send(o_out.at[0, g], o_in.at[0, g], o_send.at[0, g], o_recv.at[0, g], {"sp": 1}).wait_recv()
                close(g, g, own + through * o_in[0, g].astype(f32))

        @pl.when(me == 3)
        def _():
            through = pair(own_t[g, 0], own_t[g, 1])
            src = 2 if g == far_g else 1
            send(o_out.at[1, g], o_in.at[src - 1, g], o_send.at[1, g], o_recv.at[src - 1, g], {"sp": src}).wait_recv()
            close(g, g, own + through * o_in[src - 1, g].astype(f32))

    for copy in attend_copies(False):
        copy.wait()
    share = rows // tp
    theirs = pl.ds(pl.multiple_of(partner * share, share), share)
    ours = pl.ds(pl.multiple_of(core * share, share), share)
    weight_swap = send(out_weights.at[1, pl.ds(cut, LANES)], partner_weights, swap_send.at[0], swap_recv.at[0], {"tp": partner})
    heads_swap = send(heads_last.at[theirs], partner_heads, swap_send.at[1], swap_recv.at[1], {"tp": partner})
    weight_swap.start()
    for g in range(final):
        finish(g)
    leaves = []
    for c in range(0, model, tile):
        cols = slice(c, c + tile)
        leaving[:, cols] = (conv_share[theirs, cols] + jnp.dot(
            heads_ref[theirs, :cut], out_weights[1, :cut, cols], preferred_element_type=f32)).astype(bf16)
        copy = send(leaving.at[:, pl.ds(c, tile)], arrived_ref.at[:, pl.ds(c, tile)],
                    out_send.at[c // tile], out_recv.at[c // tile], {"tp": partner})
        copy.start()
        leaves.append(copy)
    for c in range(0, model, tile):
        cols = slice(c, c + tile)
        conv_share[ours, cols] += jnp.dot(
            heads_ref[ours, :cut], out_weights[1, :cut, cols], preferred_element_type=f32)
    @pl.when(me == 1)
    def _():
        keys, values = kv_from(0, far_g)
        parts = []
        for h in range(2):
            res, _ = attend([packet[0, far_g]], keys[h], values[h], off_of(1, far_g, h), False)[0]
            res = own_r[far_g, h] + own_t[far_g, h] * res
            note(0, far_g, h, res, res)
            parts.append(res)
        close(final, far_g, pair(*parts))

    finish(final)
    heads_last[...] = heads_ref[:, cut:]
    heads_swap.start()
    for copy in leaves:
        copy.wait()
    weight_swap.wait()
    for c in range(0, model, tile):
        cols = slice(c, c + tile)
        conv_share[ours, cols] += arrived_ref[:, cols].astype(f32) + jnp.dot(
            heads_ref[ours, cut:], out_weights[1, cut:, cols], preferred_element_type=f32)

    mine = stat_rows(0)

    def write_log(m_odd, m_even):
        for g in range(groups):
            log_ref[2 * g:2 * g + 1] = jnp.log(jnp.maximum(m_even[g:g + 1], mass_floor))
            log_ref[2 * g + 1:2 * g + 2] = jnp.log(jnp.maximum(m_odd[g:g + 1], mass_floor))

    @pl.when(me < 2)
    def _():
        write_log(mine[0:4], mine[8:12])

    @pl.when(me == 2)
    def _():
        stat_copy(1, 2).wait_recv()
        far = stat_in[0]
        write_log(mine[0:4] + jnp.exp2(-mine[4:8]) * far[0:4], mine[8:12] + jnp.exp2(-mine[12:16]) * far[8:12])

    @pl.when(me == 3)
    def _():
        for src in (1, 2):
            send(stat_out.at[1], stat_in.at[src - 1], flow_send.at[2, 2], stat_recv.at[src - 1], {"sp": src}).wait_recv()
        far = stat_in[0] + stat_in[1]
        write_log(mine[0:4] + jnp.exp2(-mine[4:8]) * far[0:4], mine[8:12] + jnp.exp2(-mine[12:16]) * far[8:12])

    heads_swap.wait()
    for c in range(0, model, tile):
        cols = slice(c, c + tile)
        out_ref[:, cols] = (conv_share[ours, cols] + jnp.dot(
            partner_heads[...], partner_weights[:, cols], preferred_element_type=f32)).astype(bf16)

    @pl.when(me < n - 1)
    def _():
        halo_copy.wait_send()

    @pl.when(me == 0)
    def _():
        offs_copy(0, 1).wait_send()
        offs_copy(0, 2).wait_send()
        for t in range(2):
            for g in range(groups):
                kv_copy(0, t, g).wait_send()
            kv_last(t, 0).wait_send()

    @pl.when(me == 1)
    def _():
        offs_copy(1, 2).wait_send()
        for t in range(2):
            kv_last(t, 1).wait_send()
        for i in (1, 0):
            for g in dev1_groups:
                o_copy(1, i + 2, g).wait_send()
            stat_copy(1, i + 2).wait_send()

    @pl.when(me == 2)
    def _():
        offs_copy(2, 3).wait_send()
        for g in dev1_groups:
            q_copy(2, 1, g).wait_send()
            for t in range(2):
                kv_copy(2, t, g).wait_send()
        o_copy(2, 3, far_g).wait_send()
        stat_copy(2, 3).wait_send()

    @pl.when(me == 3)
    def _():
        for g in dev1_groups:
            q_copy(3, 1, g).wait_send()
        q_copy(3, 2, far_g).wait_send()


def place(mixed, mass_log, out_ref, log_ref, sem):
    copies = [
        pltpu.make_async_copy(mixed, out_ref, sem.at[0]),
        pltpu.make_async_copy(mass_log, log_ref, sem.at[1]),
    ]
    for copy in copies:
        copy.start()
    for copy in copies:
        copy.wait()


def local(n, tp,
    stream, norm_gain, query_weight, key_weight, value_weight, filter_input, filter_gate,
    score_offset, head_gain, filter_taps, channel_gain, channel_shift, attend_out, filter_out,
):
    f32, bf16 = jnp.float32, jnp.bfloat16
    rows = stream.shape[1]
    heads = score_offset.shape[2]
    groups = heads * HEAD_DIM // LANES
    chans = filter_input.shape[1]
    slabs = chans // LANES
    taps = filter_taps.shape[0]
    model = stream.shape[2]
    share = rows // tp
    tiles = model // min(1024, model)

    vmem = pl.BlockSpec(memory_space=pltpu.VMEM)
    hbm = pl.BlockSpec(memory_space=pltpu.HBM)
    dma = pltpu.SemaphoreType.DMA
    mixed, mass_log = pl.pallas_call(
        functools.partial(kernel, n, tp, taps, chans * tp),
        out_shape=(pltpu.VMEM((share, model), bf16), pltpu.VMEM((heads, rows), f32)),
        in_specs=[hbm] * 14,
        out_specs=(vmem,) * 2,
        scratch_shapes=[
            pltpu.VMEM((model,), bf16),
            pltpu.VMEM((heads, rows), bf16),
            pltpu.VMEM((taps, chans), bf16),
            pltpu.VMEM((chans,), bf16),
            pltpu.VMEM((chans,), bf16),
            pltpu.VMEM((chans,), bf16),
            pltpu.VMEM((rows, model), bf16),
            pltpu.VMEM((rows, model), bf16),
            pltpu.VMEM((5, model, chans), bf16),
            pltpu.VMEM((2, chans, model), bf16),
            pltpu.VMEM((3, groups, rows, LANES), bf16),
            pltpu.VMEM((2, groups, rows, LANES), bf16),
            pltpu.VMEM((2, groups, rows, LANES), bf16),
            pltpu.VMEM((3, heads, rows), bf16),
            pltpu.VMEM((2, groups, rows, LANES), bf16),
            pltpu.VMEM((2, groups, rows, LANES), bf16),
            pltpu.VMEM((2, 16, rows), f32),
            pltpu.VMEM((2, 16, rows), f32),
            pltpu.VMEM((groups, 2, rows, LANES), f32),
            pltpu.VMEM((groups, 2, rows, LANES), f32),
            pltpu.VMEM((2, 2, rows, LANES), f32),
            pltpu.VMEM((2, 2, rows, LANES), f32),
            pltpu.VMEM((3, rows, LANES), f32),
            pltpu.VMEM((3, heads, rows), f32),
            pltpu.VMEM((slabs, taps + -taps % 8, LANES), f32),
            pltpu.VMEM((rows, heads * HEAD_DIM), bf16),
            pltpu.VMEM((rows, chans), bf16),
            pltpu.VMEM((rows, model), f32),
            pltpu.VMEM((share, model), bf16),
            pltpu.VMEM((share, model), bf16),
            pltpu.VMEM((rows, LANES), bf16),
            pltpu.VMEM((share, LANES), bf16),
            pltpu.VMEM((LANES, model), bf16),
            pltpu.VMEM((HALO, chans), bf16),
            pltpu.VMEM((HALO, chans), bf16),
            pltpu.VMEM((slabs, HALO + rows, LANES), f32),
            pltpu.VMEM((slabs, rows, LANES), f32),
            pltpu.VMEM((rows, LANES), f32),
            pltpu.VMEM((rows, LANES), f32),
            dma((5, chans // (2 * LANES))), dma((3,)), dma((3, groups)), dma((4, groups)), dma((2,)), dma((2,)),
            dma((tiles,)), dma((tiles,)), dma, dma, dma, dma, pltpu.SemaphoreType.REGULAR, dma((2,)), dma((2,)),
        ],
        compiler_params=pltpu.CompilerParams(
            collective_id=0, has_side_effects=True, vmem_limit_bytes=56 * 1024 * 1024),
    )(stream[0], norm_gain, score_offset[0].T, filter_taps, head_gain, channel_gain, channel_shift,
      query_weight, key_weight, value_weight, filter_input, filter_gate, attend_out, filter_out)
    mixed, mass_log = pl.pallas_call(
        place,
        out_shape=(
            jax.ShapeDtypeStruct((share, model), bf16),
            jax.ShapeDtypeStruct((heads, rows), f32),
        ),
        in_specs=[vmem] * 2,
        out_specs=(hbm,) * 2,
        scratch_shapes=[dma((2,))],
    )(*[pltpu.with_memory_space_constraint(a, pltpu.VMEM) for a in (mixed, mass_log)])
    return (mixed[None], mass_log.T[None])


def shifted(value, axis, steps):
    count = lax.axis_size(axis)
    first, last = (max(0, -steps), min(count, count - steps))
    return lax.ppermute(value, axis, [(source, source + steps) for source in range(first, last)])


def local_ring(
    stream,
    norm_gain,
    query_weight,
    key_weight,
    value_weight,
    filter_input,
    filter_gate,
    score_offset,
    head_gain,
    filter_taps,
    channel_gain,
    channel_shift,
    attend_out,
    filter_out,
):
    rows_here = stream.shape[1]
    total_channels = filter_input.shape[1] * lax.axis_size("tp")
    xfloat = stream[0].astype(jnp.float32)
    normed = xfloat * lax.rsqrt(jnp.mean(xfloat * xfloat, axis=-1, keepdims=True) + rms_eps)
    normed = (normed * norm_gain.astype(jnp.float32)).astype(jnp.bfloat16)

    def project(weight):
        return jnp.dot(normed, weight, preferred_element_type=jnp.float32).astype(jnp.bfloat16)

    queries = project(query_weight)
    keys_here = project(key_weight)
    values_here = project(value_weight)
    conv_in = project(filter_input)
    conv_gate = project(filter_gate)
    offsets_here = score_offset[0]
    heads_here = offsets_here.shape[1]
    first_pos = lax.axis_index("sp") * rows_here
    position = first_pos + jnp.arange(rows_here, dtype=jnp.int32)
    qheads = queries.reshape(rows_here, heads_here, HEAD_DIM)

    def absorb(state_now, kblock, vblock, oblock, first_key):
        attended, weight_mass, survive = state_now
        span = kblock.shape[0]
        kblock = kblock.reshape(span, heads_here, HEAD_DIM)
        vblock = vblock.reshape(span, heads_here, HEAD_DIM)
        scores = jnp.einsum(
            "thd,shd->hts", qheads, kblock, preferred_element_type=jnp.float32
        ) * HEAD_DIM ** (-0.5)
        scores = scores + oblock.astype(jnp.float32).T[:, None, :]
        key_pos = first_key + jnp.arange(span, dtype=jnp.int32)
        strict = ((key_pos[None, :] < position[:, None]) & (key_pos[None, :] >= 0))[None]
        losing = jnp.where(strict, jax.nn.log_sigmoid(-scores), 0.0)
        beyond = lax.cumsum(losing, axis=2, reverse=True) - losing + survive[:, :, None]
        weights = jnp.where(strict, jnp.exp(jax.nn.log_sigmoid(scores) + beyond), 0.0)
        weight_mass = weight_mass + jnp.sum(weights, axis=2)
        attended = attended + jnp.einsum(
            "hts,shd->thd", weights.astype(jnp.bfloat16), vblock, preferred_element_type=jnp.float32
        )
        survive = survive + jnp.sum(losing, axis=2)
        return (attended, weight_mass, survive)

    initial = (
        jnp.zeros((rows_here, heads_here, HEAD_DIM), jnp.float32),
        jnp.zeros((heads_here, rows_here), jnp.float32),
        jnp.zeros((heads_here, rows_here), jnp.float32),
    )
    state_now = absorb(initial, keys_here, values_here, offsets_here, first_pos)

    def pass_turn(turn_index, carried):
        state_now, travelling = carried
        travelling = shifted((travelling[0], travelling[1], travelling[2]), "sp", 1)
        first_key = first_pos - (turn_index + 1) * rows_here
        state_now = absorb(state_now, travelling[0], travelling[1], travelling[2], first_key)
        return (state_now, travelling)

    state_now, travelling = lax.fori_loop(
        0, lax.axis_size("sp") - 1, pass_turn, (state_now, (keys_here, values_here, offsets_here))
    )
    attended, weight_mass, survive = state_now
    head_scale = lax.rsqrt(jnp.mean(attended * attended, axis=-1, keepdims=True) + rms_eps)
    heads_flat = attended * head_scale * head_gain.astype(jnp.float32).reshape(heads_here, HEAD_DIM)
    heads_flat = heads_flat.astype(jnp.bfloat16).reshape(rows_here, heads_here * HEAD_DIM)
    mass_log = jnp.log(jnp.maximum(weight_mass.T, mass_floor))
    gated_rows = (
        conv_in.astype(jnp.float32) * jax.nn.sigmoid(conv_gate.astype(jnp.float32))
    ).astype(jnp.bfloat16)
    reach_back = filter_taps.shape[0] - 1
    earlier = shifted(gated_rows[rows_here - reach_back :], "sp", 1)
    extended = jnp.concatenate([earlier, gated_rows], axis=0).astype(jnp.float32)
    tap_values = filter_taps.astype(jnp.float32)
    filtered = jnp.zeros((rows_here, gated_rows.shape[1]), jnp.float32)
    for tap_index in range(reach_back + 1):
        filtered = filtered + extended[tap_index : tap_index + rows_here] * tap_values[tap_index]
    center = lax.psum(jnp.sum(filtered, axis=-1), "tp") / total_channels
    deviation = filtered - center[:, None]
    spread = lax.psum(jnp.sum(deviation * deviation, axis=-1), "tp") / total_channels
    conv_out = jax.nn.silu(
        deviation * lax.rsqrt(spread[:, None] + norm_eps) * channel_gain.astype(jnp.float32)
        + channel_shift.astype(jnp.float32)
    ).astype(jnp.bfloat16)
    mixed_out = lax.psum_scatter(
        (
            jnp.dot(heads_flat, attend_out, preferred_element_type=jnp.float32)
            + jnp.dot(conv_out, filter_out, preferred_element_type=jnp.float32)
        ).astype(jnp.bfloat16),
        "tp",
        scatter_dimension=0,
        tiled=True,
    )
    return (mixed_out[None], mass_log[None])


def solution(mesh):
    n, tp = mesh.shape["sp"], mesh.shape["tp"]

    def choose(*args):
        rows, heads, chans = args[0].shape[1], args[7].shape[2], args[5].shape[1]
        same = args[2].shape[1] == chans and heads * HEAD_DIM == 4 * LANES == chans
        if n == 4 and tp == 2 and same and rows % 128 == 0:
            return local(n, tp, *args)
        return local_ring(*args)

    return jax.shard_map(
        choose,
        mesh=mesh,
        in_specs=(
            P("fs", "sp", None), P(), P(None, "tp"), P(None, "tp"), P(None, "tp"),
            P(None, "tp"), P(None, "tp"), P("fs", "sp", "tp"), P("tp"), P(None, "tp"),
            P("tp"), P("tp"), P("tp", None), P("tp", None),
        ),
        out_specs=(P("fs", ("sp", "tp"), None), P("fs", "sp", "tp")),
        check_vma=False,
    )
```
